128 devices in a mesh: sp: 16 (over z, x), tp: 8 (over y, core).
Axes of the slice: x: 4, y: 4, z: 4, core: 2. Of those that a mesh axis runs over, the one named last changes fastest.
Arguments:
- latent: bfloat16 [2, 8192, 2048], P(None, ('sp', 'tp')), may hold values from -6 to 6
- context: bfloat16 [2, 1024, 2048], P(None, 'sp'), may hold values from -6 to 6
- cond: bfloat16 [2, 2048], replicated, may hold values from -6 to 6
- ctx_cond: bfloat16 [2048], replicated, may hold values from -6 to 6
- w_shift: bfloat16 [2048, 2048], P('sp', 'tp'), may hold values from -0.125 to 0.125
- w_scale: bfloat16 [2048, 2048], P('sp', 'tp'), may hold values from -0.125 to 0.125
- w_gate: bfloat16 [2048, 2048], P('sp', 'tp'), may hold values from -0.125 to 0.125
- norm_gain: float32 [2048], replicated, may hold values from 0.1 to 1.9
- w_query: bfloat16 [2048, 2048], P(None, 'tp'), may hold values from -1.08275726 to 1.08275726
- w_key: bfloat16 [2048, 2048], P(None, 'tp'), may hold values from -0.090598056 to 0.090598056
- w_value: bfloat16 [2048, 2048], P(None, 'tp'), may hold values from -0.125 to 0.125
- w_out: bfloat16 [2048, 2048], P('tp'), may hold values from -1.5 to 1.5
- rel_bias: float32 [32, 15, 31], P('tp'), may hold values from -4 to 4
- ctx_bias: float32 [32], P('tp'), may hold values from -3.5 to -2
Outputs:
- mixed: bfloat16 [2, 8192, 2048], P(None, ('sp', 'tp'))
The draws below stay inside these ranges and needn't reach their ends.
All inputs are finite; a program needn't handle non-finite values.
Results may differ from the reference program's by a relative error of at most 0.0154.
Values may be sent and summed in bfloat16 or wider, within the bound.
No kernel may reach another device: no remote copies, remote signals or barrier semaphores. Data moves between devices by JAX's collectives and lax.ppermute only.
A program may use at most 128 MiB of HBM per device.

```python
import jax
import jax.numpy as jnp
from jax import lax

D = 2048
HEADS = 32
HEAD_DIM = 64
GRID_W = 64
WIN_ROWS = 8
WIN_COLS = 16
SAMPLES = 2
ROWS = 128
TOKENS = 8192
CTX = 1024
N_TP = 8


def shared_keys(key):
    base = jax.random.normal(jax.random.fold_in(key, 11), (D, D), jnp.float32)
    return jnp.clip(base, -4.0, 4.0) * D ** (-0.5)


def draw_w_key(key, part):
    return shared_keys(key).astype(jnp.bfloat16)


def draw_w_query(key, part):
    own = jax.random.normal(jax.random.fold_in(key, 12), (D, D), jnp.float32)
    own = jnp.clip(own, -4.0, 4.0) * D ** (-0.5)
    return own.astype(jnp.bfloat16)


def levels(own_key, extent, pieces, smallest, high):
    loudness, own = 1.0, jax.random.fold_in(own_key, 6)
    for axis_at, parts in pieces:
        steps = jnp.exp(jax.random.uniform(jax.random.fold_in(own, axis_at), (parts,), jnp.float32, smallest / len(pieces), high / len(pieces)))
        loudness = loudness * jnp.repeat(steps, extent[axis_at] // parts).reshape([-1 if axis == axis_at else 1 for axis in range(len(extent))])
    return loudness


def noise(stream_key, extent, width, limit, shards=(), kind=jnp.bfloat16):
    entries = jax.random.normal(stream_key, extent, jnp.float32) * width
    if len(shards) > 0:
        entries = levels(stream_key, extent, shards, -0.22, 0.18) * entries
    return jnp.clip(entries, min=-limit, max=limit).astype(kind)


def setup_inputs(seed: int = 0) -> dict:
    key_list = jax.random.split(jax.random.key(seed), 15)
    return {
        "latent": noise(key_list[0], (SAMPLES, TOKENS, D), 1.0, 6.0, ((1, 128),)),
        "context": noise(key_list[1], (SAMPLES, CTX, D), 1.0, 6.0, ((1, 16),)),
        "cond": noise(key_list[2], (SAMPLES, D), 1.0, 6.0),
        "ctx_cond": noise(key_list[3], (D,), 1.0, 6.0),
        "w_shift": noise(key_list[4], (D, D), D ** -0.5, 0.125, ((0, 16), (1, 8))),
        "w_scale": noise(key_list[5], (D, D), D ** -0.5, 0.125, ((0, 16), (1, 8))),
        "w_gate": noise(key_list[6], (D, D), D ** -0.5, 0.125, ((0, 16), (1, 8))),
        "norm_gain": jnp.clip(1.0 + 0.18 * jax.random.normal(key_list[7], (D,), jnp.float32), 0.1, 1.9),
        "w_query": draw_w_query(jax.random.fold_in(key_list[14], 71), 0),
        "w_key": draw_w_key(jax.random.fold_in(key_list[14], 71), 0),
        "w_value": noise(key_list[10], (D, D), D ** -0.5, 0.125, ((1, 8),)),
        "w_out": noise(key_list[11], (D, D), 16 ** -0.5, 1.5, ((0, 8),)),
        "rel_bias": noise(key_list[12], (HEADS, 2 * WIN_ROWS - 1, 2 * WIN_COLS - 1), 1.0, 4.0, ((0, 8),), jnp.float32),
        "ctx_bias": jnp.clip(-3.5 + 1.5 * jax.random.uniform(key_list[13], (HEADS,), jnp.float32) ** levels(key_list[13], (HEADS,), ((0, 8),), -0.2, 0.2), -3.5, -2.0),
    }


EPSILON = 1e-06

def modulate_rows(rows, gain, shift, scale):
    floats = rows.astype(jnp.float32)
    inverse = lax.rsqrt(lax.optimization_barrier(jnp.mean(floats * floats, axis=-1, keepdims=True)) + EPSILON)
    return (floats * inverse * gain * (1.0 + scale) + shift).astype(jnp.bfloat16)

def project(rows, weight):
    return jnp.dot(rows, weight, preferred_element_type=jnp.float32).astype(jnp.bfloat16)

def reference(latent, context, cond, ctx_cond, w_shift, w_scale, w_gate, norm_gain, w_query, w_key, w_value, w_out, rel_bias, ctx_bias):
    ada = jax.nn.silu(cond.astype(jnp.float32)).astype(jnp.bfloat16)
    ada_ctx = jax.nn.silu(ctx_cond.astype(jnp.float32)).astype(jnp.bfloat16)[None, :]
    shift = jnp.dot(ada, w_shift, preferred_element_type=jnp.float32)
    scale = jnp.dot(ada, w_scale, preferred_element_type=jnp.float32)
    gate = jnp.dot(ada, w_gate, preferred_element_type=jnp.float32)
    ctx_shift = jnp.dot(ada_ctx, w_shift, preferred_element_type=jnp.float32)[0]
    ctx_scale = jnp.dot(ada_ctx, w_scale, preferred_element_type=jnp.float32)[0]
    hidden = modulate_rows(latent, norm_gain, shift[:, None, :], scale[:, None, :])
    ctx_hidden = modulate_rows(context, norm_gain, ctx_shift, ctx_scale)
    query = project(hidden, w_query).reshape(SAMPLES, ROWS, GRID_W, HEADS, HEAD_DIM)
    key = project(hidden, w_key).reshape(SAMPLES, ROWS, GRID_W, HEADS, HEAD_DIM)
    value = project(hidden, w_value).reshape(SAMPLES, ROWS, GRID_W, HEADS, HEAD_DIM)
    ctx_key = project(ctx_hidden, w_key).reshape(SAMPLES, CTX, HEADS, HEAD_DIM).astype(jnp.float32)
    ctx_value = project(ctx_hidden, w_value).reshape(SAMPLES, CTX, HEADS, HEAD_DIM).astype(jnp.float32)
    factor = HEAD_DIM ** (-0.5)
    columns = jnp.arange(GRID_W, dtype=jnp.int32)
    col_start = jnp.clip(columns - WIN_COLS // 2, 0, GRID_W - WIN_COLS)
    col_mask = (columns[None, :] >= col_start[:, None]) & (columns[None, :] < col_start[:, None] + WIN_COLS)
    col_index = jnp.clip(columns[None, :] - columns[:, None] + WIN_COLS - 1, 0, 2 * WIN_COLS - 2)

    def one_row(row):
        first = jnp.clip(row - WIN_ROWS // 2, 0, ROWS - WIN_ROWS).astype(jnp.int32)
        query_row = lax.dynamic_index_in_dim(query, row, axis=1, keepdims=False).astype(jnp.float32)
        key_rows = lax.dynamic_slice_in_dim(key, first, WIN_ROWS, axis=1).astype(jnp.float32)
        value_rows = lax.dynamic_slice_in_dim(value, first, WIN_ROWS, axis=1).astype(jnp.float32)
        row_index = first + jnp.arange(WIN_ROWS, dtype=jnp.int32) - row + WIN_ROWS - 1
        bias = rel_bias[:, row_index][:, :, col_index]
        near = jnp.einsum('sqhd,siwhd->shqiw', query_row, key_rows) * factor + bias.transpose(0, 2, 1, 3)[None]
        near = jnp.where(col_mask[None, None, :, None, :], near, -jnp.inf).reshape(SAMPLES, HEADS, GRID_W, WIN_ROWS * GRID_W)
        far = jnp.einsum('sqhd,schd->shqc', query_row, ctx_key) * factor + ctx_bias[None, :, None, None]
        top = jnp.maximum(lax.optimization_barrier(jnp.max(near, axis=-1)), lax.optimization_barrier(jnp.max(far, axis=-1)))[..., None]
        near_exp = jnp.exp(near - top)
        far_exp = jnp.exp(far - top)
        total = lax.optimization_barrier(jnp.sum(near_exp, axis=-1, keepdims=True)) + lax.optimization_barrier(jnp.sum(far_exp, axis=-1, keepdims=True))
        near_weight = (near_exp / total).astype(jnp.bfloat16).astype(jnp.float32)
        far_weight = (far_exp / total).astype(jnp.bfloat16).astype(jnp.float32)
        near_weight = near_weight.reshape(SAMPLES, HEADS, GRID_W, WIN_ROWS, GRID_W)
        mixed = jnp.einsum('shqiw,siwhd->sqhd', near_weight, value_rows) + jnp.einsum('shqc,schd->sqhd', far_weight, ctx_value)
        return mixed.astype(jnp.bfloat16)
    attended = lax.map(one_row, jnp.arange(ROWS, dtype=jnp.int32))
    attended = attended.transpose(1, 0, 2, 3, 4).reshape(SAMPLES, TOKENS, D)
    group = D // N_TP
    update = jnp.zeros((SAMPLES, TOKENS, D), jnp.float32)
    for index in range(N_TP):
        part = jnp.dot(attended[..., index * group:(index + 1) * group], w_out[index * group:(index + 1) * group], preferred_element_type=jnp.float32).astype(jnp.bfloat16)
        part = lax.optimization_barrier(part)
        update = update + part.astype(jnp.float32)
    mixed_out = latent.astype(jnp.float32) + gate[:, None, :] * update
    return mixed_out.astype(jnp.bfloat16)
```

```python
import jax
import jax.numpy as jnp
from jax import lax
from jax.experimental import pallas as pl
from jax.experimental.pallas import tpu as pltpu
from jax.sharding import PartitionSpec as P

HEAD_DIM = 64
GRID_W = 64
WIN_ROWS = 8
WIN_COLS = 16
EPSILON = 1e-06
MASKED = -1e30
REACH = WIN_ROWS // 2
BIAS_BLOCKS = 7


def copy_for_each(shard, axis):
    length = lax.axis_size(axis)
    return lax.all_to_all(
        jnp.broadcast_to(shard[None], (length, *shard.shape)), axis, 0, 0, tiled=True
    )


def silu_rows(values):
    return jax.nn.silu(values.astype(jnp.float32)).astype(jnp.bfloat16)


def whole(shape):
    return pl.BlockSpec(shape, lambda *_: (0,) * len(shape))


def project(rows, gain, shift, scale, weights, parts, block):
    count, width = rows.shape
    cols = weights[0].shape[1]

    def body(rows_ref, gain_ref, shift_ref, scale_ref, *refs):
        weight_refs, out_refs = refs[: len(weights)], refs[len(weights) :]
        floats = rows_ref[...].astype(jnp.float32)
        inverse = lax.rsqrt(jnp.mean(floats * floats, axis=-1, keepdims=True) + EPSILON)
        factor = gain_ref[...] * (1.0 + scale_ref[...])
        hidden = (floats * inverse * factor + shift_ref[...]).astype(jnp.bfloat16)
        at = 0
        for out_ref, part in zip(out_refs, parts):
            for index, multiple in enumerate(part):
                product = jnp.dot(hidden, weight_refs[at][...], preferred_element_type=jnp.float32)
                if multiple != 1.0:
                    product = product.astype(jnp.bfloat16).astype(jnp.float32) * multiple
                out_ref[:, index * cols : (index + 1) * cols] = product.astype(jnp.bfloat16)
                at += 1

    return pl.pallas_call(
        body,
        grid=(count // block,),
        in_specs=[pl.BlockSpec((block, width), lambda i: (i, 0))]
        + [whole((1, width))] * 3
        + [whole(weight.shape) for weight in weights],
        out_specs=[pl.BlockSpec((block, cols * len(part)), lambda i: (i, 0)) for part in parts],
        out_shape=[
            jax.ShapeDtypeStruct((count, cols * len(part)), jnp.bfloat16) for part in parts
        ],
        name="project",
    )(rows, gain, shift, scale, *weights)


def bias_table(rel_bias):
    heads, offsets, spread = rel_bias.shape
    slots = 2 * BIAS_BLOCKS + 2
    padded = jnp.pad(rel_bias, ((0, 0), (0, slots - offsets), (0, 128 - spread)))
    padded = padded.reshape(heads * slots, 128)

    def body(rel_ref, out_ref):
        query = lax.broadcasted_iota(jnp.int32, (GRID_W, 128), 0)
        lane = lax.broadcasted_iota(jnp.int32, (GRID_W, 128), 1)
        low = lane < GRID_W
        key = jnp.where(low, lane, lane - GRID_W)
        start = jnp.clip(query - WIN_COLS // 2, 0, GRID_W - WIN_COLS)
        inside = (key >= start) & (key < start + WIN_COLS)

        def diagonal(head, slot, move):
            row = jnp.broadcast_to(rel_ref[pl.ds(head * slots + slot, 1), :], (GRID_W, 128))
            return pltpu.roll(row, (128 - (WIN_COLS - 1) + move) % 128, 1, stride=1, stride_axis=0)

        for parity in range(2):
            for head in range(heads):
                for block in range(BIAS_BLOCKS):
                    slot = 2 * block + parity
                    both = jnp.where(
                        low, diagonal(head, slot, 0), diagonal(head, slot + 1, GRID_W)
                    )
                    out_ref[
                        parity, head * GRID_W : (head + 1) * GRID_W, block * 128 : (block + 1) * 128
                    ] = jnp.where(inside, both, MASKED)

    return pl.pallas_call(
        body,
        out_shape=jax.ShapeDtypeStruct((2, heads * GRID_W, BIAS_BLOCKS * 128), jnp.float32),
        name="bias_table",
    )(padded)


def attend(place, query, before, pair, after, ctx_pair, table, ctx_bias, rows_all):
    tokens, cols = query.shape
    heads = cols // HEAD_DIM
    rows_dev = tokens // GRID_W
    near_keys = WIN_ROWS * GRID_W
    padded = before.shape[0] + pair.shape[0] + after.shape[0]
    ctx_count = ctx_pair.shape[0]
    queries = heads * GRID_W

    def body(place_ref, q_ref, before_ref, pair_ref, after_ref, ctx_ref, table_ref, cb_ref, out_ref, keys):
        row = pl.program_id(0)

        @pl.when(row == 0)
        def _():
            first = before_ref.shape[0]
            keys[0:first] = before_ref[...]
            keys[first : first + tokens] = pair_ref[...]
            keys[first + tokens : padded] = after_ref[...]

        base = place_ref[0] * rows_dev
        actual = base + row
        start = jnp.clip(actual - REACH, 0, rows_all - WIN_ROWS)
        local = start - base + REACH
        offset = start - actual + WIN_ROWS - 1
        q = q_ref[...]
        lane = lax.broadcasted_iota(jnp.int32, (GRID_W, cols), 1)
        masks = [(lane >= h * HEAD_DIM) & (lane < (h + 1) * HEAD_DIM) for h in range(heads)]
        spread = jnp.concatenate([jnp.where(mask, q, jnp.zeros_like(q)) for mask in masks], axis=0)
        at = pl.multiple_of(local * GRID_W, GRID_W)
        near_pair = keys[pl.ds(at, near_keys), :]
        nt = (((1,), (1,)), ((), ()))
        near = lax.dot_general(
            spread, near_pair[:, :cols], nt, preferred_element_type=jnp.float32
        )
        column = pl.multiple_of((offset // 2) * 128, 128)
        near = near + table_ref[offset % 2, :, pl.ds(column, near_keys)]
        far = lax.dot_general(
            spread, ctx_ref[:, :cols], nt, preferred_element_type=jnp.float32
        )
        cb = cb_ref[...]
        top = jnp.maximum(
            jnp.max(near, axis=-1, keepdims=True), jnp.max(far, axis=-1, keepdims=True) + cb
        )
        near_exp = jnp.exp(near - top)
        far_exp = jnp.exp(far - (top - cb))
        total = jnp.sum(near_exp, axis=-1, keepdims=True) + jnp.sum(far_exp, axis=-1, keepdims=True)
        mixed = jnp.dot(
            near_exp.astype(jnp.bfloat16), near_pair[:, cols:], preferred_element_type=jnp.float32
        ) + jnp.dot(
            far_exp.astype(jnp.bfloat16), ctx_ref[:, cols:], preferred_element_type=jnp.float32
        )
        mixed = mixed / total
        result = jnp.where(masks[0], mixed[:GRID_W], 0.0)
        for h in range(1, heads):
            result = jnp.where(masks[h], mixed[h * GRID_W : (h + 1) * GRID_W], result)
        out_ref[...] = result.astype(jnp.bfloat16)

    return pl.pallas_call(
        body,
        grid=(rows_dev,),
        in_specs=[
            pl.BlockSpec(memory_space=pltpu.SMEM),
            pl.BlockSpec((GRID_W, cols), lambda i: (i, 0)),
            whole(before.shape),
            whole(pair.shape),
            whole(after.shape),
            whole(ctx_pair.shape),
            whole(table.shape),
            whole((queries, 1)),
        ],
        out_specs=pl.BlockSpec((GRID_W, cols), lambda i: (i, 0)),
        out_shape=jax.ShapeDtypeStruct((tokens, cols), jnp.bfloat16),
        scratch_shapes=[pltpu.VMEM((padded, 2 * cols), jnp.bfloat16)],
        name="attend",
    )(place, query, before, pair, after, ctx_pair, table, ctx_bias)


def on_device(
    latent,
    context,
    cond,
    ctx_cond,
    w_shift,
    w_scale,
    w_gate,
    norm_gain,
    w_query,
    w_key,
    w_value,
    w_out,
    rel_bias,
    ctx_bias,
):
    samples, tokens_dev, width = latent.shape
    rows_sp, local_cols = w_shift.shape
    heads = local_cols // HEAD_DIM
    sp_index = lax.axis_index("sp")
    sp_size = lax.axis_size("sp")
    gathered = [lax.all_gather(latent[s], "tp", axis=0, tiled=True) for s in range(samples)]
    ada = silu_rows(jnp.concatenate([cond, ctx_cond[None, :]], axis=0))
    ada_rows = lax.dynamic_slice_in_dim(ada, sp_index * rows_sp, rows_sp, 1)
    partial_value = jnp.stack(
        [
            jnp.dot(ada_rows, weight, preferred_element_type=jnp.float32)
            for weight in (w_shift, w_scale, w_gate)
        ]
    )
    summed = jnp.sum(copy_for_each(partial_value, "sp"), axis=0)
    tiles = copy_for_each(summed, "tp")
    modulation = jnp.moveaxis(tiles, 0, 2).reshape(3, samples + 1, width)
    gain = norm_gain[None, :]
    table = bias_table(rel_bias)
    place = jnp.full((1,), sp_index, jnp.int32)
    ctx_rows = context.shape[1]
    (ctx_pair,) = project(
        context.reshape(samples * ctx_rows, width),
        gain,
        modulation[0, samples][None],
        modulation[1, samples][None],
        (w_key, w_value),
        ((1.0, 1.0),),
        samples * ctx_rows,
    )
    ctx_pair = lax.all_gather(
        ctx_pair.reshape(samples, ctx_rows, 2 * local_cols), "sp", axis=1, tiled=True
    )
    cb = jnp.repeat(ctx_bias, GRID_W)[:, None]
    up = [(i, i + 1) for i in range(sp_size - 1)]
    down = [(j, i) for i, j in up]
    outs = []
    for s in range(samples):
        query, pair = project(
            gathered[s],
            gain,
            modulation[0, s][None],
            modulation[1, s][None],
            (w_query, w_key, w_value),
            ((HEAD_DIM**-0.5,), (1.0, 1.0)),
            128,
        )
        tokens = pair.shape[0]
        before = lax.ppermute(pair[tokens - REACH * GRID_W :], "sp", up)
        after = lax.ppermute(pair[: (WIN_ROWS - REACH - 1) * GRID_W], "sp", down)
        attended = attend(
            place,
            query,
            before,
            pair,
            after,
            ctx_pair[s],
            table,
            cb,
            tokens // GRID_W * sp_size,
        )
        part = jnp.dot(attended, w_out, preferred_element_type=jnp.float32).astype(jnp.bfloat16)
        update = lax.psum_scatter(part, "tp", scatter_dimension=0, tiled=True)
        outs.append(
            (
                latent[s].astype(jnp.float32)
                + modulation[2, s][None] * update.astype(jnp.float32)
            ).astype(jnp.bfloat16)
        )
    return jnp.stack(outs)


def solution(mesh):
    return jax.shard_map(
        on_device,
        mesh=mesh,
        in_specs=(
            P(None, ("sp", "tp"), None),
            P(None, "sp", None),
            P(),
            P(),
            P("sp", "tp"),
            P("sp", "tp"),
            P("sp", "tp"),
            P(),
            P(None, "tp"),
            P(None, "tp"),
            P(None, "tp"),
            P("tp", None),
            P("tp", None, None),
            P("tp"),
        ),
        out_specs=P(None, ("sp", "tp"), None),
        check_vma=False,
    )
```

```python
import jax
import jax.numpy as jnp
from jax import lax
from jax.experimental import pallas as pl
from jax.experimental.pallas import tpu as pltpu
from jax.sharding import PartitionSpec as P

HEAD_DIM = 64
GRID_W = 64
WIN_ROWS = 8
WIN_COLS = 16
EPSILON = 1e-06
MASKED = -1e30
REACH = WIN_ROWS // 2
BIAS_BLOCKS = 7


def copy_for_each(shard, axis):
    length = lax.axis_size(axis)
    return lax.all_to_all(
        jnp.broadcast_to(shard[None], (length, *shard.shape)), axis, 0, 0, tiled=True
    )


def silu_rows(values):
    return jax.nn.silu(values.astype(jnp.float32)).astype(jnp.bfloat16)


def modulation_parts(place, cond, ctx_cond, weights, copies):
    samples = cond.shape[0]
    rows, cols = weights[0].shape

    def body(place_ref, cond_ref, ctx_ref, shift_ref, scale_ref, gate_ref, out_ref):
        at = pl.multiple_of(place_ref[0] * rows, rows)
        ada = silu_rows(cond_ref[:, pl.ds(at, rows)])
        ada_ctx = silu_rows(ctx_ref[:, pl.ds(at, rows)])
        both = jnp.concatenate([ada.astype(jnp.float32), ada_ctx.astype(jnp.float32)], axis=0)
        both = both.astype(jnp.bfloat16)
        result = jnp.concatenate(
            [
                jnp.dot(both, shift_ref[...], preferred_element_type=jnp.float32),
                jnp.dot(both, scale_ref[...], preferred_element_type=jnp.float32),
                jnp.dot(ada, gate_ref[...], preferred_element_type=jnp.float32),
            ],
            axis=0,
        )
        for copy in range(copies):
            out_ref[copy] = result

    return pl.pallas_call(
        body,
        in_specs=[pl.BlockSpec(memory_space=pltpu.SMEM)]
        + [pl.BlockSpec(memory_space=pltpu.VMEM)] * 5,
        out_shape=jax.ShapeDtypeStruct((copies, 3 * samples + 2, cols), jnp.float32),
        name="modulation_parts",
    )(place, cond, ctx_cond, *weights)


def whole(shape):
    return pl.BlockSpec(shape, lambda *_: (0,) * len(shape))


def project(rows, sample, gain, shift, scale, weights, block, ends):
    _, count, width = rows.shape
    cols = weights[0].shape[1]
    first, last = ends if ends else (0, 0)
    steps = count // block

    def body(rows_ref, gain_ref, shift_ref, scale_ref, *refs):
        weight_refs, out_refs = refs[: len(weights)], refs[len(weights) :]
        step = pl.program_id(0)
        floats = rows_ref[0].astype(jnp.float32)
        inverse = lax.rsqrt(jnp.mean(floats * floats, axis=-1, keepdims=True) + EPSILON)
        factor = gain_ref[...] * (1.0 + scale_ref[...])
        hidden = (floats * inverse * factor + shift_ref[...]).astype(jnp.bfloat16)
        pair = [
            jnp.dot(hidden, ref[...], preferred_element_type=jnp.float32).astype(jnp.bfloat16)
            for ref in weight_refs[:2]
        ]
        out_refs[0][:, :cols] = pair[0]
        out_refs[0][:, cols:] = pair[1]
        if ends:
            query = jnp.dot(hidden, weight_refs[2][...], preferred_element_type=jnp.float32)
            query = query.astype(jnp.bfloat16).astype(jnp.float32) * HEAD_DIM**-0.5
            out_refs[1][...] = query.astype(jnp.bfloat16)
            for number in range(steps):
                low = number * block
                for out_ref, start, stop in (
                    (out_refs[2], 0, first),
                    (out_refs[3], count - last, count),
                ):
                    lo, hi = max(low, start), min(low + block, stop)
                    if lo < hi:

                        @pl.when(step == number)
                        def _(out_ref=out_ref, start=start, lo=lo, hi=hi, low=low):
                            for index in range(2):
                                out_ref[
                                    lo - start : hi - start, index * cols : (index + 1) * cols
                                ] = pair[index][lo - low : hi - low]

    out_specs = [pl.BlockSpec((block, 2 * cols), lambda i: (i, 0))]
    out_shape = [jax.ShapeDtypeStruct((count, 2 * cols), jnp.bfloat16)]
    if ends:
        out_specs += [pl.BlockSpec((block, cols), lambda i: (i, 0))]
        out_shape += [jax.ShapeDtypeStruct((count, cols), jnp.bfloat16)]
        for length in ends:
            out_specs += [whole((length, 2 * cols))]
            out_shape += [jax.ShapeDtypeStruct((length, 2 * cols), jnp.bfloat16)]
    return pl.pallas_call(
        body,
        grid=(steps,),
        in_specs=[pl.BlockSpec((1, block, width), lambda i: (sample, i, 0))]
        + [whole((1, width))] * 3
        + [whole(weight.shape) for weight in weights],
        out_specs=out_specs,
        out_shape=out_shape,
        name="project",
    )(rows, gain, shift, scale, *weights)


def bias_table(rel_bias):
    heads, offsets, spread = rel_bias.shape
    slots = 2 * BIAS_BLOCKS + 2
    padded = jnp.pad(rel_bias, ((0, 0), (0, slots - offsets), (0, 128 - spread)))
    padded = padded.reshape(heads * slots, 128)

    def body(rel_ref, out_ref):
        query = lax.broadcasted_iota(jnp.int32, (GRID_W, 128), 0)
        lane = lax.broadcasted_iota(jnp.int32, (GRID_W, 128), 1)
        low = lane < GRID_W
        key = jnp.where(low, lane, lane - GRID_W)
        start = jnp.clip(query - WIN_COLS // 2, 0, GRID_W - WIN_COLS)
        inside = (key >= start) & (key < start + WIN_COLS)

        def diagonal(head, slot, move):
            row = jnp.broadcast_to(rel_ref[pl.ds(head * slots + slot, 1), :], (GRID_W, 128))
            return pltpu.roll(row, (128 - (WIN_COLS - 1) + move) % 128, 1, stride=1, stride_axis=0)

        for parity in range(2):
            for head in range(heads):
                for block in range(BIAS_BLOCKS):
                    slot = 2 * block + parity
                    both = jnp.where(
                        low, diagonal(head, slot, 0), diagonal(head, slot + 1, GRID_W)
                    )
                    out_ref[
                        parity, head * GRID_W : (head + 1) * GRID_W, block * 128 : (block + 1) * 128
                    ] = jnp.where(inside, both, MASKED)

    return pl.pallas_call(
        body,
        out_shape=jax.ShapeDtypeStruct((2, heads * GRID_W, BIAS_BLOCKS * 128), jnp.float32),
        name="bias_table",
    )(padded)


def attend(place, sample, query, before, pair, after, ctx_keys, ctx_values, table, ctx_bias, rows_all, per):
    tokens, cols = query.shape
    heads = cols // HEAD_DIM
    rows_dev = tokens // GRID_W
    near_keys = WIN_ROWS * GRID_W
    ahead, behind = before.shape[0], after.shape[0]
    padded = ahead + tokens + behind
    lanes = -(-padded // 128) * 128
    groups, members, _, ctx_rows, _ = (len(ctx_keys), *ctx_keys[0].shape)
    ctx_count = groups * members * ctx_rows
    queries = heads * GRID_W
    bf16, f32 = jnp.bfloat16, jnp.float32

    def body(place_ref, q_ref, before_ref, pair_ref, after_ref, *refs):
        key_refs, value_refs = refs[:groups], refs[groups : groups + members]
        table_ref, cb_ref, out_ref, near_t, far_t, values, far_values = refs[groups + members :]
        step = pl.program_id(0)

        @pl.when(step == 0)
        def _():
            values[0:ahead] = before_ref[:, cols:]
            values[ahead : ahead + tokens] = pair_ref[:, cols:]
            values[ahead + tokens : padded] = after_ref[:, cols:]
            for group in range(groups):
                block = jnp.concatenate([key_refs[group][m, 0] for m in range(members)], axis=0)
                size = members * ctx_rows
                far_t[:, group * size : (group + 1) * size] = block.T
                for member in range(members):
                    at = (group * members + member) * ctx_rows
                    far_values[at : at + ctx_rows] = value_refs[member][group, 0]
            fill = jnp.zeros((lanes - padded, cols), bf16)
            near_t[0, :, :ahead] = before_ref[:, :cols].T
            near_t[0, :, ahead : ahead + tokens] = pair_ref[:, :cols].T
            near_t[0, :, ahead + tokens :] = jnp.concatenate(
                [after_ref[:, :cols], fill], axis=0
            ).T
            near_t[1] = jnp.concatenate(
                [
                    before_ref[GRID_W:, :cols],
                    pair_ref[:, :cols],
                    after_ref[:, :cols],
                    fill,
                    jnp.zeros((GRID_W, cols), bf16),
                ],
                axis=0,
            ).T

        base = place_ref[0] * rows_dev
        lane = lax.broadcasted_iota(jnp.int32, (GRID_W, cols), 1)
        masks = [(lane >= h * HEAD_DIM) & (lane < (h + 1) * HEAD_DIM) for h in range(heads)]
        cb = cb_ref[...]
        spreads, nears, starts = [], [], []
        for r in range(per):
            actual = base + step * per + r
            start = jnp.clip(actual - REACH, 0, rows_all - WIN_ROWS)
            local = start - base + REACH
            offset = start - actual + WIN_ROWS - 1
            q = q_ref[r * GRID_W : (r + 1) * GRID_W]
            spread = jnp.concatenate(
                [jnp.where(mask, q, jnp.zeros_like(q)) for mask in masks], axis=0
            )
            spreads.append(spread)
            column = pl.multiple_of((local // 2) * 128, 128)
            keys_t = near_t[local % 2, :, pl.ds(column, near_keys)]
            bias_at = pl.multiple_of((offset // 2) * 128, 128)
            nears.append(
                jnp.dot(spread, keys_t, preferred_element_type=f32)
                + table_ref[offset % 2, :, pl.ds(bias_at, near_keys)]
            )
            starts.append(pl.multiple_of(local * GRID_W, GRID_W))
        for r in range(per):
            near = nears[r]
            far = jnp.dot(spreads[r], far_t[...], preferred_element_type=f32)
            top = jnp.maximum(
                jnp.max(near, axis=-1, keepdims=True), jnp.max(far, axis=-1, keepdims=True) + cb
            )
            near_exp = jnp.exp(near - top)
            far_exp = jnp.exp(far - (top - cb))
            total = jnp.sum(near_exp, axis=-1, keepdims=True) + jnp.sum(
                far_exp, axis=-1, keepdims=True
            )
            mixed = jnp.dot(
                near_exp.astype(bf16),
                values[pl.ds(starts[r], near_keys), :],
                preferred_element_type=f32,
            ) + jnp.dot(far_exp.astype(bf16), far_values[...], preferred_element_type=f32)
            mixed = mixed * (1.0 / total)
            result = jnp.where(masks[0], mixed[:GRID_W], 0.0)
            for h in range(1, heads):
                result = jnp.where(masks[h], mixed[h * GRID_W : (h + 1) * GRID_W], result)
            out_ref[r] = result.astype(bf16)

    far_spec = pl.BlockSpec((members, 1, ctx_rows, cols), lambda i: (0, sample, 0, 0))
    return pl.pallas_call(
        body,
        grid=(rows_dev // per,),
        in_specs=[
            pl.BlockSpec(memory_space=pltpu.SMEM),
            pl.BlockSpec((per * GRID_W, cols), lambda i: (i, 0)),
            whole(before.shape),
            whole(pair.shape),
            whole(after.shape),
        ]
        + [far_spec] * (groups + members)
        + [whole(table.shape), whole((queries, 1))],
        out_specs=pl.BlockSpec((per, GRID_W, cols), lambda i: (i, 0, 0)),
        out_shape=jax.ShapeDtypeStruct((rows_dev, GRID_W, cols), bf16),
        scratch_shapes=[
            pltpu.VMEM((2, cols, lanes), bf16),
            pltpu.VMEM((cols, ctx_count), bf16),
            pltpu.VMEM((padded, cols), bf16),
            pltpu.VMEM((ctx_count, cols), bf16),
        ],
        name="attend",
    )(place, query, before, pair, after, *ctx_keys, *ctx_values, table, ctx_bias)


def finish(attended, w_out, latent, gate, block):
    groups, rows, cols = attended.shape
    samples, tokens, width = latent.shape

    def body(att_ref, w_ref, latent_ref, gate_ref, out_ref):
        update = jnp.dot(att_ref[0], w_ref[:cols], preferred_element_type=jnp.float32)
        for group in range(1, groups):
            update += jnp.dot(
                att_ref[group],
                w_ref[group * cols : (group + 1) * cols],
                preferred_element_type=jnp.float32,
            )
        for s in range(samples):
            part = update[s * tokens : (s + 1) * tokens]
            mixed = latent_ref[s].astype(jnp.float32) + gate_ref[s : s + 1] * part
            out_ref[s] = mixed.astype(jnp.bfloat16)

    return pl.pallas_call(
        body,
        grid=(width // block,),
        in_specs=[
            whole(attended.shape),
            pl.BlockSpec((width, block), lambda i: (0, i)),
            pl.BlockSpec((samples, tokens, block), lambda i: (0, 0, i)),
            pl.BlockSpec((samples, block), lambda i: (0, i)),
        ],
        out_specs=pl.BlockSpec((samples, tokens, block), lambda i: (0, 0, i)),
        out_shape=jax.ShapeDtypeStruct(latent.shape, latent.dtype),
        name="finish",
    )(attended, w_out, latent, gate)


def shifted(axis, digits, digit, value):
    size_z, size_x = digits
    pairs = []
    for z in range(size_z):
        for x in range(size_x):
            to_z = (z + value) % size_z if digit == 0 else z
            to_x = (x + value) % size_x if digit == 1 else x
            pairs.append((z * size_x + x, to_z * size_x + to_x))
    return pairs


def everywhere(block, digits, order):
    for digit in order:
        block = [block] + [
            lax.ppermute(block, "sp", shifted("sp", digits, digit, value))
            for value in range(1, digits[digit])
        ]
        if digit != order[-1]:
            block = jnp.stack(block)
    return block


def on_device(
    latent,
    context,
    cond,
    ctx_cond,
    w_shift,
    w_scale,
    w_gate,
    norm_gain,
    w_query,
    w_key,
    w_value,
    w_out,
    rel_bias,
    ctx_bias,
):
    samples, tokens_dev, width = latent.shape
    local_cols = w_shift.shape[1]
    sp_index = lax.axis_index("sp")
    sp_size, tp_size = lax.axis_size("sp"), lax.axis_size("tp")
    digits = (4, sp_size // 4)
    place = jnp.full((1,), sp_index, jnp.int32)
    gathered = lax.all_gather(latent, "tp", axis=1, tiled=True)
    parts = modulation_parts(place, cond, ctx_cond[None], (w_shift, w_scale, w_gate), sp_size)
    parts, w_out_own = lax.optimization_barrier((parts, w_out))
    w_out_all = lax.all_gather(w_out_own, "tp", axis=0, tiled=True)
    summed = jnp.sum(lax.all_to_all(parts, "sp", 0, 0, tiled=True), axis=0)
    tiles = copy_for_each(summed, "tp")
    modulation = jnp.moveaxis(tiles, 0, 1).reshape(-1, width)
    every = samples + 1
    shift, scale = modulation[:every], modulation[every : 2 * every]
    gate = modulation[2 * every :]

    gain = norm_gain[None, :]
    table = bias_table(rel_bias)
    ctx_rows = context.shape[1]
    (ctx_pair,) = project(
        context.reshape(1, samples * ctx_rows, width),
        0,
        gain,
        shift[samples:],
        scale[samples:],
        (w_key, w_value),
        samples * ctx_rows,
        None,
    )
    ctx_keys = ctx_pair[:, :local_cols].reshape(samples, ctx_rows, local_cols)
    ctx_values = ctx_pair[:, local_cols:].reshape(samples, ctx_rows, local_cols)
    ctx_keys = everywhere(ctx_keys, digits, (1, 0))
    ctx_values = everywhere(ctx_values, digits, (0, 1))
    cb = jnp.repeat(ctx_bias, GRID_W)[:, None]
    up = [(i, i + 1) for i in range(sp_size - 1)]
    down = [(j, i) for i, j in up]
    attended = []
    for s in range(samples):
        pair, query, first, last = project(
            gathered,
            s,
            gain,
            shift[s : s + 1],
            scale[s : s + 1],
            (w_key, w_value, w_query),
            128,
            ((WIN_ROWS - REACH - 1) * GRID_W, REACH * GRID_W),
        )
        before = lax.ppermute(last, "sp", up)
        after = lax.ppermute(first, "sp", down)
        rows_all = pair.shape[0] // GRID_W * sp_size
        attended.append(
            attend(
                place, s, query, before, pair, after, ctx_keys, ctx_values, table, cb, rows_all, 2
            )
        )
    attended = jnp.concatenate(attended, axis=1)
    attended = lax.all_to_all(attended, "tp", 0, 0, tiled=True)
    return finish(attended, w_out_all, latent, gate, 256)


def solution(mesh):
    return jax.shard_map(
        on_device,
        mesh=mesh,
        in_specs=(
            P(None, ("sp", "tp"), None),
            P(None, "sp", None),
            P(),
            P(),
            P("sp", "tp"),
            P("sp", "tp"),
            P("sp", "tp"),
            P(),
            P(None, "tp"),
            P(None, "tp"),
            P(None, "tp"),
            P("tp", None),
            P("tp", None, None),
            P("tp"),
        ),
        out_specs=P(None, ("sp", "tp"), None),
        check_vma=False,
    )
```

```python
import jax
import jax.numpy as jnp
from jax import lax
from jax.experimental import pallas as pl
from jax.experimental.pallas import tpu as pltpu
from jax.sharding import PartitionSpec as P


HEAD_DIM = 64
GRID_W = 64
WIN_ROWS = 8
WIN_COLS = 16
EPSILON = 1e-06
MASKED = -1e30
REACH = WIN_ROWS // 2
BIAS_BLOCKS = 7


def copy_for_each(shard, axis):
    length = lax.axis_size(axis)
    return lax.all_to_all(
        jnp.broadcast_to(shard[None], (length, *shard.shape)), axis, 0, 0, tiled=True
    )


def silu_rows(values):
    return jax.nn.silu(values.astype(jnp.float32)).astype(jnp.bfloat16)


def modulation_parts(place, cond, ctx_cond, weights, copies):
    samples = cond.shape[0]
    rows, cols = weights[0].shape

    def body(place_ref, cond_ref, ctx_ref, shift_ref, scale_ref, gate_ref, out_ref):
        at = pl.multiple_of(place_ref[0] * rows, rows)
        ada = silu_rows(cond_ref[:, pl.ds(at, rows)])
        ada_ctx = silu_rows(ctx_ref[:, pl.ds(at, rows)])
        both = jnp.concatenate([ada.astype(jnp.float32), ada_ctx.astype(jnp.float32)], axis=0)
        both = both.astype(jnp.bfloat16)
        result = jnp.concatenate(
            [
                jnp.dot(both, shift_ref[...], preferred_element_type=jnp.float32),
                jnp.dot(both, scale_ref[...], preferred_element_type=jnp.float32),
                jnp.dot(ada, gate_ref[...], preferred_element_type=jnp.float32),
            ],
            axis=0,
        )
        for copy in range(copies):
            out_ref[copy] = result

    return pl.pallas_call(
        body,
        in_specs=[pl.BlockSpec(memory_space=pltpu.SMEM)]
        + [pl.BlockSpec(memory_space=pltpu.VMEM)] * 5,
        out_shape=jax.ShapeDtypeStruct((copies, 3 * samples + 2, cols), jnp.float32),
        name="modulation_parts",
    )(place, cond, ctx_cond, *weights)


def whole(shape):
    return pl.BlockSpec(shape, lambda *_: (0,) * len(shape))


def modulation_row(tiles, row):
    return jnp.concatenate([tiles[tile, row : row + 1, :] for tile in range(tiles.shape[0])], axis=1)


def project(rows, gain, modulation, weights, row_of, block, ends):
    samples, count, width = rows.shape
    every = modulation.shape[1] // 3 + 1
    cols = weights[0].shape[1]
    first, last = ends if ends else (0, 0)
    steps = count // block

    def body(rows_ref, gain_ref, tiles_ref, *refs):
        weight_refs, out_refs = refs[: len(weights)], refs[len(weights) : -2]
        factor_ref, shift_ref = refs[-2:]
        sample, step = pl.program_id(0), pl.program_id(1)

        for number in range(samples):

            @pl.when((sample == number) & (step == 0))
            def _(number=number):
                row = row_of + number
                factor_ref[...] = gain_ref[...] * (1.0 + modulation_row(tiles_ref, every + row))
                shift_ref[...] = modulation_row(tiles_ref, row)

        floats = rows_ref[0].astype(jnp.float32)
        inverse = lax.rsqrt(jnp.mean(floats * floats, axis=-1, keepdims=True) + EPSILON)
        hidden = (floats * inverse * factor_ref[...] + shift_ref[...]).astype(jnp.bfloat16)
        pair = [
            jnp.dot(hidden, ref[...], preferred_element_type=jnp.float32).astype(jnp.bfloat16)
            for ref in weight_refs[:2]
        ]
        if not ends:
            out_refs[0][0] = pair[0]
            out_refs[1][0] = pair[1]
            return
        out_refs[0][0, :, :cols] = pair[0]
        out_refs[0][0, :, cols:] = pair[1]
        query = jnp.dot(hidden, weight_refs[2][...], preferred_element_type=jnp.float32)
        query = query.astype(jnp.bfloat16).astype(jnp.float32) * HEAD_DIM**-0.5
        out_refs[1][0] = query.astype(jnp.bfloat16)
        for number in range(steps):
            low = number * block
            for out_ref, start, stop in (
                (out_refs[2], 0, first),
                (out_refs[3], count - last, count),
            ):
                lo, hi = max(low, start), min(low + block, stop)
                if lo < hi:

                    @pl.when(step == number)
                    def _(out_ref=out_ref, start=start, lo=lo, hi=hi, low=low):
                        for index in range(2):
                            out_ref[
                                0, lo - start : hi - start, index * cols : (index + 1) * cols
                            ] = pair[index][lo - low : hi - low]

    def blocks(size):
        return pl.BlockSpec((1, block, size), lambda s, i: (s, i, 0))

    if ends:
        out_specs = [blocks(2 * cols), blocks(cols)]
        out_shape = [(samples, count, 2 * cols), (samples, count, cols)]
        for length in ends:
            out_specs += [pl.BlockSpec((1, length, 2 * cols), lambda s, i: (s, 0, 0))]
            out_shape += [(samples, length, 2 * cols)]
    else:
        out_specs = [blocks(cols)] * 2
        out_shape = [(samples, count, cols)] * 2
    return pl.pallas_call(
        body,
        grid=(samples, steps),
        in_specs=[blocks(width), whole((1, width)), whole(modulation.shape)]
        + [whole(weight.shape) for weight in weights],
        out_specs=out_specs,
        out_shape=[jax.ShapeDtypeStruct(shape, jnp.bfloat16) for shape in out_shape],
        scratch_shapes=[pltpu.VMEM((1, width), jnp.float32)] * 2,
        name="project",
    )(rows, gain, modulation, *weights)


def bias_table(rel_bias):
    heads, offsets, spread = rel_bias.shape
    slots = 2 * BIAS_BLOCKS + 2
    padded = jnp.pad(rel_bias, ((0, 0), (0, slots - offsets), (0, 128 - spread)))
    padded = padded.reshape(heads * slots, 128)

    def body(rel_ref, out_ref):
        query = lax.broadcasted_iota(jnp.int32, (GRID_W, 128), 0)
        lane = lax.broadcasted_iota(jnp.int32, (GRID_W, 128), 1)
        low = lane < GRID_W
        key = jnp.where(low, lane, lane - GRID_W)
        start = jnp.clip(query - WIN_COLS // 2, 0, GRID_W - WIN_COLS)
        inside = (key >= start) & (key < start + WIN_COLS)

        def diagonal(head, slot, move):
            row = jnp.broadcast_to(rel_ref[pl.ds(head * slots + slot, 1), :], (GRID_W, 128))
            return pltpu.roll(row, (128 - (WIN_COLS - 1) + move) % 128, 1, stride=1, stride_axis=0)

        for parity in range(2):
            for head in range(heads):
                for block in range(BIAS_BLOCKS):
                    slot = 2 * block + parity
                    both = jnp.where(
                        low, diagonal(head, slot, 0), diagonal(head, slot + 1, GRID_W)
                    )
                    out_ref[
                        parity, head * GRID_W : (head + 1) * GRID_W, block * 128 : (block + 1) * 128
                    ] = jnp.where(inside, both, MASKED)

    return pl.pallas_call(
        body,
        out_shape=jax.ShapeDtypeStruct((2, heads * GRID_W, BIAS_BLOCKS * 128), jnp.float32),
        name="bias_table",
    )(padded)


def attend(place, query, before, pair, after, ctx_keys, ctx_values, table, ctx_bias, rows_all, per):
    samples, tokens, cols = query.shape
    heads = cols // HEAD_DIM
    rows_dev = tokens // GRID_W
    near_keys = WIN_ROWS * GRID_W
    ahead, behind = before.shape[1], after.shape[1]
    padded = ahead + tokens + behind
    lanes = -(-padded // 128) * 128
    groups, members, _, ctx_rows, _ = (len(ctx_keys), *ctx_keys[0].shape)
    ctx_count = groups * members * ctx_rows
    queries = heads * GRID_W
    bf16, f32 = jnp.bfloat16, jnp.float32

    def body(place_ref, q_ref, before_ref, pair_ref, after_ref, *refs):
        key_refs, value_refs = refs[:groups], refs[groups : groups + members]
        table_ref, cb_ref, out_ref, near_t, far_t, values, far_values = refs[groups + members :]
        step = pl.program_id(1)

        @pl.when(step == 0)
        def _():
            values[0:ahead] = before_ref[0, :, cols:]
            values[ahead : ahead + tokens] = pair_ref[0, :, cols:]
            values[ahead + tokens : padded] = after_ref[0, :, cols:]
            for group in range(groups):
                block = jnp.concatenate([key_refs[group][m, 0] for m in range(members)], axis=0)
                size = members * ctx_rows
                far_t[:, group * size : (group + 1) * size] = block.T
                for member in range(members):
                    at = (group * members + member) * ctx_rows
                    far_values[at : at + ctx_rows] = value_refs[member][group, 0]
            fill = jnp.zeros((lanes - padded, cols), bf16)
            near_t[0, :, :ahead] = before_ref[0, :, :cols].T
            near_t[0, :, ahead : ahead + tokens] = pair_ref[0, :, :cols].T
            near_t[0, :, ahead + tokens :] = jnp.concatenate(
                [after_ref[0, :, :cols], fill], axis=0
            ).T
            near_t[1] = jnp.concatenate(
                [
                    before_ref[0, GRID_W:, :cols],
                    pair_ref[0, :, :cols],
                    after_ref[0, :, :cols],
                    fill,
                    jnp.zeros((GRID_W, cols), bf16),
                ],
                axis=0,
            ).T

        base = place_ref[0] * rows_dev
        lane = lax.broadcasted_iota(jnp.int32, (GRID_W, cols), 1)
        masks = [(lane >= h * HEAD_DIM) & (lane < (h + 1) * HEAD_DIM) for h in range(heads)]
        cb = cb_ref[...]
        spreads, nears, starts = [], [], []
        for r in range(per):
            actual = base + step * per + r
            start = jnp.clip(actual - REACH, 0, rows_all - WIN_ROWS)
            local = start - base + REACH
            offset = start - actual + WIN_ROWS - 1
            q = q_ref[0, r * GRID_W : (r + 1) * GRID_W]
            spread = jnp.concatenate(
                [jnp.where(mask, q, jnp.zeros_like(q)) for mask in masks], axis=0
            )
            spreads.append(spread)
            column = pl.multiple_of((local // 2) * 128, 128)
            keys_t = near_t[local % 2, :, pl.ds(column, near_keys)]
            bias_at = pl.multiple_of((offset // 2) * 128, 128)
            nears.append(
                jnp.dot(spread, keys_t, preferred_element_type=f32)
                + table_ref[offset % 2, :, pl.ds(bias_at, near_keys)]
            )
            starts.append(pl.multiple_of(local * GRID_W, GRID_W))
        for r in range(per):
            near = nears[r]
            far = jnp.dot(spreads[r], far_t[...], preferred_element_type=f32)
            top = jnp.maximum(
                jnp.max(near, axis=-1, keepdims=True), jnp.max(far, axis=-1, keepdims=True) + cb
            )
            near_exp = jnp.exp(near - top)
            far_exp = jnp.exp(far - (top - cb))
            total = jnp.sum(near_exp, axis=-1, keepdims=True) + jnp.sum(
                far_exp, axis=-1, keepdims=True
            )
            mixed = jnp.dot(
                near_exp.astype(bf16),
                values[pl.ds(starts[r], near_keys), :],
                preferred_element_type=f32,
            ) + jnp.dot(far_exp.astype(bf16), far_values[...], preferred_element_type=f32)
            mixed = mixed * (1.0 / total)
            result = jnp.where(masks[0], mixed[:GRID_W], 0.0)
            for h in range(1, heads):
                result = jnp.where(masks[h], mixed[h * GRID_W : (h + 1) * GRID_W], result)
            out_ref[r, 0] = result.astype(bf16)

    def of_sample(array):
        return pl.BlockSpec((1, *array.shape[1:]), lambda s, i: (s, 0, 0))

    far_spec = pl.BlockSpec((members, 1, ctx_rows, cols), lambda s, i: (0, s, 0, 0))
    return pl.pallas_call(
        body,
        grid=(samples, rows_dev // per),
        in_specs=[
            pl.BlockSpec(memory_space=pltpu.SMEM),
            pl.BlockSpec((1, per * GRID_W, cols), lambda s, i: (s, i, 0)),
            of_sample(before),
            of_sample(pair),
            of_sample(after),
        ]
        + [far_spec] * (groups + members)
        + [whole(table.shape), whole((queries, 1))],
        out_specs=pl.BlockSpec((per, 1, GRID_W, cols), lambda s, i: (i, s, 0, 0)),
        out_shape=jax.ShapeDtypeStruct((rows_dev, samples, GRID_W, cols), bf16),
        scratch_shapes=[
            pltpu.VMEM((2, cols, lanes), bf16),
            pltpu.VMEM((cols, ctx_count), bf16),
            pltpu.VMEM((padded, cols), bf16),
            pltpu.VMEM((ctx_count, cols), bf16),
        ],
        name="attend",
    )(place, query, before, pair, after, *ctx_keys, *ctx_values, table, ctx_bias)


def finish(attended, w_out, latent, modulation):
    groups, _, _ = attended.shape
    samples, tokens, width = latent.shape
    block = modulation.shape[2]
    first = modulation.shape[1] - samples

    def body(att_ref, w_ref, latent_ref, tile_ref, out_ref):
        everything = jnp.concatenate([att_ref[group] for group in range(groups)], axis=1)
        update = jnp.dot(everything, w_ref[...], preferred_element_type=jnp.float32)
        for s in range(samples):
            gate = tile_ref[0, first + s : first + s + 1, :]
            part = update[s * tokens : (s + 1) * tokens]
            out_ref[s] = (latent_ref[s].astype(jnp.float32) + gate * part).astype(jnp.bfloat16)

    return pl.pallas_call(
        body,
        grid=(width // block,),
        in_specs=[
            whole(attended.shape),
            pl.BlockSpec((width, block), lambda i: (0, i)),
            pl.BlockSpec((samples, tokens, block), lambda i: (0, 0, i)),
            pl.BlockSpec((1, *modulation.shape[1:]), lambda i: (i, 0, 0)),
        ],
        out_specs=pl.BlockSpec((samples, tokens, block), lambda i: (0, 0, i)),
        out_shape=jax.ShapeDtypeStruct(latent.shape, latent.dtype),
        name="finish",
    )(attended, w_out, latent, modulation)


def shifted(size, side, stride, value):
    span = side * stride
    return [(i, i // span * span + (i + value * stride) % span) for i in range(size)]


def from_line(block, axis, side, stride):
    size = lax.axis_size(axis)
    return [block] + [
        lax.ppermute(block, axis, shifted(size, side, stride, value)) for value in range(1, side)
    ]


def computation(
    latent,
    context,
    cond,
    ctx_cond,
    w_shift,
    w_scale,
    w_gate,
    norm_gain,
    w_query,
    w_key,
    w_value,
    w_out,
    rel_bias,
    ctx_bias,
):
    samples, tokens_dev, width = latent.shape
    local_cols = w_shift.shape[1]
    sp_index = lax.axis_index("sp")
    sp_size, tp_size = lax.axis_size("sp"), lax.axis_size("tp")
    place = jnp.full((1,), sp_index, jnp.int32)
    gathered = lax.all_gather(latent, "tp", axis=1, tiled=True)
    parts = modulation_parts(place, cond, ctx_cond[None], (w_shift, w_scale, w_gate), sp_size)
    parts, w_out_own = lax.optimization_barrier((parts, w_out))
    w_out_all = lax.all_gather(w_out_own, "tp", axis=0, tiled=True)
    table = bias_table(rel_bias)
    cb = jnp.repeat(ctx_bias, GRID_W)[:, None]
    summed = jnp.sum(lax.all_to_all(parts, "sp", 0, 0, tiled=True), axis=0)
    summed, table, cb = lax.optimization_barrier((summed, table, cb))
    modulation = copy_for_each(summed, "tp")

    gain = norm_gain[None, :]
    ctx_rows = context.shape[1]
    ctx_keys, ctx_values = project(
        context.reshape(1, samples * ctx_rows, width),
        gain,
        modulation,
        (w_key, w_value),
        samples,
        samples * ctx_rows,
        None,
    )
    ctx_keys = ctx_keys.reshape(samples, ctx_rows, local_cols)
    ctx_values = ctx_values.reshape(samples, ctx_rows, local_cols)
    ctx_keys = jnp.stack(from_line(ctx_keys, "sp", 4, 1))
    ctx_values = jnp.stack(from_line(ctx_values, "sp", 4, 4))
    gathered, ctx_keys, ctx_values = lax.optimization_barrier((gathered, ctx_keys, ctx_values))
    ctx_keys = from_line(ctx_keys, "sp", 4, 4)
    ctx_values = from_line(ctx_values, "sp", 4, 1)
    up = [(i, i + 1) for i in range(sp_size - 1)]
    down = [(j, i) for i, j in up]
    pair, query, first, last = project(
        gathered,
        gain,
        modulation,
        (w_key, w_value, w_query),
        0,
        256,
        ((WIN_ROWS - REACH - 1) * GRID_W, REACH * GRID_W),
    )
    before = lax.ppermute(last, "sp", up)
    after = lax.ppermute(first, "sp", down)
    rows_all = pair.shape[1] // GRID_W * sp_size
    attended = attend(
        place, query, before, pair, after, ctx_keys, ctx_values, table, cb, rows_all, 2
    )
    attended = attended.reshape(tp_size, samples * tokens_dev, local_cols)
    attended = lax.all_to_all(attended, "tp", 0, 0, tiled=True)
    return finish(attended, w_out_all, latent, modulation)


def solution(mesh):
    return jax.shard_map(
        computation,
        mesh=mesh,
        in_specs=(
            P(None, ("sp", "tp"), None),
            P(None, "sp", None),
            P(),
            P(),
            P("sp", "tp"),
            P("sp", "tp"),
            P("sp", "tp"),
            P(),
            P(None, "tp"),
            P(None, "tp"),
            P(None, "tp"),
            P("tp", None),
            P("tp", None, None),
            P("tp"),
        ),
        out_specs=P(None, ("sp", "tp"), None),
        check_vma=False,
    )
```

```python
import jax
import jax.numpy as jnp
from jax import lax
from jax.experimental import pallas as pl
from jax.experimental.pallas import tpu as pltpu
from jax.sharding import PartitionSpec as P

HEAD_DIM = 64
GRID_W = 64
WIN_ROWS = 8
WIN_COLS = 16
EPSILON = 1e-06
MASKED = -1e30
REACH = WIN_ROWS // 2
BIAS_BLOCKS = 7


def copy_for_each(shard, axis):
    length = lax.axis_size(axis)
    return lax.all_to_all(
        jnp.broadcast_to(shard[None], (length, *shard.shape)), axis, 0, 0, tiled=True
    )


def silu_rows(values):
    return jax.nn.silu(values.astype(jnp.float32)).astype(jnp.bfloat16)


def modulation_parts(place, cond, ctx_cond, weights, copies):
    samples = cond.shape[0]
    rows, cols = weights[0].shape

    def body(place_ref, cond_ref, ctx_ref, shift_ref, scale_ref, gate_ref, out_ref):
        at = pl.multiple_of(place_ref[0] * rows, rows)
        ada = silu_rows(cond_ref[:, pl.ds(at, rows)])
        ada_ctx = silu_rows(ctx_ref[:, pl.ds(at, rows)])
        both = jnp.concatenate([ada.astype(jnp.float32), ada_ctx.astype(jnp.float32)], axis=0)
        both = both.astype(jnp.bfloat16)
        result = jnp.concatenate(
            [
                jnp.dot(both, shift_ref[...], preferred_element_type=jnp.float32),
                jnp.dot(both, scale_ref[...], preferred_element_type=jnp.float32),
                jnp.dot(ada, gate_ref[...], preferred_element_type=jnp.float32),
            ],
            axis=0,
        )
        for copy in range(copies):
            out_ref[copy] = result

    return pl.pallas_call(
        body,
        in_specs=[pl.BlockSpec(memory_space=pltpu.SMEM)]
        + [pl.BlockSpec(memory_space=pltpu.VMEM)] * 5,
        out_shape=jax.ShapeDtypeStruct((copies, 3 * samples + 2, cols), jnp.float32),
        name="modulation_parts",
    )(place, cond, ctx_cond, *weights)


def whole(shape):
    return pl.BlockSpec(shape, lambda *_: (0,) * len(shape))


def modulation_row(tiles, row):
    return jnp.concatenate([tiles[tile, row : row + 1, :] for tile in range(tiles.shape[0])], axis=1)


def project(rows, gain, modulation, weights, row_of, block, ends, copies=0, copy_samples=1):
    samples, count, width = rows.shape
    every = modulation.shape[1] // 3 + 1
    cols = weights[0].shape[1]
    first, last = ends if ends else (0, 0)
    steps = count // block

    def body(rows_ref, gain_ref, tiles_ref, *refs):
        weight_refs, out_refs = refs[: len(weights)], refs[len(weights) : -2]
        factor_ref, shift_ref = refs[-2:]
        sample, step = pl.program_id(0), pl.program_id(1)

        for number in range(samples):

            @pl.when((sample == number) & (step == 0))
            def _(number=number):
                row = row_of + number
                factor_ref[...] = gain_ref[...] * (1.0 + modulation_row(tiles_ref, every + row))
                shift_ref[...] = modulation_row(tiles_ref, row)

        floats = rows_ref[0].astype(jnp.float32)
        inverse = lax.rsqrt(jnp.mean(floats * floats, axis=-1, keepdims=True) + EPSILON)
        hidden = (floats * inverse * factor_ref[...] + shift_ref[...]).astype(jnp.bfloat16)
        pair = [
            jnp.dot(hidden, ref[...], preferred_element_type=jnp.float32).astype(jnp.bfloat16)
            for ref in weight_refs[:2]
        ]
        if not ends:
            for copy in range(copies):
                for number in range(copy_samples):
                    size = block // copy_samples
                    low = number * size
                    out_refs[0][copy, number, :, :cols] = pair[0][low : low + size]
                    out_refs[0][copy, number, :, cols:] = pair[1][low : low + size]
            return
        out_refs[0][0, :, :cols] = pair[0]
        out_refs[0][0, :, cols:] = pair[1]
        query = jnp.dot(hidden, weight_refs[2][...], preferred_element_type=jnp.float32)
        query = query.astype(jnp.bfloat16).astype(jnp.float32) * HEAD_DIM**-0.5
        out_refs[1][0] = query.astype(jnp.bfloat16)
        for number in range(steps):
            low = number * block
            for out_ref, start, stop in (
                (out_refs[2], 0, first),
                (out_refs[3], count - last, count),
            ):
                lo, hi = max(low, start), min(low + block, stop)
                if lo < hi:

                    @pl.when(step == number)
                    def _(out_ref=out_ref, start=start, lo=lo, hi=hi, low=low):
                        for index in range(2):
                            out_ref[
                                0, lo - start : hi - start, index * cols : (index + 1) * cols
                            ] = pair[index][lo - low : hi - low]

    def blocks(size):
        return pl.BlockSpec((1, block, size), lambda s, i: (s, i, 0))

    if ends:
        out_specs = [blocks(2 * cols), blocks(cols)]
        out_shape = [(samples, count, 2 * cols), (samples, count, cols)]
        for length in ends:
            out_specs += [pl.BlockSpec((1, length, 2 * cols), lambda s, i: (s, 0, 0))]
            out_shape += [(samples, length, 2 * cols)]
    else:
        out_shape = [(copies, copy_samples, count // copy_samples, 2 * cols)]
        out_specs = [whole(out_shape[0])]
    return pl.pallas_call(
        body,
        grid=(samples, steps),
        in_specs=[blocks(width), whole((1, width)), whole(modulation.shape)]
        + [whole(weight.shape) for weight in weights],
        out_specs=out_specs,
        out_shape=[jax.ShapeDtypeStruct(shape, jnp.bfloat16) for shape in out_shape],
        scratch_shapes=[pltpu.VMEM((1, width), jnp.float32)] * 2,
        name="project",
    )(rows, gain, modulation, *weights)


def bias_table(rel_bias):
    heads, offsets, spread = rel_bias.shape
    slots = 2 * BIAS_BLOCKS + 2
    padded = jnp.pad(rel_bias, ((0, 0), (0, slots - offsets), (0, 128 - spread)))
    padded = padded.reshape(heads * slots, 128)

    def body(rel_ref, out_ref):
        query = lax.broadcasted_iota(jnp.int32, (GRID_W, 128), 0)
        lane = lax.broadcasted_iota(jnp.int32, (GRID_W, 128), 1)
        low = lane < GRID_W
        key = jnp.where(low, lane, lane - GRID_W)
        start = jnp.clip(query - WIN_COLS // 2, 0, GRID_W - WIN_COLS)
        inside = (key >= start) & (key < start + WIN_COLS)

        def diagonal(head, slot, move):
            row = jnp.broadcast_to(rel_ref[pl.ds(head * slots + slot, 1), :], (GRID_W, 128))
            return pltpu.roll(row, (128 - (WIN_COLS - 1) + move) % 128, 1, stride=1, stride_axis=0)

        for parity in range(2):
            for head in range(heads):
                for block in range(BIAS_BLOCKS):
                    slot = 2 * block + parity
                    both = jnp.where(
                        low, diagonal(head, slot, 0), diagonal(head, slot + 1, GRID_W)
                    )
                    out_ref[
                        parity, head * GRID_W : (head + 1) * GRID_W, block * 128 : (block + 1) * 128
                    ] = jnp.where(inside, both, MASKED)

    return pl.pallas_call(
        body,
        out_shape=jax.ShapeDtypeStruct((2, heads * GRID_W, BIAS_BLOCKS * 128), jnp.float32),
        name="bias_table",
    )(padded)


def head_masks(cols):
    lane = lax.broadcasted_iota(jnp.int32, (GRID_W, cols), 1)
    return [(lane >= low) & (lane < low + HEAD_DIM) for low in range(0, cols, HEAD_DIM)]


def spread_heads(query, masks):
    return jnp.concatenate(
        [jnp.where(mask, query, jnp.zeros_like(query)) for mask in masks], axis=0
    )


def gather_heads(values, masks):
    result = jnp.where(masks[0], values[:GRID_W], 0.0)
    for h in range(1, len(masks)):
        result = jnp.where(masks[h], values[h * GRID_W : (h + 1) * GRID_W], result)
    return result


def weighed(scores, values, masks):
    top = jnp.max(scores, axis=-1, keepdims=True)
    exps = jnp.exp(scores - top)
    total = jnp.sum(exps, axis=-1, keepdims=True)
    mixed = jnp.dot(exps.astype(jnp.bfloat16), values, preferred_element_type=jnp.float32)
    return [gather_heads(array, masks) for array in (mixed, top, total)]


def attend_near(place, query, before, pair, after, table, rows_all, per):
    samples, tokens, cols = query.shape
    rows_dev = tokens // GRID_W
    near_keys = WIN_ROWS * GRID_W
    ahead, behind = before.shape[1], after.shape[1]
    padded = ahead + tokens + behind
    lanes = -(-padded // 128) * 128
    bf16, f32 = jnp.bfloat16, jnp.float32

    def body(place_ref, q_ref, before_ref, pair_ref, after_ref, table_ref, *refs):
        out_refs, (near_t, values) = refs[:3], refs[3:]
        step = pl.program_id(1)

        @pl.when(step == 0)
        def _():
            values[0:ahead] = before_ref[0, :, cols:]
            values[ahead : ahead + tokens] = pair_ref[0, :, cols:]
            values[ahead + tokens : padded] = after_ref[0, :, cols:]
            fill = jnp.zeros((lanes - padded, cols), bf16)
            near_t[0, :, :ahead] = before_ref[0, :, :cols].T
            near_t[0, :, ahead : ahead + tokens] = pair_ref[0, :, :cols].T
            near_t[0, :, ahead + tokens :] = jnp.concatenate(
                [after_ref[0, :, :cols], fill], axis=0
            ).T
            near_t[1] = jnp.concatenate(
                [
                    before_ref[0, GRID_W:, :cols],
                    pair_ref[0, :, :cols],
                    after_ref[0, :, :cols],
                    fill,
                    jnp.zeros((GRID_W, cols), bf16),
                ],
                axis=0,
            ).T

        base = place_ref[0] * rows_dev
        masks = head_masks(cols)
        scores, starts = [], []
        for r in range(per):
            actual = base + step * per + r
            start = jnp.clip(actual - REACH, 0, rows_all - WIN_ROWS)
            local = start - base + REACH
            offset = start - actual + WIN_ROWS - 1
            spread = spread_heads(q_ref[0, r * GRID_W : (r + 1) * GRID_W], masks)
            column = pl.multiple_of((local // 2) * 128, 128)
            keys_t = near_t[local % 2, :, pl.ds(column, near_keys)]
            bias_at = pl.multiple_of((offset // 2) * 128, 128)
            scores.append(
                jnp.dot(spread, keys_t, preferred_element_type=f32)
                + table_ref[offset % 2, :, pl.ds(bias_at, near_keys)]
            )
            starts.append(pl.multiple_of(local * GRID_W, GRID_W))
        for r in range(per):
            parts = weighed(scores[r], values[pl.ds(starts[r], near_keys), :], masks)
            for out_ref, part in zip(out_refs, parts):
                out_ref[0, r * GRID_W : (r + 1) * GRID_W] = part

    def of_sample(array):
        return pl.BlockSpec((1, *array.shape[1:]), lambda s, i: (s, 0, 0))

    rows_spec = pl.BlockSpec((1, per * GRID_W, cols), lambda s, i: (s, i, 0))
    return pl.pallas_call(
        body,
        grid=(samples, rows_dev // per),
        in_specs=[
            pl.BlockSpec(memory_space=pltpu.SMEM),
            rows_spec,
            of_sample(before),
            of_sample(pair),
            of_sample(after),
            whole(table.shape),
        ],
        out_specs=[rows_spec] * 3,
        out_shape=[jax.ShapeDtypeStruct((samples, tokens, cols), f32)] * 3,
        scratch_shapes=[
            pltpu.VMEM((2, cols, lanes), bf16),
            pltpu.VMEM((padded, cols), bf16),
        ],
        name="attend_near",
    )(place, query, before, pair, after, table)


def attend_far(query, ctx_pair, ctx_bias, near, per):
    samples, tokens, cols = query.shape
    rows_dev = tokens // GRID_W
    owners, _, ctx_rows, _ = ctx_pair.shape
    ctx_count = owners * ctx_rows
    bf16, f32 = jnp.bfloat16, jnp.float32

    def body(q_ref, ctx_ref, cb_ref, mixed_ref, top_ref, total_ref, out_ref, far_t, values):
        @pl.when(pl.program_id(1) == 0)
        def _():
            for owner in range(owners):
                values[owner * ctx_rows : (owner + 1) * ctx_rows] = ctx_ref[owner, 0, :, cols:]
            for first in range(0, owners, 2):
                block = jnp.concatenate(
                    [ctx_ref[first, 0, :, :cols], ctx_ref[first + 1, 0, :, :cols]], axis=0
                )
                far_t[:, first * ctx_rows : (first + 2) * ctx_rows] = block.T

        masks = head_masks(cols)
        scores = [
            jnp.dot(
                spread_heads(q_ref[0, r * GRID_W : (r + 1) * GRID_W], masks),
                far_t[...],
                preferred_element_type=f32,
            )
            for r in range(per)
        ]
        for r in range(per):
            mixed, top, total = weighed(scores[r], values[...], masks)
            at = slice(r * GRID_W, (r + 1) * GRID_W)
            top = top + cb_ref[...]
            near_top = top_ref[0, at]
            highest = jnp.maximum(top, near_top)
            far_part = jnp.exp(top - highest)
            near_part = jnp.exp(near_top - highest)
            total = total * far_part + total_ref[0, at] * near_part
            mixed = mixed * far_part + mixed_ref[0, at] * near_part
            out_ref[r, 0] = (mixed / total).astype(bf16)

    rows_spec = pl.BlockSpec((1, per * GRID_W, cols), lambda s, i: (s, i, 0))
    return pl.pallas_call(
        body,
        grid=(samples, rows_dev // per),
        in_specs=[
            rows_spec,
            pl.BlockSpec((owners, 1, ctx_rows, 2 * cols), lambda s, i: (0, s, 0, 0)),
            whole(ctx_bias.shape),
        ]
        + [rows_spec] * 3,
        out_specs=pl.BlockSpec((per, 1, GRID_W, cols), lambda s, i: (i, s, 0, 0)),
        out_shape=jax.ShapeDtypeStruct((rows_dev, samples, GRID_W, cols), bf16),
        scratch_shapes=[
            pltpu.VMEM((cols, ctx_count), bf16),
            pltpu.VMEM((ctx_count, cols), bf16),
        ],
        name="attend_far",
    )(query, ctx_pair, ctx_bias, *near)


def finish(attended, w_out, latent, modulation):
    groups, rows, cols = attended.shape
    samples, tokens, width = latent.shape
    block = modulation.shape[2]
    first = modulation.shape[1] - samples

    def body(att_ref, w_ref, latent_ref, tile_ref, out_ref):
        everything = jnp.concatenate([att_ref[group] for group in range(groups)], axis=1)
        update = jnp.dot(everything, w_ref[...], preferred_element_type=jnp.float32)
        for s in range(samples):
            gate = tile_ref[0, first + s : first + s + 1, :]
            part = update[s * tokens : (s + 1) * tokens]
            out_ref[s] = (latent_ref[s].astype(jnp.float32) + gate * part).astype(jnp.bfloat16)

    return pl.pallas_call(
        body,
        grid=(width // block,),
        in_specs=[
            whole(attended.shape),
            pl.BlockSpec((width, block), lambda i: (0, i)),
            pl.BlockSpec((samples, tokens, block), lambda i: (0, 0, i)),
            pl.BlockSpec((1, *modulation.shape[1:]), lambda i: (i, 0, 0)),
        ],
        out_specs=pl.BlockSpec((samples, tokens, block), lambda i: (0, 0, i)),
        out_shape=jax.ShapeDtypeStruct(latent.shape, latent.dtype),
        name="finish",
    )(attended, w_out, latent, modulation)


def on_device(
    latent,
    context,
    cond,
    ctx_cond,
    w_shift,
    w_scale,
    w_gate,
    norm_gain,
    w_query,
    w_key,
    w_value,
    w_out,
    rel_bias,
    ctx_bias,
):
    samples, tokens_dev, width = latent.shape
    local_cols = w_shift.shape[1]
    sp_index = lax.axis_index("sp")
    sp_size, tp_size = lax.axis_size("sp"), lax.axis_size("tp")
    place = jnp.full((1,), sp_index, jnp.int32)
    gathered = lax.all_gather(latent, "tp", axis=1, tiled=True)
    parts = modulation_parts(place, cond, ctx_cond[None], (w_shift, w_scale, w_gate), sp_size)
    parts, w_out_own = lax.optimization_barrier((parts, w_out))
    w_out_all = lax.all_gather(w_out_own, "tp", axis=0, tiled=True)
    table = bias_table(rel_bias)
    cb = jnp.repeat(ctx_bias, HEAD_DIM)[None, :]
    summed = jnp.sum(lax.all_to_all(parts, "sp", 0, 0, tiled=True), axis=0)
    summed, table, cb = lax.optimization_barrier((summed, table, cb))
    modulation = copy_for_each(summed, "tp")

    gain = norm_gain[None, :]
    ctx_rows = context.shape[1]
    (ctx_pair,) = project(
        context.reshape(1, samples * ctx_rows, width),
        gain,
        modulation,
        (w_key, w_value),
        samples,
        samples * ctx_rows,
        None,
        sp_size,
        samples,
    )
    ctx_pair = lax.all_to_all(ctx_pair, "sp", 0, 0, tiled=True)
    up = [(i, i + 1) for i in range(sp_size - 1)]
    down = [(j, i) for i, j in up]
    pair, query, first, last = project(
        gathered,
        gain,
        modulation,
        (w_key, w_value, w_query),
        0,
        256,
        ((WIN_ROWS - REACH - 1) * GRID_W, REACH * GRID_W),
    )
    before = lax.ppermute(last, "sp", up)
    after = lax.ppermute(first, "sp", down)
    rows_all = pair.shape[1] // GRID_W * sp_size
    near = attend_near(place, query, before, pair, after, table, rows_all, 2)
    attended = attend_far(query, ctx_pair, cb, near, 2)
    attended = attended.reshape(tp_size, samples * tokens_dev, local_cols)
    attended = lax.all_to_all(attended, "tp", 0, 0, tiled=True)
    return finish(attended, w_out_all, latent, modulation)


def solution(mesh):
    return jax.shard_map(
        on_device,
        mesh=mesh,
        in_specs=(
            P(None, ("sp", "tp"), None),
            P(None, "sp", None),
            P(),
            P(),
            P("sp", "tp"),
            P("sp", "tp"),
            P("sp", "tp"),
            P(),
            P(None, "tp"),
            P(None, "tp"),
            P(None, "tp"),
            P("tp", None),
            P("tp", None, None),
            P("tp"),
        ),
        out_specs=P(None, ("sp", "tp"), None),
        check_vma=False,
    )
```

```python
import jax
import jax.numpy as jnp
from jax import lax
from jax.experimental import pallas as pl
from jax.experimental.pallas import tpu as pltpu
from jax.sharding import PartitionSpec as P


HEAD_DIM = 64
GRID_W = 64
WIN_ROWS = 8
WIN_COLS = 16
EPSILON = 1e-06
MASKED = -1e30
REACH = WIN_ROWS // 2
BIAS_BLOCKS = 7


def copy_for_each(shard, axis):
    length = lax.axis_size(axis)
    return lax.all_to_all(
        jnp.broadcast_to(shard[None], (length, *shard.shape)), axis, 0, 0, tiled=True
    )


def silu_rows(values):
    return jax.nn.silu(values.astype(jnp.float32)).astype(jnp.bfloat16)


def modulation_parts(place, cond, ctx_cond, weights, copies):
    samples = cond.shape[0]
    rows, cols = weights[0].shape

    def body(place_ref, cond_ref, ctx_ref, shift_ref, scale_ref, gate_ref, out_ref):
        at = pl.multiple_of(place_ref[0] * rows, rows)
        ada = silu_rows(cond_ref[:, pl.ds(at, rows)])
        ada_ctx = silu_rows(ctx_ref[:, pl.ds(at, rows)])
        both = jnp.concatenate([ada.astype(jnp.float32), ada_ctx.astype(jnp.float32)], axis=0)
        both = both.astype(jnp.bfloat16)
        result = jnp.concatenate(
            [
                jnp.dot(both, shift_ref[...], preferred_element_type=jnp.float32),
                jnp.dot(both, scale_ref[...], preferred_element_type=jnp.float32),
                jnp.dot(ada, gate_ref[...], preferred_element_type=jnp.float32),
            ],
            axis=0,
        )
        for copy in range(copies):
            out_ref[copy] = result

    return pl.pallas_call(
        body,
        in_specs=[pl.BlockSpec(memory_space=pltpu.SMEM)]
        + [pl.BlockSpec(memory_space=pltpu.VMEM)] * 5,
        out_shape=jax.ShapeDtypeStruct((copies, 3 * samples + 2, cols), jnp.float32),
        name="modulation_parts",
    )(place, cond, ctx_cond, *weights)


def whole(shape):
    return pl.BlockSpec(shape, lambda *_: (0,) * len(shape))


def modulation_row(tiles, row):
    return jnp.concatenate([tiles[tile, row : row + 1, :] for tile in range(tiles.shape[0])], axis=1)


def project(rows, gain, modulation, weights, row_of, block, ends):
    samples, count, width = rows.shape
    every = modulation.shape[1] // 3 + 1
    cols = weights[0].shape[1]
    first, last = ends if ends else (0, 0)
    steps = count // block

    def body(rows_ref, gain_ref, tiles_ref, *refs):
        weight_refs, out_refs = refs[: len(weights)], refs[len(weights) : -2]
        factor_ref, shift_ref = refs[-2:]
        sample, step = pl.program_id(0), pl.program_id(1)

        for number in range(samples):

            @pl.when((sample == number) & (step == 0))
            def _(number=number):
                row = row_of + number
                factor_ref[...] = gain_ref[...] * (1.0 + modulation_row(tiles_ref, every + row))
                shift_ref[...] = modulation_row(tiles_ref, row)

        floats = rows_ref[0].astype(jnp.float32)
        inverse = lax.rsqrt(jnp.mean(floats * floats, axis=-1, keepdims=True) + EPSILON)
        hidden = (floats * inverse * factor_ref[...] + shift_ref[...]).astype(jnp.bfloat16)
        pair = [
            jnp.dot(hidden, ref[...], preferred_element_type=jnp.float32).astype(jnp.bfloat16)
            for ref in weight_refs[:2]
        ]
        if not ends:
            out_refs[0][0, :, :cols] = pair[0]
            out_refs[0][0, :, cols:] = pair[1]
            return
        out_refs[0][0, :, :cols] = pair[0]
        out_refs[0][0, :, cols:] = pair[1]
        query = jnp.dot(hidden, weight_refs[2][...], preferred_element_type=jnp.float32)
        query = query.astype(jnp.bfloat16).astype(jnp.float32) * HEAD_DIM**-0.5
        out_refs[1][0] = query.astype(jnp.bfloat16)
        for number in range(steps):
            low = number * block
            for out_ref, start, stop in (
                (out_refs[2], 0, first),
                (out_refs[3], count - last, count),
            ):
                lo, hi = max(low, start), min(low + block, stop)
                if lo < hi:

                    @pl.when(step == number)
                    def _(out_ref=out_ref, start=start, lo=lo, hi=hi, low=low):
                        for index in range(2):
                            out_ref[
                                0, lo - start : hi - start, index * cols : (index + 1) * cols
                            ] = pair[index][lo - low : hi - low]

    def blocks(size):
        return pl.BlockSpec((1, block, size), lambda s, i: (s, i, 0))

    if ends:
        out_specs = [blocks(2 * cols), blocks(cols)]
        out_shape = [(samples, count, 2 * cols), (samples, count, cols)]
        for length in ends:
            out_specs += [pl.BlockSpec((1, length, 2 * cols), lambda s, i: (s, 0, 0))]
            out_shape += [(samples, length, 2 * cols)]
    else:
        out_specs = [blocks(2 * cols)]
        out_shape = [(samples, count, 2 * cols)]
    return pl.pallas_call(
        body,
        grid=(samples, steps),
        in_specs=[blocks(width), whole((1, width)), whole(modulation.shape)]
        + [whole(weight.shape) for weight in weights],
        out_specs=out_specs,
        out_shape=[jax.ShapeDtypeStruct(shape, jnp.bfloat16) for shape in out_shape],
        scratch_shapes=[pltpu.VMEM((1, width), jnp.float32)] * 2,
        name="project",
    )(rows, gain, modulation, *weights)


def bias_table(rel_bias):
    heads, offsets, spread = rel_bias.shape
    slots = 2 * BIAS_BLOCKS + 2
    padded = jnp.pad(rel_bias, ((0, 0), (0, slots - offsets), (0, 128 - spread)))
    padded = padded.reshape(heads * slots, 128)

    def body(rel_ref, out_ref):
        query = lax.broadcasted_iota(jnp.int32, (GRID_W, 128), 0)
        lane = lax.broadcasted_iota(jnp.int32, (GRID_W, 128), 1)
        low = lane < GRID_W
        key = jnp.where(low, lane, lane - GRID_W)
        start = jnp.clip(query - WIN_COLS // 2, 0, GRID_W - WIN_COLS)
        inside = (key >= start) & (key < start + WIN_COLS)

        def diagonal(head, slot, move):
            row = jnp.broadcast_to(rel_ref[pl.ds(head * slots + slot, 1), :], (GRID_W, 128))
            return pltpu.roll(row, (128 - (WIN_COLS - 1) + move) % 128, 1, stride=1, stride_axis=0)

        for parity in range(2):
            for head in range(heads):
                for block in range(BIAS_BLOCKS):
                    slot = 2 * block + parity
                    both = jnp.where(
                        low, diagonal(head, slot, 0), diagonal(head, slot + 1, GRID_W)
                    )
                    out_ref[
                        parity, head * GRID_W : (head + 1) * GRID_W, block * 128 : (block + 1) * 128
                    ] = jnp.where(inside, both, MASKED)

    return pl.pallas_call(
        body,
        out_shape=jax.ShapeDtypeStruct((2, heads * GRID_W, BIAS_BLOCKS * 128), jnp.float32),
        name="bias_table",
    )(padded)


def head_masks(cols):
    lane = lax.broadcasted_iota(jnp.int32, (GRID_W, cols), 1)
    return [(lane >= low) & (lane < low + HEAD_DIM) for low in range(0, cols, HEAD_DIM)]


def spread_heads(query, masks):
    return jnp.concatenate(
        [jnp.where(mask, query, jnp.zeros_like(query)) for mask in masks], axis=0
    )


def gather_heads(values, masks):
    result = jnp.where(masks[0], values[:GRID_W], 0.0)
    for h in range(1, len(masks)):
        result = jnp.where(masks[h], values[h * GRID_W : (h + 1) * GRID_W], result)
    return result


def weighed(scores, values, masks):
    top = jnp.max(scores, axis=-1, keepdims=True)
    exps = jnp.exp(scores - top)
    total = jnp.sum(exps, axis=-1, keepdims=True)
    mixed = jnp.dot(exps.astype(jnp.bfloat16), values, preferred_element_type=jnp.float32)
    return [gather_heads(array, masks) for array in (mixed, top, total)]


def attend_near(place, query, before, pair, after, table, rows_all, per):
    samples, tokens, cols = query.shape
    rows_dev = tokens // GRID_W
    near_keys = WIN_ROWS * GRID_W
    ahead, behind = before.shape[1], after.shape[1]
    padded = ahead + tokens + behind
    lanes = -(-padded // 128) * 128
    bf16, f32 = jnp.bfloat16, jnp.float32

    def body(place_ref, q_ref, before_ref, pair_ref, after_ref, table_ref, *refs):
        out_refs, (near_t, values) = refs[:3], refs[3:]
        step = pl.program_id(1)

        @pl.when(step == 0)
        def _():
            values[0:ahead] = before_ref[0, :, cols:]
            values[ahead : ahead + tokens] = pair_ref[0, :, cols:]
            values[ahead + tokens : padded] = after_ref[0, :, cols:]
            fill = jnp.zeros((lanes - padded, cols), bf16)
            near_t[0, :, :ahead] = before_ref[0, :, :cols].T
            near_t[0, :, ahead : ahead + tokens] = pair_ref[0, :, :cols].T
            near_t[0, :, ahead + tokens :] = jnp.concatenate(
                [after_ref[0, :, :cols], fill], axis=0
            ).T
            near_t[1] = jnp.concatenate(
                [
                    before_ref[0, GRID_W:, :cols],
                    pair_ref[0, :, :cols],
                    after_ref[0, :, :cols],
                    fill,
                    jnp.zeros((GRID_W, cols), bf16),
                ],
                axis=0,
            ).T

        base = place_ref[0] * rows_dev
        masks = head_masks(cols)
        scores, starts = [], []
        for r in range(per):
            actual = base + step * per + r
            start = jnp.clip(actual - REACH, 0, rows_all - WIN_ROWS)
            local = start - base + REACH
            offset = start - actual + WIN_ROWS - 1
            spread = spread_heads(q_ref[0, r * GRID_W : (r + 1) * GRID_W], masks)
            column = pl.multiple_of((local // 2) * 128, 128)
            keys_t = near_t[local % 2, :, pl.ds(column, near_keys)]
            bias_at = pl.multiple_of((offset // 2) * 128, 128)
            scores.append(
                jnp.dot(spread, keys_t, preferred_element_type=f32)
                + table_ref[offset % 2, :, pl.ds(bias_at, near_keys)]
            )
            starts.append(pl.multiple_of(local * GRID_W, GRID_W))
        for r in range(per):
            parts = weighed(scores[r], values[pl.ds(starts[r], near_keys), :], masks)
            for out_ref, part in zip(out_refs, parts):
                out_ref[0, r * GRID_W : (r + 1) * GRID_W] = part

    def of_sample(array):
        return pl.BlockSpec((1, *array.shape[1:]), lambda s, i: (s, 0, 0))

    rows_spec = pl.BlockSpec((1, per * GRID_W, cols), lambda s, i: (s, i, 0))
    return pl.pallas_call(
        body,
        grid=(samples, rows_dev // per),
        in_specs=[
            pl.BlockSpec(memory_space=pltpu.SMEM),
            rows_spec,
            of_sample(before),
            of_sample(pair),
            of_sample(after),
            whole(table.shape),
        ],
        out_specs=[rows_spec] * 3,
        out_shape=[jax.ShapeDtypeStruct((samples, tokens, cols), f32)] * 3,
        scratch_shapes=[
            pltpu.VMEM((2, cols, lanes), bf16),
            pltpu.VMEM((padded, cols), bf16),
        ],
        name="attend_near",
    )(place, query, before, pair, after, table)


def attend_far(query, ctx_pairs, ctx_bias, near, per):
    samples, tokens, cols = query.shape
    rows_dev = tokens // GRID_W
    lines = len(ctx_pairs)
    members, _, ctx_rows, _ = ctx_pairs[0].shape
    ctx_count = lines * members * ctx_rows
    bf16, f32 = jnp.bfloat16, jnp.float32

    def body(q_ref, *refs):
        ctx_refs = refs[:lines]
        cb_ref, mixed_ref, top_ref, total_ref, out_ref, far_t, values = refs[lines:]

        @pl.when(pl.program_id(1) == 0)
        def _():
            size = members * ctx_rows
            for line, ctx_ref in enumerate(ctx_refs):
                at = line * size
                for member in range(members):
                    low = at + member * ctx_rows
                    values[low : low + ctx_rows] = ctx_ref[member, 0, :, cols:]
                block = jnp.concatenate(
                    [ctx_ref[member, 0, :, :cols] for member in range(members)], axis=0
                )
                far_t[:, at : at + size] = block.T

        masks = head_masks(cols)
        scores = [
            jnp.dot(
                spread_heads(q_ref[0, r * GRID_W : (r + 1) * GRID_W], masks),
                far_t[...],
                preferred_element_type=f32,
            )
            for r in range(per)
        ]
        for r in range(per):
            mixed, top, total = weighed(scores[r], values[...], masks)
            at = slice(r * GRID_W, (r + 1) * GRID_W)
            top = top + cb_ref[...]
            near_top = top_ref[0, at]
            highest = jnp.maximum(top, near_top)
            far_part = jnp.exp(top - highest)
            near_part = jnp.exp(near_top - highest)
            total = total * far_part + total_ref[0, at] * near_part
            mixed = mixed * far_part + mixed_ref[0, at] * near_part
            out_ref[r, 0] = (mixed / total).astype(bf16)

    rows_spec = pl.BlockSpec((1, per * GRID_W, cols), lambda s, i: (s, i, 0))
    return pl.pallas_call(
        body,
        grid=(samples, rows_dev // per),
        in_specs=[
            rows_spec,
        ]
        + [pl.BlockSpec((members, 1, ctx_rows, 2 * cols), lambda s, i: (0, s, 0, 0))] * lines
        + [whole(ctx_bias.shape)]
        + [rows_spec] * 3,
        out_specs=pl.BlockSpec((per, 1, GRID_W, cols), lambda s, i: (i, s, 0, 0)),
        out_shape=jax.ShapeDtypeStruct((rows_dev, samples, GRID_W, cols), bf16),
        scratch_shapes=[
            pltpu.VMEM((cols, ctx_count), bf16),
            pltpu.VMEM((ctx_count, cols), bf16),
        ],
        name="attend_far",
    )(query, *ctx_pairs, ctx_bias, *near)


def finish(attended, w_out, latent, modulation, tiles):
    groups, _, _ = attended.shape
    samples, tokens, width = latent.shape
    block = modulation.shape[2] * tiles
    first = modulation.shape[1] - samples

    def body(att_ref, w_ref, latent_ref, tile_ref, out_ref):
        everything = jnp.concatenate([att_ref[group] for group in range(groups)], axis=1)
        update = jnp.dot(everything, w_ref[...], preferred_element_type=jnp.float32)
        for s in range(samples):
            gate = modulation_row(tile_ref, first + s)
            part = update[s * tokens : (s + 1) * tokens]
            out_ref[s] = (latent_ref[s].astype(jnp.float32) + gate * part).astype(jnp.bfloat16)

    return pl.pallas_call(
        body,
        grid=(width // block,),
        in_specs=[
            whole(attended.shape),
            pl.BlockSpec((width, block), lambda i: (0, i)),
            pl.BlockSpec((samples, tokens, block), lambda i: (0, 0, i)),
            pl.BlockSpec((tiles, *modulation.shape[1:]), lambda i: (i, 0, 0)),
        ],
        out_specs=pl.BlockSpec((samples, tokens, block), lambda i: (0, 0, i)),
        out_shape=jax.ShapeDtypeStruct(latent.shape, latent.dtype),
        name="finish",
    )(attended, w_out, latent, modulation)


def shifted(size, side, stride, value):
    span = side * stride
    return [(i, i // span * span + (i + value * stride) % span) for i in range(size)]


def from_line(block, axis, side, stride):
    size = lax.axis_size(axis)
    return [block] + [
        lax.ppermute(block, axis, shifted(size, side, stride, value)) for value in range(1, side)
    ]


def computation(
    latent,
    context,
    cond,
    ctx_cond,
    w_shift,
    w_scale,
    w_gate,
    norm_gain,
    w_query,
    w_key,
    w_value,
    w_out,
    rel_bias,
    ctx_bias,
):
    samples, tokens_dev, width = latent.shape
    local_cols = w_shift.shape[1]
    sp_index = lax.axis_index("sp")
    sp_size, tp_size = lax.axis_size("sp"), lax.axis_size("tp")
    place = jnp.full((1,), sp_index, jnp.int32)
    gathered = lax.all_gather(latent, "tp", axis=1, tiled=True)
    parts = modulation_parts(place, cond, ctx_cond[None], (w_shift, w_scale, w_gate), sp_size)
    parts, w_out_own = lax.optimization_barrier((parts, w_out))
    w_out_all = lax.all_gather(w_out_own, "tp", axis=0, tiled=True)
    table = bias_table(rel_bias)
    cb = jnp.repeat(ctx_bias, HEAD_DIM)[None, :]
    summed = jnp.sum(lax.all_to_all(parts, "sp", 0, 0, tiled=True), axis=0)
    summed, table, cb = lax.optimization_barrier((summed, table, cb))
    modulation = copy_for_each(summed, "tp")

    gain = norm_gain[None, :]
    ctx_rows = context.shape[1]
    (ctx_pair,) = project(
        context.reshape(1, samples * ctx_rows, width),
        gain,
        modulation,
        (w_key, w_value),
        samples,
        samples * ctx_rows,
        None,
    )
    ctx_pair = ctx_pair.reshape(samples, ctx_rows, 2 * local_cols)
    ctx_pairs = from_line(ctx_pair, "sp", 4, 1)
    up = [(i, i + 1) for i in range(sp_size - 1)]
    down = [(j, i) for i, j in up]
    pair, query, first, last = project(
        gathered,
        gain,
        modulation,
        (w_key, w_value, w_query),
        0,
        256,
        ((WIN_ROWS - REACH - 1) * GRID_W, REACH * GRID_W),
    )
    ctx_pairs, query = lax.optimization_barrier((ctx_pairs, query))
    ctx_line = jnp.stack(ctx_pairs)
    ctx_pairs = from_line(ctx_line, "sp", 4, 4)
    before = lax.ppermute(last, "sp", up)
    after = lax.ppermute(first, "sp", down)
    rows_all = pair.shape[1] // GRID_W * sp_size
    near = attend_near(place, query, before, pair, after, table, rows_all, 2)
    attended = attend_far(query, ctx_pairs, cb, near, 2)
    attended = attended.reshape(tp_size, samples * tokens_dev, local_cols)
    attended = lax.all_to_all(attended, "tp", 0, 0, tiled=True)
    return finish(attended, w_out_all, latent, modulation, 4)


def solution(mesh):
    return jax.shard_map(
        computation,
        mesh=mesh,
        in_specs=(
            P(None, ("sp", "tp"), None),
            P(None, "sp", None),
            P(),
            P(),
            P("sp", "tp"),
            P("sp", "tp"),
            P("sp", "tp"),
            P(),
            P(None, "tp"),
            P(None, "tp"),
            P(None, "tp"),
            P("tp", None),
            P("tp", None, None),
            P("tp"),
        ),
        out_specs=P(None, ("sp", "tp"), None),
        check_vma=False,
    )
```

```python
import jax
import jax.numpy as jnp
from jax import lax
from jax.experimental import pallas as pl
from jax.experimental.pallas import tpu as pltpu
from jax.sharding import PartitionSpec as P


HEAD_DIM = 64
GRID_W = 64
WIN_ROWS = 8
WIN_COLS = 16
EPSILON = 1e-06
MASKED = -1e30
REACH = WIN_ROWS // 2
BIAS_BLOCKS = 7


def copy_for_each(shard, axis):
    length = lax.axis_size(axis)
    return lax.all_to_all(
        jnp.broadcast_to(shard[None], (length, *shard.shape)), axis, 0, 0, tiled=True
    )


def silu_rows(values):
    return jax.nn.silu(values.astype(jnp.float32)).astype(jnp.bfloat16)


def modulation_parts(place, cond, ctx_cond, weights, copies):
    samples = cond.shape[0]
    rows, cols = weights[0].shape

    def body(place_ref, cond_ref, ctx_ref, shift_ref, scale_ref, gate_ref, out_ref):
        at = pl.multiple_of(place_ref[0] * rows, rows)
        ada = silu_rows(cond_ref[:, pl.ds(at, rows)])
        ada_ctx = silu_rows(ctx_ref[:, pl.ds(at, rows)])
        both = jnp.concatenate([ada.astype(jnp.float32), ada_ctx.astype(jnp.float32)], axis=0)
        both = both.astype(jnp.bfloat16)
        result = jnp.concatenate(
            [
                jnp.dot(both, shift_ref[...], preferred_element_type=jnp.float32),
                jnp.dot(both, scale_ref[...], preferred_element_type=jnp.float32),
                jnp.dot(ada, gate_ref[...], preferred_element_type=jnp.float32),
            ],
            axis=0,
        )
        for copy in range(copies):
            out_ref[copy] = result

    return pl.pallas_call(
        body,
        in_specs=[pl.BlockSpec(memory_space=pltpu.SMEM)]
        + [pl.BlockSpec(memory_space=pltpu.VMEM)] * 5,
        out_shape=jax.ShapeDtypeStruct((copies, 3 * samples + 2, cols), jnp.float32),
        name="modulation_parts",
    )(place, cond, ctx_cond, *weights)


def whole(shape):
    return pl.BlockSpec(shape, lambda *_: (0,) * len(shape))


def modulation_row(tiles, row):
    return jnp.concatenate([tiles[tile, row : row + 1, :] for tile in range(tiles.shape[0])], axis=1)


def project(rows, gain, modulation, weights, row_of, block, ends):
    samples, count, width = rows.shape
    every = modulation.shape[1] // 3 + 1
    cols = weights[0].shape[1]
    first, last = ends if ends else (0, 0)
    steps = count // block

    def body(rows_ref, gain_ref, tiles_ref, *refs):
        weight_refs, out_refs = refs[: len(weights)], refs[len(weights) : -2]
        factor_ref, shift_ref = refs[-2:]
        sample, step = pl.program_id(0), pl.program_id(1)

        for number in range(samples):

            @pl.when((sample == number) & (step == 0))
            def _(number=number):
                row = row_of + number
                factor_ref[...] = gain_ref[...] * (1.0 + modulation_row(tiles_ref, every + row))
                shift_ref[...] = modulation_row(tiles_ref, row)

        floats = rows_ref[0].astype(jnp.float32)
        inverse = lax.rsqrt(jnp.mean(floats * floats, axis=-1, keepdims=True) + EPSILON)
        hidden = (floats * inverse * factor_ref[...] + shift_ref[...]).astype(jnp.bfloat16)
        pair = [
            jnp.dot(hidden, ref[...], preferred_element_type=jnp.float32).astype(jnp.bfloat16)
            for ref in weight_refs[:2]
        ]
        if not ends:
            out_refs[0][0, :, :cols] = pair[0]
            out_refs[0][0, :, cols:] = pair[1]
            return
        out_refs[0][0, :, :cols] = pair[0]
        out_refs[0][0, :, cols:] = pair[1]
        query = jnp.dot(hidden, weight_refs[2][...], preferred_element_type=jnp.float32)
        query = query.astype(jnp.bfloat16).astype(jnp.float32) * HEAD_DIM**-0.5
        out_refs[1][0] = query.astype(jnp.bfloat16)
        for number in range(steps):
            low = number * block
            for out_ref, start, stop in (
                (out_refs[2], 0, first),
                (out_refs[3], count - last, count),
            ):
                lo, hi = max(low, start), min(low + block, stop)
                if lo < hi:

                    @pl.when(step == number)
                    def _(out_ref=out_ref, start=start, lo=lo, hi=hi, low=low):
                        for index in range(2):
                            out_ref[
                                0, lo - start : hi - start, index * cols : (index + 1) * cols
                            ] = pair[index][lo - low : hi - low]

    def blocks(size):
        return pl.BlockSpec((1, block, size), lambda s, i: (s, i, 0))

    if ends:
        out_specs = [blocks(2 * cols), blocks(cols)]
        out_shape = [(samples, count, 2 * cols), (samples, count, cols)]
        for length in ends:
            out_specs += [pl.BlockSpec((1, length, 2 * cols), lambda s, i: (s, 0, 0))]
            out_shape += [(samples, length, 2 * cols)]
    else:
        out_specs = [blocks(2 * cols)]
        out_shape = [(samples, count, 2 * cols)]
    return pl.pallas_call(
        body,
        grid=(samples, steps),
        in_specs=[blocks(width), whole((1, width)), whole(modulation.shape)]
        + [whole(weight.shape) for weight in weights],
        out_specs=out_specs,
        out_shape=[jax.ShapeDtypeStruct(shape, jnp.bfloat16) for shape in out_shape],
        scratch_shapes=[pltpu.VMEM((1, width), jnp.float32)] * 2,
        name="project",
    )(rows, gain, modulation, *weights)


def bias_table(rel_bias):
    heads, offsets, spread = rel_bias.shape
    slots = 2 * BIAS_BLOCKS + 2
    padded = jnp.pad(rel_bias, ((0, 0), (0, slots - offsets), (0, 128 - spread)))
    padded = padded.reshape(heads * slots, 128)

    def body(rel_ref, out_ref):
        query = lax.broadcasted_iota(jnp.int32, (GRID_W, 128), 0)
        lane = lax.broadcasted_iota(jnp.int32, (GRID_W, 128), 1)
        low = lane < GRID_W
        key = jnp.where(low, lane, lane - GRID_W)
        start = jnp.clip(query - WIN_COLS // 2, 0, GRID_W - WIN_COLS)
        inside = (key >= start) & (key < start + WIN_COLS)

        def diagonal(head, slot, move):
            row = jnp.broadcast_to(rel_ref[pl.ds(head * slots + slot, 1), :], (GRID_W, 128))
            return pltpu.roll(row, (128 - (WIN_COLS - 1) + move) % 128, 1, stride=1, stride_axis=0)

        for parity in range(2):
            for head in range(heads):
                for block in range(BIAS_BLOCKS):
                    slot = 2 * block + parity
                    both = jnp.where(
                        low, diagonal(head, slot, 0), diagonal(head, slot + 1, GRID_W)
                    )
                    out_ref[
                        parity, head * GRID_W : (head + 1) * GRID_W, block * 128 : (block + 1) * 128
                    ] = jnp.where(inside, both, MASKED)

    return pl.pallas_call(
        body,
        out_shape=jax.ShapeDtypeStruct((2, heads * GRID_W, BIAS_BLOCKS * 128), jnp.float32),
        name="bias_table",
    )(padded)


def attend(place, query, before, pair, after, ctx_pairs, table, ctx_bias, rows_all, per):
    samples, tokens, cols = query.shape
    heads = cols // HEAD_DIM
    rows_dev = tokens // GRID_W
    near_keys = WIN_ROWS * GRID_W
    ahead, behind = before.shape[1], after.shape[1]
    padded = ahead + tokens + behind
    lanes = -(-padded // 128) * 128
    ctx_rows = ctx_pairs[0].shape[2]
    members = [array.shape[0] for array in ctx_pairs]
    ctx_count = sum(members) * ctx_rows
    queries = heads * GRID_W
    bf16, f32 = jnp.bfloat16, jnp.float32

    def body(place_ref, q_ref, before_ref, pair_ref, after_ref, *refs):
        ctx_refs = refs[: len(members)]
        table_ref, cb_ref, out_ref, near_t, far_t, values, far_values = refs[len(members) :]
        step = pl.program_id(1)

        @pl.when(step == 0)
        def _():
            values[0:ahead] = before_ref[0, :, cols:]
            values[ahead : ahead + tokens] = pair_ref[0, :, cols:]
            values[ahead + tokens : padded] = after_ref[0, :, cols:]
            at = 0
            for ctx_ref, count in zip(ctx_refs, members):
                for member in range(count):
                    low = at + member * ctx_rows
                    far_values[low : low + ctx_rows] = ctx_ref[member, 0, :, cols:]
                size = count * ctx_rows
                block = jnp.concatenate(
                    [ctx_ref[member, 0, :, :cols] for member in range(count)], axis=0
                )
                far_t[:, at : at + size] = block.T
                at += size
            fill = jnp.zeros((lanes - padded, cols), bf16)
            near_t[0, :, :ahead] = before_ref[0, :, :cols].T
            near_t[0, :, ahead : ahead + tokens] = pair_ref[0, :, :cols].T
            near_t[0, :, ahead + tokens :] = jnp.concatenate(
                [after_ref[0, :, :cols], fill], axis=0
            ).T
            near_t[1] = jnp.concatenate(
                [
                    before_ref[0, GRID_W:, :cols],
                    pair_ref[0, :, :cols],
                    after_ref[0, :, :cols],
                    fill,
                    jnp.zeros((GRID_W, cols), bf16),
                ],
                axis=0,
            ).T

        base = place_ref[0] * rows_dev
        lane = lax.broadcasted_iota(jnp.int32, (GRID_W, cols), 1)
        masks = [(lane >= h * HEAD_DIM) & (lane < (h + 1) * HEAD_DIM) for h in range(heads)]
        cb = cb_ref[...]
        spreads, nears, starts = [], [], []
        for r in range(per):
            actual = base + step * per + r
            start = jnp.clip(actual - REACH, 0, rows_all - WIN_ROWS)
            local = start - base + REACH
            offset = start - actual + WIN_ROWS - 1
            q = q_ref[0, r * GRID_W : (r + 1) * GRID_W]
            spread = jnp.concatenate(
                [jnp.where(mask, q, jnp.zeros_like(q)) for mask in masks], axis=0
            )
            spreads.append(spread)
            column = pl.multiple_of((local // 2) * 128, 128)
            keys_t = near_t[local % 2, :, pl.ds(column, near_keys)]
            bias_at = pl.multiple_of((offset // 2) * 128, 128)
            nears.append(
                jnp.dot(spread, keys_t, preferred_element_type=f32)
                + table_ref[offset % 2, :, pl.ds(bias_at, near_keys)]
            )
            starts.append(pl.multiple_of(local * GRID_W, GRID_W))
        for r in range(per):
            near = nears[r]
            far = jnp.dot(spreads[r], far_t[...], preferred_element_type=f32)
            top = jnp.maximum(
                jnp.max(near, axis=-1, keepdims=True), jnp.max(far, axis=-1, keepdims=True) + cb
            )
            near_exp = jnp.exp(near - top)
            far_exp = jnp.exp(far - (top - cb))
            total = jnp.sum(near_exp, axis=-1, keepdims=True) + jnp.sum(
                far_exp, axis=-1, keepdims=True
            )
            mixed = jnp.dot(
                near_exp.astype(bf16),
                values[pl.ds(starts[r], near_keys), :],
                preferred_element_type=f32,
            ) + jnp.dot(far_exp.astype(bf16), far_values[...], preferred_element_type=f32)
            mixed = mixed * (1.0 / total)
            result = jnp.where(masks[0], mixed[:GRID_W], 0.0)
            for h in range(1, heads):
                result = jnp.where(masks[h], mixed[h * GRID_W : (h + 1) * GRID_W], result)
            out_ref[r, 0] = result.astype(bf16)

    def of_sample(array):
        return pl.BlockSpec((1, *array.shape[1:]), lambda s, i: (s, 0, 0))

    return pl.pallas_call(
        body,
        grid=(samples, rows_dev // per),
        in_specs=[
            pl.BlockSpec(memory_space=pltpu.SMEM),
            pl.BlockSpec((1, per * GRID_W, cols), lambda s, i: (s, i, 0)),
            of_sample(before),
            of_sample(pair),
            of_sample(after),
        ]
        + [
            pl.BlockSpec((count, 1, ctx_rows, 2 * cols), lambda s, i: (0, s, 0, 0))
            for count in members
        ]
        + [whole(table.shape), whole((queries, 1))],
        out_specs=pl.BlockSpec((per, 1, GRID_W, cols), lambda s, i: (i, s, 0, 0)),
        out_shape=jax.ShapeDtypeStruct((rows_dev, samples, GRID_W, cols), bf16),
        scratch_shapes=[
            pltpu.VMEM((2, cols, lanes), bf16),
            pltpu.VMEM((cols, ctx_count), bf16),
            pltpu.VMEM((padded, cols), bf16),
            pltpu.VMEM((ctx_count, cols), bf16),
        ],
        name="attend",
    )(place, query, before, pair, after, *ctx_pairs, table, ctx_bias)


def finish(attended, w_out, latent, modulation, tiles):
    groups, _, _ = attended.shape
    samples, tokens, width = latent.shape
    block = modulation.shape[2] * tiles
    first = modulation.shape[1] - samples

    def body(att_ref, w_ref, latent_ref, tile_ref, out_ref):
        everything = jnp.concatenate([att_ref[group] for group in range(groups)], axis=1)
        update = jnp.dot(everything, w_ref[...], preferred_element_type=jnp.float32)
        for s in range(samples):
            gate = modulation_row(tile_ref, first + s)
            part = update[s * tokens : (s + 1) * tokens]
            out_ref[s] = (latent_ref[s].astype(jnp.float32) + gate * part).astype(jnp.bfloat16)

    return pl.pallas_call(
        body,
        grid=(width // block,),
        in_specs=[
            whole(attended.shape),
            pl.BlockSpec((width, block), lambda i: (0, i)),
            pl.BlockSpec((samples, tokens, block), lambda i: (0, 0, i)),
            pl.BlockSpec((tiles, *modulation.shape[1:]), lambda i: (i, 0, 0)),
        ],
        out_specs=pl.BlockSpec((samples, tokens, block), lambda i: (0, 0, i)),
        out_shape=jax.ShapeDtypeStruct(latent.shape, latent.dtype),
        name="finish",
    )(attended, w_out, latent, modulation)


def shifted(size, side, stride, value):
    span = side * stride
    return [(i, i // span * span + (i + value * stride) % span) for i in range(size)]


def from_line(block, axis, side, stride):
    size = lax.axis_size(axis)
    return [block] + [
        lax.ppermute(block, axis, shifted(size, side, stride, value)) for value in range(1, side)
    ]


def computation(
    latent,
    context,
    cond,
    ctx_cond,
    w_shift,
    w_scale,
    w_gate,
    norm_gain,
    w_query,
    w_key,
    w_value,
    w_out,
    rel_bias,
    ctx_bias,
):
    samples, tokens_dev, width = latent.shape
    local_cols = w_shift.shape[1]
    sp_index = lax.axis_index("sp")
    sp_size, tp_size = lax.axis_size("sp"), lax.axis_size("tp")
    place = jnp.full((1,), sp_index, jnp.int32)
    gathered = lax.all_gather(latent, "tp", axis=1, tiled=True)
    parts = modulation_parts(place, cond, ctx_cond[None], (w_shift, w_scale, w_gate), sp_size)
    parts, w_out_own = lax.optimization_barrier((parts, w_out))
    w_out_all = lax.all_gather(w_out_own, "tp", axis=0, tiled=True)
    table = bias_table(rel_bias)
    cb = jnp.repeat(ctx_bias, GRID_W)[:, None]
    summed = jnp.sum(lax.all_to_all(parts, "sp", 0, 0, tiled=True), axis=0)
    summed, table, cb = lax.optimization_barrier((summed, table, cb))
    modulation = copy_for_each(summed, "tp")

    gain = norm_gain[None, :]
    ctx_rows = context.shape[1]
    (ctx_pair,) = project(
        context.reshape(1, samples * ctx_rows, width),
        gain,
        modulation,
        (w_key, w_value),
        samples,
        samples * ctx_rows,
        None,
    )
    ctx_pair = ctx_pair.reshape(samples, ctx_rows, 2 * local_cols)
    ctx_pairs = from_line(ctx_pair, "sp", 4, 1)
    up = [(i, i + 1) for i in range(sp_size - 1)]
    down = [(j, i) for i, j in up]
    pair, query, first, last = project(
        gathered,
        gain,
        modulation,
        (w_key, w_value, w_query),
        0,
        256,
        ((WIN_ROWS - REACH - 1) * GRID_W, REACH * GRID_W),
    )
    ctx_pairs, query = lax.optimization_barrier((ctx_pairs, query))
    ctx_line = jnp.stack(ctx_pairs)
    below = lax.ppermute(ctx_line, "sp", shifted(sp_size, 4, 4, 1))
    above = lax.ppermute(ctx_line, "sp", shifted(sp_size, 4, 4, 3))
    before = lax.ppermute(last, "sp", up)
    after = lax.ppermute(first, "sp", down)
    rows_all = pair.shape[1] // GRID_W * sp_size
    ctx_pairs = [
        ctx_line,
        below,
        above,
        lax.ppermute(below[:2], "sp", shifted(sp_size, 4, 4, 1)),
        lax.ppermute(above[2:], "sp", shifted(sp_size, 4, 4, 3)),
    ]
    attended = attend(
        place, query, before, pair, after, ctx_pairs, table, cb, rows_all, 2
    )
    attended = attended.reshape(tp_size, samples * tokens_dev, local_cols)
    attended = lax.all_to_all(attended, "tp", 0, 0, tiled=True)
    return finish(attended, w_out_all, latent, modulation, 4)


def solution(mesh):
    return jax.shard_map(
        computation,
        mesh=mesh,
        in_specs=(
            P(None, ("sp", "tp"), None),
            P(None, "sp", None),
            P(),
            P(),
            P("sp", "tp"),
            P("sp", "tp"),
            P("sp", "tp"),
            P(),
            P(None, "tp"),
            P(None, "tp"),
            P(None, "tp"),
            P("tp", None),
            P("tp", None, None),
            P("tp"),
        ),
        out_specs=P(None, ("sp", "tp"), None),
        check_vma=False,
    )
```

```python
import jax
import jax.numpy as jnp
from jax import lax
from jax.experimental import pallas as pl
from jax.experimental.pallas import tpu as pltpu
from jax.sharding import PartitionSpec as P


HEAD_DIM = 64
GRID_W = 64
WIN_ROWS = 8
WIN_COLS = 16
EPSILON = 1e-06
MASKED = -1e30
REACH = WIN_ROWS // 2
BIAS_BLOCKS = 7


def copy_for_each(shard, axis):
    length = lax.axis_size(axis)
    return lax.all_to_all(
        jnp.broadcast_to(shard[None], (length, *shard.shape)), axis, 0, 0, tiled=True
    )


def silu_rows(values):
    return jax.nn.silu(values.astype(jnp.float32)).astype(jnp.bfloat16)


def modulation_parts(place, cond, ctx_cond, weights, copies):
    samples = cond.shape[0]
    rows, cols = weights[0].shape

    def body(place_ref, cond_ref, ctx_ref, shift_ref, scale_ref, gate_ref, out_ref, wide):
        at = pl.multiple_of(place_ref[0] * rows, rows)
        ada = silu_rows(cond_ref[:, pl.ds(at, rows)])
        wide[...] = ctx_ref[...].astype(jnp.float32).reshape(1, ctx_ref.shape[0])
        ada_ctx = silu_rows(wide[:, pl.ds(at, rows)])
        both = jnp.concatenate([ada.astype(jnp.float32), ada_ctx.astype(jnp.float32)], axis=0)
        both = both.astype(jnp.bfloat16)
        result = jnp.concatenate(
            [
                jnp.dot(both, shift_ref[...], preferred_element_type=jnp.float32),
                jnp.dot(both, scale_ref[...], preferred_element_type=jnp.float32),
                jnp.dot(ada, gate_ref[...], preferred_element_type=jnp.float32),
            ],
            axis=0,
        )
        for copy in range(copies):
            out_ref[copy] = result

    return pl.pallas_call(
        body,
        in_specs=[pl.BlockSpec(memory_space=pltpu.SMEM)]
        + [pl.BlockSpec(memory_space=pltpu.VMEM)] * 5,
        out_shape=jax.ShapeDtypeStruct((copies, 3 * samples + 2, cols), jnp.float32),
        scratch_shapes=[pltpu.VMEM((1, ctx_cond.shape[0]), jnp.float32)],
        name="modulation_parts",
    )(place, cond, ctx_cond, *weights)


def whole(shape):
    return pl.BlockSpec(shape, lambda *_: (0,) * len(shape))


def modulation_row(tiles, row):
    return jnp.concatenate([tiles[tile, row : row + 1, :] for tile in range(tiles.shape[0])], axis=1)


def project(rows, gain, modulation, weights, row_of, block, ends, sample=None, buffers=()):
    samples, count, width = rows.shape
    every = modulation.shape[1] // 3 + 1
    chosen = range(samples) if sample is None else (sample,)
    begin = chosen[0]
    cols = weights[0].shape[1]
    first, last = ends if ends else (0, 0)
    steps = count // block

    def body(rows_ref, gain_ref, tiles_ref, *refs):
        weight_refs, out_refs = refs[: len(weights)], refs[len(weights) + len(buffers) : -2]
        factor_ref, shift_ref = refs[-2:]
        turn, step = pl.program_id(0), pl.program_id(1)

        for number in chosen:

            @pl.when((turn == number - begin) & (step == 0))
            def _(number=number):
                row = row_of + number
                factor_ref[...] = gain_ref[...] * (1.0 + modulation_row(tiles_ref, every + row))
                shift_ref[...] = modulation_row(tiles_ref, row)

        floats = rows_ref[0].astype(jnp.float32)
        inverse = lax.rsqrt(jnp.mean(floats * floats, axis=-1, keepdims=True) + EPSILON)
        hidden = (floats * inverse * factor_ref[...] + shift_ref[...]).astype(jnp.bfloat16)
        pair = [
            jnp.dot(hidden, ref[...], preferred_element_type=jnp.float32).astype(jnp.bfloat16)
            for ref in weight_refs[:2]
        ]
        if not ends:
            out_refs[0][0, :, :cols] = pair[0]
            out_refs[0][0, :, cols:] = pair[1]
            return
        out_refs[0][0, :, :cols] = pair[0]
        out_refs[0][0, :, cols:] = pair[1]
        query = jnp.dot(hidden, weight_refs[2][...], preferred_element_type=jnp.float32)
        query = query.astype(jnp.bfloat16).astype(jnp.float32) * HEAD_DIM**-0.5
        out_refs[1][0] = query.astype(jnp.bfloat16)
        for number in range(steps):
            low = number * block
            for out_ref, start, stop in (
                (out_refs[2], 0, first),
                (out_refs[3], count - last, count),
            ):
                lo, hi = max(low, start), min(low + block, stop)
                if lo < hi:

                    @pl.when(step == number)
                    def _(out_ref=out_ref, start=start, lo=lo, hi=hi, low=low):
                        for index in range(2):
                            out_ref[
                                0, lo - start : hi - start, index * cols : (index + 1) * cols
                            ] = pair[index][lo - low : hi - low]

    def blocks(size):
        return pl.BlockSpec((1, block, size), lambda s, i: (begin + s, i, 0))

    if ends:
        out_specs = [blocks(2 * cols), blocks(cols)]
        out_shape = [(samples, count, 2 * cols), (samples, count, cols)]
        for length in ends:
            out_specs += [pl.BlockSpec((1, length, 2 * cols), lambda s, i: (begin + s, 0, 0))]
            out_shape += [(samples, length, 2 * cols)]
    else:
        out_specs = [blocks(2 * cols)]
        out_shape = [(samples, count, 2 * cols)]
    return pl.pallas_call(
        body,
        grid=(len(chosen), steps),
        in_specs=[blocks(width), whole((1, width)), whole(modulation.shape)]
        + [whole(weight.shape) for weight in weights]
        + [pl.BlockSpec(memory_space=pl.ANY)] * len(buffers),
        out_specs=out_specs,
        out_shape=[jax.ShapeDtypeStruct(shape, jnp.bfloat16) for shape in out_shape],
        scratch_shapes=[pltpu.VMEM((1, width), jnp.float32)] * 2,
        input_output_aliases={3 + len(weights) + i: i for i in range(len(buffers))},
        name="project",
    )(rows, gain, modulation, *weights, *buffers)


def bias_table(rel_bias):
    heads, offsets, spread = rel_bias.shape
    slots = 2 * BIAS_BLOCKS + 2
    padded = jnp.pad(rel_bias, ((0, 0), (0, slots - offsets), (0, 128 - spread)))
    padded = padded.reshape(heads * slots, 128)

    def body(rel_ref, out_ref):
        query = lax.broadcasted_iota(jnp.int32, (GRID_W, 128), 0)
        lane = lax.broadcasted_iota(jnp.int32, (GRID_W, 128), 1)
        low = lane < GRID_W
        key = jnp.where(low, lane, lane - GRID_W)
        start = jnp.clip(query - WIN_COLS // 2, 0, GRID_W - WIN_COLS)
        inside = (key >= start) & (key < start + WIN_COLS)

        def diagonal(head, slot, move):
            row = jnp.broadcast_to(rel_ref[pl.ds(head * slots + slot, 1), :], (GRID_W, 128))
            return pltpu.roll(row, (128 - (WIN_COLS - 1) + move) % 128, 1, stride=1, stride_axis=0)

        for parity in range(2):
            for head in range(heads):
                for block in range(BIAS_BLOCKS):
                    slot = 2 * block + parity
                    both = jnp.where(
                        low, diagonal(head, slot, 0), diagonal(head, slot + 1, GRID_W)
                    )
                    out_ref[
                        parity, head * GRID_W : (head + 1) * GRID_W, block * 128 : (block + 1) * 128
                    ] = jnp.where(inside, both, MASKED)

    return pl.pallas_call(
        body,
        out_shape=jax.ShapeDtypeStruct((2, heads * GRID_W, BIAS_BLOCKS * 128), jnp.float32),
        name="bias_table",
    )(padded)


def attend(place, query, before, pair, after, ctx_pairs, table, ctx_bias, rows_all, per):
    samples, tokens, cols = query.shape
    heads = cols // HEAD_DIM
    rows_dev = tokens // GRID_W
    near_keys = WIN_ROWS * GRID_W
    ahead, behind = before.shape[1], after.shape[1]
    padded = ahead + tokens + behind
    lanes = -(-padded // 128) * 128
    ctx_rows = ctx_pairs[0].shape[2]
    members = [array.shape[0] for array in ctx_pairs]
    ctx_count = sum(members) * ctx_rows
    bf16, f32 = jnp.bfloat16, jnp.float32

    def body(place_ref, q_ref, before_ref, pair_ref, after_ref, *refs):
        ctx_refs = refs[: len(members)]
        table_ref, cb_ref, out_ref, near_t, far_t, values, far_values = refs[len(members) :]
        step = pl.program_id(1)

        @pl.when(step == 0)
        def _():
            values[0:ahead] = before_ref[0, :, cols:]
            values[ahead : ahead + tokens] = pair_ref[0, :, cols:]
            values[ahead + tokens : padded] = after_ref[0, :, cols:]
            at = 0
            for ctx_ref, count in zip(ctx_refs, members):
                for member in range(count):
                    low = at + member * ctx_rows
                    far_values[low : low + ctx_rows] = ctx_ref[member, 0, :, cols:]
                size = count * ctx_rows
                block = jnp.concatenate(
                    [ctx_ref[member, 0, :, :cols] for member in range(count)], axis=0
                )
                far_t[:, at : at + size] = block.T
                at += size
            fill = jnp.zeros((lanes - padded, cols), bf16)
            near_t[0, :, :ahead] = before_ref[0, :, :cols].T
            near_t[0, :, ahead : ahead + tokens] = pair_ref[0, :, :cols].T
            near_t[0, :, ahead + tokens :] = jnp.concatenate(
                [after_ref[0, :, :cols], fill], axis=0
            ).T
            near_t[1] = jnp.concatenate(
                [
                    before_ref[0, GRID_W:, :cols],
                    pair_ref[0, :, :cols],
                    after_ref[0, :, :cols],
                    fill,
                    jnp.zeros((GRID_W, cols), bf16),
                ],
                axis=0,
            ).T

        base = place_ref[0] * rows_dev
        lane = lax.broadcasted_iota(jnp.int32, (GRID_W, cols), 1)
        masks = [(lane >= h * HEAD_DIM) & (lane < (h + 1) * HEAD_DIM) for h in range(heads)]
        cb = jnp.concatenate(
            [jnp.full((GRID_W, 1), cb_ref[h], f32) for h in range(heads)], axis=0
        )
        spreads, nears, starts = [], [], []
        for r in range(per):
            actual = base + step * per + r
            start = jnp.clip(actual - REACH, 0, rows_all - WIN_ROWS)
            local = start - base + REACH
            offset = start - actual + WIN_ROWS - 1
            q = q_ref[0, r * GRID_W : (r + 1) * GRID_W]
            spread = jnp.concatenate(
                [jnp.where(mask, q, jnp.zeros_like(q)) for mask in masks], axis=0
            )
            spreads.append(spread)
            column = pl.multiple_of((local // 2) * 128, 128)
            keys_t = near_t[local % 2, :, pl.ds(column, near_keys)]
            bias_at = pl.multiple_of((offset // 2) * 128, 128)
            nears.append(
                jnp.dot(spread, keys_t, preferred_element_type=f32)
                + table_ref[offset % 2, :, pl.ds(bias_at, near_keys)]
            )
            starts.append(pl.multiple_of(local * GRID_W, GRID_W))
        for r in range(per):
            near = nears[r]
            far = jnp.dot(spreads[r], far_t[...], preferred_element_type=f32)
            top = jnp.maximum(
                jnp.max(near, axis=-1, keepdims=True), jnp.max(far, axis=-1, keepdims=True) + cb
            )
            near_exp = jnp.exp(near - top)
            far_exp = jnp.exp(far - (top - cb))
            total = jnp.sum(near_exp, axis=-1, keepdims=True) + jnp.sum(
                far_exp, axis=-1, keepdims=True
            )
            mixed = jnp.dot(
                near_exp.astype(bf16),
                values[pl.ds(starts[r], near_keys), :],
                preferred_element_type=f32,
            ) + jnp.dot(far_exp.astype(bf16), far_values[...], preferred_element_type=f32)
            mixed = mixed * (1.0 / total)
            result = jnp.where(masks[0], mixed[:GRID_W], 0.0)
            for h in range(1, heads):
                result = jnp.where(masks[h], mixed[h * GRID_W : (h + 1) * GRID_W], result)
            out_ref[r, 0] = result.astype(bf16)

    def of_sample(array):
        return pl.BlockSpec((1, *array.shape[1:]), lambda s, i: (s, 0, 0))

    return pl.pallas_call(
        body,
        grid=(samples, rows_dev // per),
        in_specs=[
            pl.BlockSpec(memory_space=pltpu.SMEM),
            pl.BlockSpec((1, per * GRID_W, cols), lambda s, i: (s, i, 0)),
            of_sample(before),
            of_sample(pair),
            of_sample(after),
        ]
        + [
            pl.BlockSpec((count, 1, ctx_rows, 2 * cols), lambda s, i: (0, s, 0, 0))
            for count in members
        ]
        + [whole(table.shape), pl.BlockSpec(memory_space=pltpu.SMEM)],
        out_specs=pl.BlockSpec((per, 1, GRID_W, cols), lambda s, i: (i, s, 0, 0)),
        out_shape=jax.ShapeDtypeStruct((rows_dev, samples, GRID_W, cols), bf16),
        scratch_shapes=[
            pltpu.VMEM((2, cols, lanes), bf16),
            pltpu.VMEM((cols, ctx_count), bf16),
            pltpu.VMEM((padded, cols), bf16),
            pltpu.VMEM((ctx_count, cols), bf16),
        ],
        name="attend",
    )(place, query, before, pair, after, *ctx_pairs, table, ctx_bias)


def finish(attended, w_out, latent, modulation, tiles):
    groups, _, _ = attended.shape
    samples, tokens, width = latent.shape
    block = modulation.shape[2] * tiles
    first = modulation.shape[1] - samples

    def body(att_ref, w_ref, latent_ref, tile_ref, out_ref):
        everything = jnp.concatenate([att_ref[group] for group in range(groups)], axis=1)
        update = jnp.dot(everything, w_ref[...], preferred_element_type=jnp.float32)
        for s in range(samples):
            gate = modulation_row(tile_ref, first + s)
            part = update[s * tokens : (s + 1) * tokens]
            out_ref[s] = (latent_ref[s].astype(jnp.float32) + gate * part).astype(jnp.bfloat16)

    return pl.pallas_call(
        body,
        grid=(width // block,),
        in_specs=[
            whole(attended.shape),
            pl.BlockSpec((width, block), lambda i: (0, i)),
            pl.BlockSpec((samples, tokens, block), lambda i: (0, 0, i)),
            pl.BlockSpec((tiles, *modulation.shape[1:]), lambda i: (i, 0, 0)),
        ],
        out_specs=pl.BlockSpec((samples, tokens, block), lambda i: (0, 0, i)),
        out_shape=jax.ShapeDtypeStruct(latent.shape, latent.dtype),
        name="finish",
    )(attended, w_out, latent, modulation)


def shifted(size, side, stride, value):
    span = side * stride
    return [(i, i // span * span + (i + value * stride) % span) for i in range(size)]


def from_line(block, axis, side, stride):
    size = lax.axis_size(axis)
    return [block] + [
        lax.ppermute(block, axis, shifted(size, side, stride, value)) for value in range(1, side)
    ]


def computation(
    latent,
    context,
    cond,
    ctx_cond,
    w_shift,
    w_scale,
    w_gate,
    norm_gain,
    w_query,
    w_key,
    w_value,
    w_out,
    rel_bias,
    ctx_bias,
):
    samples, tokens_dev, width = latent.shape
    local_cols = w_shift.shape[1]
    sp_index = lax.axis_index("sp")
    sp_size, tp_size = lax.axis_size("sp"), lax.axis_size("tp")
    place = jnp.full((1,), sp_index, jnp.int32)
    gathered = lax.all_gather(latent, "tp", axis=1, tiled=True)
    parts = modulation_parts(place, cond, ctx_cond, (w_shift, w_scale, w_gate), sp_size)
    parts, w_out_own = lax.optimization_barrier((parts, w_out))
    w_out_all = lax.all_gather(w_out_own, "tp", axis=0, tiled=True)
    table = bias_table(rel_bias)
    summed = jnp.sum(lax.all_to_all(parts, "sp", 0, 0, tiled=True), axis=0)
    summed, table = lax.optimization_barrier((summed, table))
    modulation = copy_for_each(summed, "tp")

    gain = norm_gain[None, :]
    ctx_rows = context.shape[1]
    (ctx_pair,) = project(
        context.reshape(1, samples * ctx_rows, width),
        gain,
        modulation,
        (w_key, w_value),
        samples,
        samples * ctx_rows,
        None,
    )
    ctx_pair = ctx_pair.reshape(samples, ctx_rows, 2 * local_cols)
    ctx_pairs = from_line(ctx_pair, "sp", 4, 1)
    up = [(i, i + 1) for i in range(sp_size - 1)]
    down = [(j, i) for i, j in up]
    ends = ((WIN_ROWS - REACH - 1) * GRID_W, REACH * GRID_W)
    w_triple = (w_key, w_value, w_query)
    outs = project(gathered, gain, modulation, w_triple, 0, 256, ends, 0)
    ctx_pairs, outs = lax.optimization_barrier((ctx_pairs, outs))
    ctx_line = jnp.stack(ctx_pairs)
    below = lax.ppermute(ctx_line, "sp", shifted(sp_size, 4, 4, 1))
    above = lax.ppermute(ctx_line, "sp", shifted(sp_size, 4, 4, 3))
    for s in range(1, samples):
        outs = project(gathered, gain, modulation, w_triple, 0, 256, ends, s, outs)
    pair, query, first, last = outs
    before = lax.ppermute(last, "sp", up)
    after = lax.ppermute(first, "sp", down)
    rows_all = pair.shape[1] // GRID_W * sp_size
    ctx_pairs = [
        ctx_line,
        below,
        above,
        lax.ppermute(below[:2], "sp", shifted(sp_size, 4, 4, 1)),
        lax.ppermute(above[2:], "sp", shifted(sp_size, 4, 4, 3)),
    ]
    attended = attend(
        place, query, before, pair, after, ctx_pairs, table, ctx_bias, rows_all, 4
    )
    attended = attended.reshape(tp_size, samples * tokens_dev, local_cols)
    attended = lax.all_to_all(attended, "tp", 0, 0, tiled=True)
    return finish(attended, w_out_all, latent, modulation, 4)


def solution(mesh):
    return jax.shard_map(
        computation,
        mesh=mesh,
        in_specs=(
            P(None, ("sp", "tp"), None),
            P(None, "sp", None),
            P(),
            P(),
            P("sp", "tp"),
            P("sp", "tp"),
            P("sp", "tp"),
            P(),
            P(None, "tp"),
            P(None, "tp"),
            P(None, "tp"),
            P("tp", None),
            P("tp", None, None),
            P("tp"),
        ),
        out_specs=P(None, ("sp", "tp"), None),
        check_vma=False,
    )
```

```python
import jax
import jax.numpy as jnp
from jax import lax
from jax.experimental import pallas as pl
from jax.experimental.pallas import tpu as pltpu
from jax.sharding import PartitionSpec as P


HEAD_DIM = 64
GRID_W = 64
WIN_ROWS = 8
WIN_COLS = 16
EPSILON = 1e-06
MASKED = -1e30
REACH = WIN_ROWS // 2
BIAS_BLOCKS = 7
RESIDENT = pl.BlockSpec(memory_space=pltpu.VMEM)


def copy_for_each(shard, axis):
    length = lax.axis_size(axis)
    return lax.all_to_all(
        jnp.broadcast_to(shard[None], (length, *shard.shape)), axis, 0, 0, tiled=True
    )


def silu_rows(values):
    return jax.nn.silu(values.astype(jnp.float32)).astype(jnp.bfloat16)


def modulation_parts(place, cond, ctx_cond, weights, copies):
    samples = cond.shape[0]
    rows, cols = weights[0].shape

    def body(place_ref, cond_ref, ctx_ref, shift_ref, scale_ref, gate_ref, out_ref, wide):
        at = pl.multiple_of(place_ref[0] * rows, rows)
        ada = silu_rows(cond_ref[:, pl.ds(at, rows)])
        wide[...] = ctx_ref[...].astype(jnp.float32).reshape(1, ctx_ref.shape[0])
        ada_ctx = silu_rows(wide[:, pl.ds(at, rows)])
        both = jnp.concatenate([ada.astype(jnp.float32), ada_ctx.astype(jnp.float32)], axis=0)
        both = both.astype(jnp.bfloat16)
        result = jnp.concatenate(
            [
                jnp.dot(both, shift_ref[...], preferred_element_type=jnp.float32),
                jnp.dot(both, scale_ref[...], preferred_element_type=jnp.float32),
                jnp.dot(ada, gate_ref[...], preferred_element_type=jnp.float32),
            ],
            axis=0,
        )
        for copy in range(copies):
            out_ref[copy] = result

    return pl.pallas_call(
        body,
        in_specs=[pl.BlockSpec(memory_space=pltpu.SMEM)]
        + [pl.BlockSpec(memory_space=pltpu.VMEM)] * 5,
        out_shape=jax.ShapeDtypeStruct((copies, 3 * samples + 2, cols), jnp.float32),
        scratch_shapes=[pltpu.VMEM((1, ctx_cond.shape[0]), jnp.float32)],
        compiler_params=pltpu.CompilerParams(vmem_limit_bytes=16 * 2**20),
        name="modulation_parts",
    )(place, cond, ctx_cond, *weights)


def resident(array):
    return pltpu.with_memory_space_constraint(array, pltpu.VMEM)


def whole(shape):
    return pl.BlockSpec(shape, lambda *_: (0,) * len(shape))


def modulation_row(tiles, row):
    return jnp.concatenate([tiles[tile, row : row + 1, :] for tile in range(tiles.shape[0])], axis=1)


def project(rows, gain, modulation, weights, row_of, block, ends, sample=None, buffers=()):
    samples, count, width = rows.shape
    every = modulation.shape[1] // 3 + 1
    chosen = range(samples) if sample is None else (sample,)
    begin = chosen[0]
    cols = weights[0].shape[1]
    first, last = ends if ends else (0, 0)
    steps = count // block

    def body(rows_ref, gain_ref, tiles_ref, *refs):
        weight_refs, out_refs = refs[: len(weights)], refs[len(weights) + len(buffers) : -2]
        factor_ref, shift_ref = refs[-2:]
        turn, step = pl.program_id(0), pl.program_id(1)

        for number in chosen:

            @pl.when((turn == number - begin) & (step == 0))
            def _(number=number):
                row = row_of + number
                factor_ref[...] = gain_ref[...] * (1.0 + modulation_row(tiles_ref, every + row))
                shift_ref[...] = modulation_row(tiles_ref, row)

        floats = rows_ref[0].astype(jnp.float32)
        inverse = lax.rsqrt(jnp.mean(floats * floats, axis=-1, keepdims=True) + EPSILON)
        hidden = (floats * inverse * factor_ref[...] + shift_ref[...]).astype(jnp.bfloat16)
        pair = [
            jnp.dot(hidden, ref[...], preferred_element_type=jnp.float32).astype(jnp.bfloat16)
            for ref in weight_refs[:2]
        ]
        if not ends:
            out_refs[0][0, :, :cols] = pair[0]
            out_refs[0][0, :, cols:] = pair[1]
            return
        out_refs[0][0, :, :cols] = pair[0]
        out_refs[0][0, :, cols:] = pair[1]
        query = jnp.dot(hidden, weight_refs[2][...], preferred_element_type=jnp.float32)
        query = query.astype(jnp.bfloat16).astype(jnp.float32) * HEAD_DIM**-0.5
        out_refs[1][0] = query.astype(jnp.bfloat16)
        for number in range(steps):
            low = number * block
            for out_ref, start, stop in (
                (out_refs[2], 0, first),
                (out_refs[3], count - last, count),
            ):
                lo, hi = max(low, start), min(low + block, stop)
                if lo < hi:

                    @pl.when(step == number)
                    def _(out_ref=out_ref, start=start, lo=lo, hi=hi, low=low):
                        for index in range(2):
                            out_ref[
                                0, lo - start : hi - start, index * cols : (index + 1) * cols
                            ] = pair[index][lo - low : hi - low]

    def blocks(size):
        return pl.BlockSpec((1, block, size), lambda s, i: (begin + s, i, 0))

    if ends:
        out_specs = [blocks(2 * cols), blocks(cols)]
        out_shape = [(samples, count, 2 * cols), (samples, count, cols)]
        for length in ends:
            out_specs += [pl.BlockSpec((1, length, 2 * cols), lambda s, i: (begin + s, 0, 0))]
            out_shape += [(samples, length, 2 * cols)]
    else:
        out_specs = [blocks(2 * cols)]
        out_shape = [(samples, count, 2 * cols)]
    return pl.pallas_call(
        body,
        grid=(len(chosen), steps),
        in_specs=[blocks(width), whole((1, width)), RESIDENT]
        + [RESIDENT] * len(weights)
        + [pl.BlockSpec(memory_space=pl.ANY)] * len(buffers),
        out_specs=out_specs,
        out_shape=[jax.ShapeDtypeStruct(shape, jnp.bfloat16) for shape in out_shape],
        scratch_shapes=[pltpu.VMEM((1, width), jnp.float32)] * 2,
        input_output_aliases={3 + len(weights) + i: i for i in range(len(buffers))},
        compiler_params=pltpu.CompilerParams(vmem_limit_bytes=24 * 2**20),
        name="project",
    )(rows, gain, modulation, *weights, *buffers)


def bias_table(rel_bias):
    heads, offsets, spread = rel_bias.shape
    slots = 2 * BIAS_BLOCKS + 2
    padded = jnp.pad(rel_bias, ((0, 0), (0, slots - offsets), (0, 128 - spread)))
    padded = padded.reshape(heads * slots, 128)

    def body(rel_ref, out_ref):
        query = lax.broadcasted_iota(jnp.int32, (GRID_W, 128), 0)
        lane = lax.broadcasted_iota(jnp.int32, (GRID_W, 128), 1)
        low = lane < GRID_W
        key = jnp.where(low, lane, lane - GRID_W)
        start = jnp.clip(query - WIN_COLS // 2, 0, GRID_W - WIN_COLS)
        inside = (key >= start) & (key < start + WIN_COLS)

        def diagonal(head, slot, move):
            row = jnp.broadcast_to(rel_ref[pl.ds(head * slots + slot, 1), :], (GRID_W, 128))
            return pltpu.roll(row, (128 - (WIN_COLS - 1) + move) % 128, 1, stride=1, stride_axis=0)

        for parity in range(2):
            for head in range(heads):
                for block in range(BIAS_BLOCKS):
                    slot = 2 * block + parity
                    both = jnp.where(
                        low, diagonal(head, slot, 0), diagonal(head, slot + 1, GRID_W)
                    )
                    out_ref[
                        parity, head * GRID_W : (head + 1) * GRID_W, block * 128 : (block + 1) * 128
                    ] = jnp.where(inside, both, MASKED)

    return pl.pallas_call(
        body,
        out_shape=jax.ShapeDtypeStruct((2, heads * GRID_W, BIAS_BLOCKS * 128), jnp.float32),
        compiler_params=pltpu.CompilerParams(vmem_limit_bytes=16 * 2**20),
        name="bias_table",
    )(padded)


def attend(place, query, before, pair, after, ctx_pairs, table, ctx_bias, rows_all, per):
    samples, tokens, cols = query.shape
    heads = cols // HEAD_DIM
    rows_dev = tokens // GRID_W
    near_keys = WIN_ROWS * GRID_W
    ahead, behind = before.shape[1], after.shape[1]
    padded = ahead + tokens + behind
    lanes = -(-padded // 128) * 128
    ctx_rows = ctx_pairs[0].shape[2]
    members = [array.shape[0] for array in ctx_pairs]
    ctx_count = sum(members) * ctx_rows
    bf16, f32 = jnp.bfloat16, jnp.float32

    def body(place_ref, q_ref, before_ref, pair_ref, after_ref, *refs):
        ctx_refs = refs[: len(members)]
        table_ref, cb_ref, out_ref, near_t, far_t, values, far_values = refs[len(members) :]
        sample, step = pl.program_id(0), pl.program_id(1)

        @pl.when(step == 0)
        def _():
            values[0:ahead] = before_ref[sample, :, cols:]
            values[ahead : ahead + tokens] = pair_ref[0, :, cols:]
            values[ahead + tokens : padded] = after_ref[sample, :, cols:]
            at = 0
            for ctx_ref, count in zip(ctx_refs, members):
                for member in range(count):
                    low = at + member * ctx_rows
                    far_values[low : low + ctx_rows] = ctx_ref[member, sample, :, cols:]
                size = count * ctx_rows
                block = jnp.concatenate(
                    [ctx_ref[member, sample, :, :cols] for member in range(count)], axis=0
                )
                far_t[:, at : at + size] = block.T
                at += size
            fill = jnp.zeros((lanes - padded, cols), bf16)
            near_t[0, :, :ahead] = before_ref[sample, :, :cols].T
            near_t[0, :, ahead : ahead + tokens] = pair_ref[0, :, :cols].T
            near_t[0, :, ahead + tokens :] = jnp.concatenate(
                [after_ref[sample, :, :cols], fill], axis=0
            ).T
            near_t[1] = jnp.concatenate(
                [
                    before_ref[sample, GRID_W:, :cols],
                    pair_ref[0, :, :cols],
                    after_ref[sample, :, :cols],
                    fill,
                    jnp.zeros((GRID_W, cols), bf16),
                ],
                axis=0,
            ).T

        base = place_ref[0] * rows_dev
        lane = lax.broadcasted_iota(jnp.int32, (GRID_W, cols), 1)
        masks = [(lane >= h * HEAD_DIM) & (lane < (h + 1) * HEAD_DIM) for h in range(heads)]
        cb = jnp.concatenate(
            [jnp.full((GRID_W, 1), cb_ref[h], f32) for h in range(heads)], axis=0
        )
        spreads, nears, starts = [], [], []
        for r in range(per):
            actual = base + step * per + r
            start = jnp.clip(actual - REACH, 0, rows_all - WIN_ROWS)
            local = start - base + REACH
            offset = start - actual + WIN_ROWS - 1
            q = q_ref[0, r * GRID_W : (r + 1) * GRID_W]
            spread = jnp.concatenate(
                [jnp.where(mask, q, jnp.zeros_like(q)) for mask in masks], axis=0
            )
            spreads.append(spread)
            column = pl.multiple_of((local // 2) * 128, 128)
            keys_t = near_t[local % 2, :, pl.ds(column, near_keys)]
            bias_at = pl.multiple_of((offset // 2) * 128, 128)
            nears.append(
                jnp.dot(spread, keys_t, preferred_element_type=f32)
                + table_ref[offset % 2, :, pl.ds(bias_at, near_keys)]
            )
            starts.append(pl.multiple_of(local * GRID_W, GRID_W))
        for r in range(per):
            near = nears[r]
            far = jnp.dot(spreads[r], far_t[...], preferred_element_type=f32)
            top = jnp.maximum(
                jnp.max(near, axis=-1, keepdims=True), jnp.max(far, axis=-1, keepdims=True) + cb
            )
            near_exp = jnp.exp(near - top)
            far_exp = jnp.exp(far - (top - cb))
            total = jnp.sum(near_exp, axis=-1, keepdims=True) + jnp.sum(
                far_exp, axis=-1, keepdims=True
            )
            mixed = jnp.dot(
                near_exp.astype(bf16),
                values[pl.ds(starts[r], near_keys), :],
                preferred_element_type=f32,
            ) + jnp.dot(far_exp.astype(bf16), far_values[...], preferred_element_type=f32)
            mixed = mixed * (1.0 / total)
            result = jnp.where(masks[0], mixed[:GRID_W], 0.0)
            for h in range(1, heads):
                result = jnp.where(masks[h], mixed[h * GRID_W : (h + 1) * GRID_W], result)
            out_ref[r, 0] = result.astype(bf16)

    def of_sample(array):
        return pl.BlockSpec((1, *array.shape[1:]), lambda s, i: (s, 0, 0))

    return pl.pallas_call(
        body,
        grid=(samples, rows_dev // per),
        in_specs=[
            pl.BlockSpec(memory_space=pltpu.SMEM),
            pl.BlockSpec((1, per * GRID_W, cols), lambda s, i: (s, i, 0)),
            RESIDENT,
            of_sample(pair),
            RESIDENT,
        ]
        + [RESIDENT] * len(members)
        + [RESIDENT, pl.BlockSpec(memory_space=pltpu.SMEM)],
        out_specs=pl.BlockSpec((per, 1, GRID_W, cols), lambda s, i: (i, s, 0, 0)),
        out_shape=jax.ShapeDtypeStruct((rows_dev, samples, GRID_W, cols), bf16),
        scratch_shapes=[
            pltpu.VMEM((2, cols, lanes), bf16),
            pltpu.VMEM((cols, ctx_count), bf16),
            pltpu.VMEM((padded, cols), bf16),
            pltpu.VMEM((ctx_count, cols), bf16),
        ],
        compiler_params=pltpu.CompilerParams(vmem_limit_bytes=32 * 2**20),
        name="attend",
    )(place, query, before, pair, after, *ctx_pairs, table, ctx_bias)


def finish(attended, w_out, latent, modulation, tiles):
    groups, _, _ = attended.shape
    samples, tokens, width = latent.shape
    block = modulation.shape[2] * tiles
    first = modulation.shape[1] - samples

    def body(att_ref, w_ref, latent_ref, tile_ref, out_ref):
        low = pl.program_id(0) * tiles
        everything = jnp.concatenate([att_ref[group] for group in range(groups)], axis=1)
        update = jnp.dot(everything, w_ref[...], preferred_element_type=jnp.float32)
        for s in range(samples):
            gate = jnp.concatenate(
                [tile_ref[low + t, first + s : first + s + 1, :] for t in range(tiles)], axis=1
            )
            part = update[s * tokens : (s + 1) * tokens]
            out_ref[s] = (latent_ref[s].astype(jnp.float32) + gate * part).astype(jnp.bfloat16)

    return pl.pallas_call(
        body,
        grid=(width // block,),
        in_specs=[
            whole(attended.shape),
            pl.BlockSpec((width, block), lambda i: (0, i)),
            pl.BlockSpec((samples, tokens, block), lambda i: (0, 0, i)),
            RESIDENT,
        ],
        out_specs=pl.BlockSpec((samples, tokens, block), lambda i: (0, 0, i)),
        out_shape=jax.ShapeDtypeStruct(latent.shape, latent.dtype),
        compiler_params=pltpu.CompilerParams(vmem_limit_bytes=24 * 2**20),
        name="finish",
    )(attended, w_out, latent, modulation)


def shifted(size, side, stride, value):
    span = side * stride
    return [(i, i // span * span + (i + value * stride) % span) for i in range(size)]


def from_line(block, axis, side, stride):
    size = lax.axis_size(axis)
    return [block] + [
        lax.ppermute(block, axis, shifted(size, side, stride, value)) for value in range(1, side)
    ]


def computation(
    latent,
    context,
    cond,
    ctx_cond,
    w_shift,
    w_scale,
    w_gate,
    norm_gain,
    w_query,
    w_key,
    w_value,
    w_out,
    rel_bias,
    ctx_bias,
):
    samples, tokens_dev, width = latent.shape
    local_cols = w_shift.shape[1]
    sp_index = lax.axis_index("sp")
    sp_size, tp_size = lax.axis_size("sp"), lax.axis_size("tp")
    place = jnp.full((1,), sp_index, jnp.int32)
    gathered = lax.all_gather(latent, "tp", axis=1, tiled=True)
    parts = modulation_parts(place, cond, ctx_cond, (w_shift, w_scale, w_gate), sp_size)
    parts, w_out_own = lax.optimization_barrier((parts, w_out))
    w_out_all = lax.all_gather(w_out_own, "tp", axis=0, tiled=True)
    table = bias_table(rel_bias)
    summed = jnp.sum(lax.all_to_all(parts, "sp", 0, 0, tiled=True), axis=0)
    summed, table = lax.optimization_barrier((summed, table))
    modulation = resident(copy_for_each(summed, "tp"))
    w_query, w_key, w_value = resident(w_query), resident(w_key), resident(w_value)
    table = resident(table)

    gain = norm_gain[None, :]
    ctx_rows = context.shape[1]
    (ctx_pair,) = project(
        context.reshape(1, samples * ctx_rows, width),
        gain,
        modulation,
        (w_key, w_value),
        samples,
        samples * ctx_rows,
        None,
    )
    ctx_pair = ctx_pair.reshape(samples, ctx_rows, 2 * local_cols)
    ctx_pairs = from_line(ctx_pair, "sp", 4, 1)
    up = [(i, i + 1) for i in range(sp_size - 1)]
    down = [(j, i) for i, j in up]
    ends = ((WIN_ROWS - REACH - 1) * GRID_W, REACH * GRID_W)
    w_triple = (w_key, w_value, w_query)
    outs = project(gathered, gain, modulation, w_triple, 0, 256, ends, 0)
    ctx_pairs, outs = lax.optimization_barrier((ctx_pairs, outs))
    ctx_line = jnp.stack(ctx_pairs)
    below = lax.ppermute(ctx_line, "sp", shifted(sp_size, 4, 4, 1))
    above = lax.ppermute(ctx_line, "sp", shifted(sp_size, 4, 4, 3))
    for s in range(1, samples):
        outs = project(gathered, gain, modulation, w_triple, 0, 256, ends, s, outs)
    pair, query, first, last = outs
    before = resident(lax.ppermute(last, "sp", up))
    after = resident(lax.ppermute(first, "sp", down))
    rows_all = pair.shape[1] // GRID_W * sp_size
    ctx_pairs = [
        ctx_line,
        below,
        above,
        lax.ppermute(below[:2], "sp", shifted(sp_size, 4, 4, 1)),
        lax.ppermute(above[2:], "sp", shifted(sp_size, 4, 4, 3)),
    ]
    ctx_pairs = [resident(array) for array in ctx_pairs]
    attended = attend(
        place, query, before, pair, after, ctx_pairs, table, ctx_bias, rows_all, 4
    )
    attended = attended.reshape(tp_size, samples * tokens_dev, local_cols)
    attended = lax.all_to_all(attended, "tp", 0, 0, tiled=True)
    return finish(attended, w_out_all, latent, modulation, 4)


def solution(mesh):
    return jax.shard_map(
        computation,
        mesh=mesh,
        in_specs=(
            P(None, ("sp", "tp"), None),
            P(None, "sp", None),
            P(),
            P(),
            P("sp", "tp"),
            P("sp", "tp"),
            P("sp", "tp"),
            P(),
            P(None, "tp"),
            P(None, "tp"),
            P(None, "tp"),
            P("tp", None),
            P("tp", None, None),
            P("tp"),
        ),
        out_specs=P(None, ("sp", "tp"), None),
        check_vma=False,
    )
```

```python
import jax
import jax.numpy as jnp
from jax import lax
from jax.experimental import pallas as pl
from jax.experimental.pallas import tpu as pltpu
from jax.sharding import PartitionSpec as P


HEAD_DIM = 64
GRID_W = 64
WIN_ROWS = 8
WIN_COLS = 16
EPSILON = 1e-06
MASKED = -1e30
REACH = WIN_ROWS // 2
BIAS_BLOCKS = 7
RESIDENT = pl.BlockSpec(memory_space=pltpu.VMEM)


def copy_for_each(shard, axis):
    length = lax.axis_size(axis)
    return lax.all_to_all(
        jnp.broadcast_to(shard[None], (length, *shard.shape)), axis, 0, 0, tiled=True
    )


def silu_rows(values):
    return jax.nn.silu(values.astype(jnp.float32)).astype(jnp.bfloat16)


def modulation_parts(place, cond, ctx_cond, weights, copies):
    samples = cond.shape[0]
    rows, cols = weights[0].shape

    def body(place_ref, cond_ref, ctx_ref, shift_ref, scale_ref, gate_ref, out_ref, wide):
        at = pl.multiple_of(place_ref[0] * rows, rows)
        ada = silu_rows(cond_ref[:, pl.ds(at, rows)])
        wide[...] = ctx_ref[...].astype(jnp.float32).reshape(1, ctx_ref.shape[0])
        ada_ctx = silu_rows(wide[:, pl.ds(at, rows)])
        both = jnp.concatenate([ada.astype(jnp.float32), ada_ctx.astype(jnp.float32)], axis=0)
        both = both.astype(jnp.bfloat16)
        result = jnp.concatenate(
            [
                jnp.dot(both, shift_ref[...], preferred_element_type=jnp.float32),
                jnp.dot(both, scale_ref[...], preferred_element_type=jnp.float32),
                jnp.dot(ada, gate_ref[...], preferred_element_type=jnp.float32),
            ],
            axis=0,
        )
        for copy in range(copies):
            out_ref[copy] = result

    return pl.pallas_call(
        body,
        in_specs=[pl.BlockSpec(memory_space=pltpu.SMEM)]
        + [pl.BlockSpec(memory_space=pltpu.VMEM)] * 5,
        out_shape=jax.ShapeDtypeStruct((copies, 3 * samples + 2, cols), jnp.float32),
        scratch_shapes=[pltpu.VMEM((1, ctx_cond.shape[0]), jnp.float32)],
        name="modulation_parts",
    )(place, cond, ctx_cond, *weights)


def resident(array):
    return pltpu.with_memory_space_constraint(array, pltpu.VMEM)


def whole(shape):
    return pl.BlockSpec(shape, lambda *_: (0,) * len(shape))


def modulation_row(tiles, row):
    return jnp.concatenate([tiles[tile, row : row + 1, :] for tile in range(tiles.shape[0])], axis=1)


def project(rows, gain, modulation, weights, row_of, block, ends, sample=None, buffers=()):
    samples, count, width = rows.shape
    every = modulation.shape[1] // 3 + 1
    chosen = range(samples) if sample is None else (sample,)
    begin = chosen[0]
    cols = weights[0].shape[1]
    first, last = ends if ends else (0, 0)
    steps = count // block

    def body(rows_ref, gain_ref, tiles_ref, *refs):
        weight_refs, out_refs = refs[: len(weights)], refs[len(weights) + len(buffers) : -2]
        factor_ref, shift_ref = refs[-2:]
        turn, step = pl.program_id(0), pl.program_id(1)

        for number in chosen:

            @pl.when((turn == number - begin) & (step == 0))
            def _(number=number):
                row = row_of + number
                factor_ref[...] = gain_ref[...] * (1.0 + modulation_row(tiles_ref, every + row))
                shift_ref[...] = modulation_row(tiles_ref, row)

        floats = rows_ref[0].astype(jnp.float32)
        inverse = lax.rsqrt(jnp.mean(floats * floats, axis=-1, keepdims=True) + EPSILON)
        hidden = (floats * inverse * factor_ref[...] + shift_ref[...]).astype(jnp.bfloat16)
        pair = [
            jnp.dot(hidden, ref[...], preferred_element_type=jnp.float32).astype(jnp.bfloat16)
            for ref in weight_refs[:2]
        ]
        if not ends:
            out_refs[0][0, :, :cols] = pair[0]
            out_refs[0][0, :, cols:] = pair[1]
            return
        out_refs[0][0, :, :cols] = pair[0]
        out_refs[0][0, :, cols:] = pair[1]
        query = jnp.dot(hidden, weight_refs[2][...], preferred_element_type=jnp.float32)
        query = query.astype(jnp.bfloat16).astype(jnp.float32) * HEAD_DIM**-0.5
        out_refs[1][0] = query.astype(jnp.bfloat16)
        for number in range(steps):
            low = number * block
            for out_ref, start, stop in (
                (out_refs[2], 0, first),
                (out_refs[3], count - last, count),
            ):
                lo, hi = max(low, start), min(low + block, stop)
                if lo < hi:

                    @pl.when(step == number)
                    def _(out_ref=out_ref, start=start, lo=lo, hi=hi, low=low):
                        for index in range(2):
                            out_ref[
                                0, lo - start : hi - start, index * cols : (index + 1) * cols
                            ] = pair[index][lo - low : hi - low]

    def blocks(size):
        return pl.BlockSpec((1, block, size), lambda s, i: (begin + s, i, 0))

    if ends:
        out_specs = [blocks(2 * cols), blocks(cols)]
        out_shape = [(samples, count, 2 * cols), (samples, count, cols)]
        for length in ends:
            out_specs += [pl.BlockSpec((1, length, 2 * cols), lambda s, i: (begin + s, 0, 0))]
            out_shape += [(samples, length, 2 * cols)]
    else:
        out_specs = [blocks(2 * cols)]
        out_shape = [(samples, count, 2 * cols)]
    return pl.pallas_call(
        body,
        grid=(len(chosen), steps),
        in_specs=[blocks(width), whole((1, width)), RESIDENT]
        + [RESIDENT] * len(weights)
        + [pl.BlockSpec(memory_space=pl.ANY)] * len(buffers),
        out_specs=out_specs,
        out_shape=[jax.ShapeDtypeStruct(shape, jnp.bfloat16) for shape in out_shape],
        scratch_shapes=[pltpu.VMEM((1, width), jnp.float32)] * 2,
        input_output_aliases={3 + len(weights) + i: i for i in range(len(buffers))},
        compiler_params=pltpu.CompilerParams(vmem_limit_bytes=24 * 2**20),
        name="project",
    )(rows, gain, modulation, *weights, *buffers)


def bias_table(rel_bias):
    heads, offsets, spread = rel_bias.shape
    slots = 2 * BIAS_BLOCKS + 2
    padded = jnp.pad(rel_bias, ((0, 0), (0, slots - offsets), (0, 128 - spread)))
    padded = padded.reshape(heads * slots, 128)

    def body(rel_ref, out_ref):
        query = lax.broadcasted_iota(jnp.int32, (GRID_W, 128), 0)
        lane = lax.broadcasted_iota(jnp.int32, (GRID_W, 128), 1)
        low = lane < GRID_W
        key = jnp.where(low, lane, lane - GRID_W)
        start = jnp.clip(query - WIN_COLS // 2, 0, GRID_W - WIN_COLS)
        inside = (key >= start) & (key < start + WIN_COLS)

        def diagonal(head, slot, move):
            row = jnp.broadcast_to(rel_ref[pl.ds(head * slots + slot, 1), :], (GRID_W, 128))
            return pltpu.roll(row, (128 - (WIN_COLS - 1) + move) % 128, 1, stride=1, stride_axis=0)

        for parity in range(2):
            for head in range(heads):
                for block in range(BIAS_BLOCKS):
                    slot = 2 * block + parity
                    both = jnp.where(
                        low, diagonal(head, slot, 0), diagonal(head, slot + 1, GRID_W)
                    )
                    out_ref[
                        parity, head * GRID_W : (head + 1) * GRID_W, block * 128 : (block + 1) * 128
                    ] = jnp.where(inside, both, MASKED)

    return pl.pallas_call(
        body,
        out_shape=jax.ShapeDtypeStruct((2, heads * GRID_W, BIAS_BLOCKS * 128), jnp.float32),
        compiler_params=pltpu.CompilerParams(vmem_limit_bytes=16 * 2**20),
        name="bias_table",
    )(padded)


def head_masks(cols):
    lane = lax.broadcasted_iota(jnp.int32, (GRID_W, cols), 1)
    return [(lane >= low) & (lane < low + HEAD_DIM) for low in range(0, cols, HEAD_DIM)]


def spread_heads(query, masks):
    return jnp.concatenate(
        [jnp.where(mask, query, jnp.zeros_like(query)) for mask in masks], axis=0
    )


def gather_heads(values, masks):
    result = jnp.where(masks[0], values[:GRID_W], 0.0)
    for h in range(1, len(masks)):
        result = jnp.where(masks[h], values[h * GRID_W : (h + 1) * GRID_W], result)
    return result


def weighed(scores, values, masks):
    top = jnp.max(scores, axis=-1, keepdims=True)
    exps = jnp.exp(scores - top)
    total = jnp.sum(exps, axis=-1, keepdims=True)
    mixed = jnp.dot(exps.astype(jnp.bfloat16), values, preferred_element_type=jnp.float32)
    return [gather_heads(array, masks) for array in (mixed, top, total)]


def attend_near(place, query, before, pair, after, table, rows_all, per):
    samples, tokens, cols = query.shape
    rows_dev = tokens // GRID_W
    near_keys = WIN_ROWS * GRID_W
    ahead, behind = before.shape[1], after.shape[1]
    padded = ahead + tokens + behind
    lanes = -(-padded // 128) * 128
    bf16, f32 = jnp.bfloat16, jnp.float32

    def body(place_ref, q_ref, before_ref, pair_ref, after_ref, table_ref, *refs):
        out_refs, (near_t, values) = refs[:3], refs[3:]
        sample, step = pl.program_id(0), pl.program_id(1)

        @pl.when(step == 0)
        def _():
            values[0:ahead] = before_ref[sample, :, cols:]
            values[ahead : ahead + tokens] = pair_ref[0, :, cols:]
            values[ahead + tokens : padded] = after_ref[sample, :, cols:]
            fill = jnp.zeros((lanes - padded, cols), bf16)
            near_t[0, :, :ahead] = before_ref[sample, :, :cols].T
            near_t[0, :, ahead : ahead + tokens] = pair_ref[0, :, :cols].T
            near_t[0, :, ahead + tokens :] = jnp.concatenate(
                [after_ref[sample, :, :cols], fill], axis=0
            ).T
            near_t[1] = jnp.concatenate(
                [
                    before_ref[sample, GRID_W:, :cols],
                    pair_ref[0, :, :cols],
                    after_ref[sample, :, :cols],
                    fill,
                    jnp.zeros((GRID_W, cols), bf16),
                ],
                axis=0,
            ).T

        base = place_ref[0] * rows_dev
        masks = head_masks(cols)
        scores, starts = [], []
        for r in range(per):
            actual = base + step * per + r
            start = jnp.clip(actual - REACH, 0, rows_all - WIN_ROWS)
            local = start - base + REACH
            offset = start - actual + WIN_ROWS - 1
            spread = spread_heads(q_ref[0, r * GRID_W : (r + 1) * GRID_W], masks)
            column = pl.multiple_of((local // 2) * 128, 128)
            keys_t = near_t[local % 2, :, pl.ds(column, near_keys)]
            bias_at = pl.multiple_of((offset // 2) * 128, 128)
            scores.append(
                jnp.dot(spread, keys_t, preferred_element_type=f32)
                + table_ref[offset % 2, :, pl.ds(bias_at, near_keys)]
            )
            starts.append(pl.multiple_of(local * GRID_W, GRID_W))
        for r in range(per):
            parts = weighed(scores[r], values[pl.ds(starts[r], near_keys), :], masks)
            for out_ref, part in zip(out_refs, parts):
                out_ref[0, r * GRID_W : (r + 1) * GRID_W] = part

    def of_sample(array):
        return pl.BlockSpec((1, *array.shape[1:]), lambda s, i: (s, 0, 0))

    rows_spec = pl.BlockSpec((1, per * GRID_W, cols), lambda s, i: (s, i, 0))
    return pl.pallas_call(
        body,
        grid=(samples, rows_dev // per),
        in_specs=[
            pl.BlockSpec(memory_space=pltpu.SMEM),
            rows_spec,
            RESIDENT,
            of_sample(pair),
            RESIDENT,
            RESIDENT,
        ],
        out_specs=[rows_spec] * 3,
        out_shape=[jax.ShapeDtypeStruct((samples, tokens, cols), f32)] * 3,
        scratch_shapes=[
            pltpu.VMEM((2, cols, lanes), bf16),
            pltpu.VMEM((padded, cols), bf16),
        ],
        compiler_params=pltpu.CompilerParams(vmem_limit_bytes=32 * 2**20),
        name="attend_near",
    )(place, query, before, pair, after, table)


def attend_far(query, ctx_pairs, ctx_bias, near, per):
    samples, tokens, cols = query.shape
    rows_dev = tokens // GRID_W
    ctx_rows = ctx_pairs[0].shape[2]
    members = [array.shape[0] for array in ctx_pairs]
    ctx_count = sum(members) * ctx_rows
    bf16, f32 = jnp.bfloat16, jnp.float32

    def body(q_ref, *refs):
        ctx_refs = refs[: len(members)]
        cb_ref, mixed_ref, top_ref, total_ref, out_ref, far_t, values = refs[len(members) :]
        sample, step = pl.program_id(0), pl.program_id(1)

        @pl.when(step == 0)
        def _():
            at = 0
            for ctx_ref, count in zip(ctx_refs, members):
                for member in range(count):
                    low = at + member * ctx_rows
                    values[low : low + ctx_rows] = ctx_ref[member, sample, :, cols:]
                size = count * ctx_rows
                block = jnp.concatenate(
                    [ctx_ref[member, sample, :, :cols] for member in range(count)], axis=0
                )
                far_t[:, at : at + size] = block.T
                at += size

        masks = head_masks(cols)
        context_bias = jnp.concatenate(
            [jnp.full((GRID_W, cols), cb_ref[h], f32) for h in range(len(masks))], axis=0
        )
        scores = [
            jnp.dot(
                spread_heads(q_ref[0, r * GRID_W : (r + 1) * GRID_W], masks),
                far_t[...],
                preferred_element_type=f32,
            )
            for r in range(per)
        ]
        for r in range(per):
            mixed, top, total = weighed(scores[r], values[...], masks)
            at = slice(r * GRID_W, (r + 1) * GRID_W)
            top = top + gather_heads(context_bias, masks)
            near_top = top_ref[0, at]
            highest = jnp.maximum(top, near_top)
            far_part = jnp.exp(top - highest)
            near_part = jnp.exp(near_top - highest)
            total = total * far_part + total_ref[0, at] * near_part
            mixed = mixed * far_part + mixed_ref[0, at] * near_part
            out_ref[r, 0] = (mixed / total).astype(bf16)

    rows_spec = pl.BlockSpec((1, per * GRID_W, cols), lambda s, i: (s, i, 0))
    return pl.pallas_call(
        body,
        grid=(samples, rows_dev // per),
        in_specs=[
            rows_spec,
        ]
        + [RESIDENT] * len(members)
        + [pl.BlockSpec(memory_space=pltpu.SMEM)]
        + [rows_spec] * 3,
        out_specs=pl.BlockSpec((per, 1, GRID_W, cols), lambda s, i: (i, s, 0, 0)),
        out_shape=jax.ShapeDtypeStruct((rows_dev, samples, GRID_W, cols), bf16),
        scratch_shapes=[
            pltpu.VMEM((cols, ctx_count), bf16),
            pltpu.VMEM((ctx_count, cols), bf16),
        ],
        compiler_params=pltpu.CompilerParams(vmem_limit_bytes=32 * 2**20),
        name="attend_far",
    )(query, *ctx_pairs, ctx_bias, *near)


def finish(attended, w_out, latent, modulation, tiles):
    groups, _, _ = attended.shape
    samples, tokens, width = latent.shape
    block = modulation.shape[2] * tiles
    first = modulation.shape[1] - samples

    def body(att_ref, w_ref, latent_ref, tile_ref, out_ref):
        low = pl.program_id(0) * tiles
        everything = jnp.concatenate([att_ref[group] for group in range(groups)], axis=1)
        update = jnp.dot(everything, w_ref[...], preferred_element_type=jnp.float32)
        for s in range(samples):
            gate = jnp.concatenate(
                [tile_ref[low + t, first + s : first + s + 1, :] for t in range(tiles)], axis=1
            )
            part = update[s * tokens : (s + 1) * tokens]
            out_ref[s] = (latent_ref[s].astype(jnp.float32) + gate * part).astype(jnp.bfloat16)

    return pl.pallas_call(
        body,
        grid=(width // block,),
        in_specs=[
            whole(attended.shape),
            pl.BlockSpec((width, block), lambda i: (0, i)),
            pl.BlockSpec((samples, tokens, block), lambda i: (0, 0, i)),
            RESIDENT,
        ],
        out_specs=pl.BlockSpec((samples, tokens, block), lambda i: (0, 0, i)),
        out_shape=jax.ShapeDtypeStruct(latent.shape, latent.dtype),
        name="finish",
    )(attended, w_out, latent, modulation)


def shifted(size, side, stride, value):
    span = side * stride
    return [(i, i // span * span + (i + value * stride) % span) for i in range(size)]


def from_line(block, axis, side, stride):
    size = lax.axis_size(axis)
    return [block] + [
        lax.ppermute(block, axis, shifted(size, side, stride, value)) for value in range(1, side)
    ]


def computation(
    latent,
    context,
    cond,
    ctx_cond,
    w_shift,
    w_scale,
    w_gate,
    norm_gain,
    w_query,
    w_key,
    w_value,
    w_out,
    rel_bias,
    ctx_bias,
):
    samples, tokens_dev, width = latent.shape
    local_cols = w_shift.shape[1]
    sp_index = lax.axis_index("sp")
    sp_size, tp_size = lax.axis_size("sp"), lax.axis_size("tp")
    place = jnp.full((1,), sp_index, jnp.int32)
    gathered = lax.all_gather(latent, "tp", axis=1, tiled=True)
    parts = modulation_parts(place, cond, ctx_cond, (w_shift, w_scale, w_gate), sp_size)
    parts, w_out_own = lax.optimization_barrier((parts, w_out))
    w_out_all = lax.all_gather(w_out_own, "tp", axis=0, tiled=True)
    table = bias_table(rel_bias)
    summed = jnp.sum(lax.all_to_all(parts, "sp", 0, 0, tiled=True), axis=0)
    summed, table = lax.optimization_barrier((summed, table))
    modulation = resident(copy_for_each(summed, "tp"))
    w_query, w_key, w_value = resident(w_query), resident(w_key), resident(w_value)
    table = resident(table)

    gain = norm_gain[None, :]
    ctx_rows = context.shape[1]
    (ctx_pair,) = project(
        context.reshape(1, samples * ctx_rows, width),
        gain,
        modulation,
        (w_key, w_value),
        samples,
        samples * ctx_rows,
        None,
    )
    ctx_pair = ctx_pair.reshape(samples, ctx_rows, 2 * local_cols)
    ctx_pairs = from_line(ctx_pair, "sp", 4, 1)
    up = [(i, i + 1) for i in range(sp_size - 1)]
    down = [(j, i) for i, j in up]
    gathered = pltpu.with_memory_space_constraint(gathered, pltpu.HBM)
    ends = ((WIN_ROWS - REACH - 1) * GRID_W, REACH * GRID_W)
    w_triple = (w_key, w_value, w_query)
    outs = project(gathered, gain, modulation, w_triple, 0, 256, ends, 0)
    ctx_pairs, outs = lax.optimization_barrier((ctx_pairs, outs))
    ctx_line = jnp.stack(ctx_pairs)
    below = lax.ppermute(ctx_line, "sp", shifted(sp_size, 4, 4, 1))
    above = lax.ppermute(ctx_line, "sp", shifted(sp_size, 4, 4, 3))
    for s in range(1, samples):
        outs = project(gathered, gain, modulation, w_triple, 0, 256, ends, s, outs)
    pair, query, first, last = outs
    before = resident(lax.ppermute(last, "sp", up))
    after = resident(lax.ppermute(first, "sp", down))
    rows_all = pair.shape[1] // GRID_W * sp_size
    ctx_pairs = [
        ctx_line,
        below,
        above,
        lax.ppermute(below[:2], "sp", shifted(sp_size, 4, 4, 1)),
        lax.ppermute(above[2:], "sp", shifted(sp_size, 4, 4, 3)),
    ]
    ctx_pairs = [resident(array) for array in ctx_pairs]
    near = attend_near(place, query, before, pair, after, table, rows_all, 4)
    attended = attend_far(query, ctx_pairs, ctx_bias, near, 4)
    attended = attended.reshape(tp_size, samples * tokens_dev, local_cols)
    attended = lax.all_to_all(attended, "tp", 0, 0, tiled=True)
    return finish(attended, w_out_all, latent, modulation, 4)


def solution(mesh):
    return jax.shard_map(
        computation,
        mesh=mesh,
        in_specs=(
            P(None, ("sp", "tp"), None),
            P(None, "sp", None),
            P(),
            P(),
            P("sp", "tp"),
            P("sp", "tp"),
            P("sp", "tp"),
            P(),
            P(None, "tp"),
            P(None, "tp"),
            P(None, "tp"),
            P("tp", None),
            P("tp", None, None),
            P("tp"),
        ),
        out_specs=P(None, ("sp", "tp"), None),
        check_vma=False,
    )
```

```python
import jax
import jax.numpy as jnp
from jax import lax
from jax.experimental import pallas as pl
from jax.experimental.pallas import tpu as pltpu
from jax.sharding import PartitionSpec as P


HEAD_DIM = 64
GRID_W = 64
WIN_ROWS = 8
WIN_COLS = 16
EPSILON = 1e-06
MASKED = -1e30
REACH = WIN_ROWS // 2
BIAS_BLOCKS = 7
RESIDENT = pl.BlockSpec(memory_space=pltpu.VMEM)


def copy_for_each(shard, axis):
    length = lax.axis_size(axis)
    return lax.all_to_all(
        jnp.broadcast_to(shard[None], (length, *shard.shape)), axis, 0, 0, tiled=True
    )


def silu_rows(values):
    return jax.nn.silu(values.astype(jnp.float32)).astype(jnp.bfloat16)


def modulation_parts(place, cond, ctx_cond, weights, copies):
    samples = cond.shape[0]
    rows, cols = weights[0].shape

    def body(place_ref, cond_ref, ctx_ref, shift_ref, scale_ref, gate_ref, out_ref, wide):
        at = pl.multiple_of(place_ref[0] * rows, rows)
        ada = silu_rows(cond_ref[:, pl.ds(at, rows)])
        wide[...] = ctx_ref[...].astype(jnp.float32).reshape(1, ctx_ref.shape[0])
        ada_ctx = silu_rows(wide[:, pl.ds(at, rows)])
        both = jnp.concatenate([ada.astype(jnp.float32), ada_ctx.astype(jnp.float32)], axis=0)
        both = both.astype(jnp.bfloat16)
        result = jnp.concatenate(
            [
                jnp.dot(both, shift_ref[...], preferred_element_type=jnp.float32),
                jnp.dot(both, scale_ref[...], preferred_element_type=jnp.float32),
                jnp.dot(ada, gate_ref[...], preferred_element_type=jnp.float32),
            ],
            axis=0,
        )
        for copy in range(copies):
            out_ref[copy] = result

    return pl.pallas_call(
        body,
        in_specs=[pl.BlockSpec(memory_space=pltpu.SMEM)]
        + [pl.BlockSpec(memory_space=pltpu.VMEM)] * 5,
        out_shape=jax.ShapeDtypeStruct((copies, 3 * samples + 2, cols), jnp.float32),
        scratch_shapes=[pltpu.VMEM((1, ctx_cond.shape[0]), jnp.float32)],
        name="modulation_parts",
    )(place, cond, ctx_cond, *weights)


def resident(array):
    return pltpu.with_memory_space_constraint(array, pltpu.VMEM)


def whole(shape):
    return pl.BlockSpec(shape, lambda *_: (0,) * len(shape))


def modulation_row(tiles, row):
    return jnp.concatenate([tiles[tile, row : row + 1, :] for tile in range(tiles.shape[0])], axis=1)


def project(rows, gain, modulation, weights, row_of, block, ends, sample=None, buffers=()):
    samples, count, width = rows.shape
    every = modulation.shape[1] // 3 + 1
    chosen = range(samples) if sample is None else (sample,)
    begin = chosen[0]
    cols = weights[0].shape[1]
    first, last = ends if ends else (0, 0)
    steps = count // block

    def body(rows_ref, gain_ref, tiles_ref, *refs):
        weight_refs, out_refs = refs[: len(weights)], refs[len(weights) + len(buffers) : -2]
        factor_ref, shift_ref = refs[-2:]
        turn, step = pl.program_id(0), pl.program_id(1)

        for number in chosen:

            @pl.when((turn == number - begin) & (step == 0))
            def _(number=number):
                row = row_of + number
                factor_ref[...] = gain_ref[...] * (1.0 + modulation_row(tiles_ref, every + row))
                shift_ref[...] = modulation_row(tiles_ref, row)

        floats = rows_ref[0].astype(jnp.float32)
        inverse = lax.rsqrt(jnp.mean(floats * floats, axis=-1, keepdims=True) + EPSILON)
        hidden = (floats * inverse * factor_ref[...] + shift_ref[...]).astype(jnp.bfloat16)
        pair = [
            jnp.dot(hidden, ref[...], preferred_element_type=jnp.float32).astype(jnp.bfloat16)
            for ref in weight_refs[:2]
        ]
        if not ends:
            out_refs[0][0, :, :cols] = pair[0]
            out_refs[0][0, :, cols:] = pair[1]
            return
        out_refs[0][0, :, :cols] = pair[0]
        out_refs[0][0, :, cols:] = pair[1]
        query = jnp.dot(hidden, weight_refs[2][...], preferred_element_type=jnp.float32)
        query = query.astype(jnp.bfloat16).astype(jnp.float32) * HEAD_DIM**-0.5
        out_refs[1][0] = query.astype(jnp.bfloat16)
        for number in range(steps):
            low = number * block
            for out_ref, start, stop in (
                (out_refs[2], 0, first),
                (out_refs[3], count - last, count),
            ):
                lo, hi = max(low, start), min(low + block, stop)
                if lo < hi:

                    @pl.when(step == number)
                    def _(out_ref=out_ref, start=start, lo=lo, hi=hi, low=low):
                        for index in range(2):
                            out_ref[
                                0, lo - start : hi - start, index * cols : (index + 1) * cols
                            ] = pair[index][lo - low : hi - low]

    def blocks(size):
        return pl.BlockSpec((1, block, size), lambda s, i: (begin + s, i, 0))

    if ends:
        out_specs = [blocks(2 * cols), blocks(cols)]
        out_shape = [(samples, count, 2 * cols), (samples, count, cols)]
        for length in ends:
            out_specs += [pl.BlockSpec((1, length, 2 * cols), lambda s, i: (begin + s, 0, 0))]
            out_shape += [(samples, length, 2 * cols)]
    else:
        out_specs = [blocks(2 * cols)]
        out_shape = [(samples, count, 2 * cols)]
    return pl.pallas_call(
        body,
        grid=(len(chosen), steps),
        in_specs=[blocks(width), whole((1, width)), RESIDENT]
        + [RESIDENT] * len(weights)
        + [pl.BlockSpec(memory_space=pl.ANY)] * len(buffers),
        out_specs=out_specs,
        out_shape=[jax.ShapeDtypeStruct(shape, jnp.bfloat16) for shape in out_shape],
        scratch_shapes=[pltpu.VMEM((1, width), jnp.float32)] * 2,
        input_output_aliases={3 + len(weights) + i: i for i in range(len(buffers))},
        compiler_params=pltpu.CompilerParams(vmem_limit_bytes=24 * 2**20),
        name="project",
    )(rows, gain, modulation, *weights, *buffers)


def bias_table(rel_bias):
    heads, offsets, spread = rel_bias.shape
    slots = 2 * BIAS_BLOCKS + 2
    padded = jnp.pad(rel_bias, ((0, 0), (0, slots - offsets), (0, 128 - spread)))
    padded = padded.reshape(heads * slots, 128)

    def body(rel_ref, out_ref):
        query = lax.broadcasted_iota(jnp.int32, (GRID_W, 128), 0)
        lane = lax.broadcasted_iota(jnp.int32, (GRID_W, 128), 1)
        low = lane < GRID_W
        key = jnp.where(low, lane, lane - GRID_W)
        start = jnp.clip(query - WIN_COLS // 2, 0, GRID_W - WIN_COLS)
        inside = (key >= start) & (key < start + WIN_COLS)

        def diagonal(head, slot, move):
            row = jnp.broadcast_to(rel_ref[pl.ds(head * slots + slot, 1), :], (GRID_W, 128))
            return pltpu.roll(row, (128 - (WIN_COLS - 1) + move) % 128, 1, stride=1, stride_axis=0)

        for parity in range(2):
            for head in range(heads):
                for block in range(BIAS_BLOCKS):
                    slot = 2 * block + parity
                    both = jnp.where(
                        low, diagonal(head, slot, 0), diagonal(head, slot + 1, GRID_W)
                    )
                    out_ref[
                        parity, head * GRID_W : (head + 1) * GRID_W, block * 128 : (block + 1) * 128
                    ] = jnp.where(inside, both, MASKED)

    return pl.pallas_call(
        body,
        out_shape=jax.ShapeDtypeStruct((2, heads * GRID_W, BIAS_BLOCKS * 128), jnp.float32),
        compiler_params=pltpu.CompilerParams(vmem_limit_bytes=16 * 2**20),
        name="bias_table",
    )(padded)


def head_masks(cols):
    lane = lax.broadcasted_iota(jnp.int32, (GRID_W, cols), 1)
    return [(lane >= low) & (lane < low + HEAD_DIM) for low in range(0, cols, HEAD_DIM)]


def spread_heads(query, masks):
    return jnp.concatenate(
        [jnp.where(mask, query, jnp.zeros_like(query)) for mask in masks], axis=0
    )


def gather_heads(values, masks):
    result = jnp.where(masks[0], values[:GRID_W], 0.0)
    for h in range(1, len(masks)):
        result = jnp.where(masks[h], values[h * GRID_W : (h + 1) * GRID_W], result)
    return result


def weighed(scores, values, masks):
    top = jnp.max(scores, axis=-1, keepdims=True)
    exps = jnp.exp(scores - top)
    total = jnp.sum(exps, axis=-1, keepdims=True)
    mixed = jnp.dot(exps.astype(jnp.bfloat16), values, preferred_element_type=jnp.float32)
    return [gather_heads(array, masks) for array in (mixed, top, total)]


def attend_near(place, query, before, pair, after, table, far, rows_all, per):
    samples, tokens, cols = query.shape
    rows_dev = tokens // GRID_W
    near_keys = WIN_ROWS * GRID_W
    ahead, behind = before.shape[1], after.shape[1]
    padded = ahead + tokens + behind
    lanes = -(-padded // 128) * 128
    bf16, f32 = jnp.bfloat16, jnp.float32

    def body(place_ref, q_ref, before_ref, pair_ref, after_ref, table_ref, *refs):
        mixed_ref, top_ref, total_ref, out_ref, near_t, values = refs
        sample, step = pl.program_id(0), pl.program_id(1)

        @pl.when(step == 0)
        def _():
            values[0:ahead] = before_ref[sample, :, cols:]
            values[ahead : ahead + tokens] = pair_ref[0, :, cols:]
            values[ahead + tokens : padded] = after_ref[sample, :, cols:]
            fill = jnp.zeros((lanes - padded, cols), bf16)
            near_t[0, :, :ahead] = before_ref[sample, :, :cols].T
            near_t[0, :, ahead : ahead + tokens] = pair_ref[0, :, :cols].T
            near_t[0, :, ahead + tokens :] = jnp.concatenate(
                [after_ref[sample, :, :cols], fill], axis=0
            ).T
            near_t[1] = jnp.concatenate(
                [
                    before_ref[sample, GRID_W:, :cols],
                    pair_ref[0, :, :cols],
                    after_ref[sample, :, :cols],
                    fill,
                    jnp.zeros((GRID_W, cols), bf16),
                ],
                axis=0,
            ).T

        base = place_ref[0] * rows_dev
        masks = head_masks(cols)
        scores, starts = [], []
        for r in range(per):
            actual = base + step * per + r
            start = jnp.clip(actual - REACH, 0, rows_all - WIN_ROWS)
            local = start - base + REACH
            offset = start - actual + WIN_ROWS - 1
            spread = spread_heads(q_ref[0, r * GRID_W : (r + 1) * GRID_W], masks)
            column = pl.multiple_of((local // 2) * 128, 128)
            keys_t = near_t[local % 2, :, pl.ds(column, near_keys)]
            bias_at = pl.multiple_of((offset // 2) * 128, 128)
            scores.append(
                jnp.dot(spread, keys_t, preferred_element_type=f32)
                + table_ref[offset % 2, :, pl.ds(bias_at, near_keys)]
            )
            starts.append(pl.multiple_of(local * GRID_W, GRID_W))
        for r in range(per):
            parts = weighed(scores[r], values[pl.ds(starts[r], near_keys), :], masks)
            mixed, top, total = parts
            at = slice(r * GRID_W, (r + 1) * GRID_W)
            far_top = top_ref[0, at]
            highest = jnp.maximum(top, far_top)
            near_part = jnp.exp(top - highest)
            far_part = jnp.exp(far_top - highest)
            total = total * near_part + total_ref[0, at] * far_part
            mixed = mixed * near_part + mixed_ref[0, at] * far_part
            out_ref[r, 0] = (mixed / total).astype(bf16)

    def of_sample(array):
        return pl.BlockSpec((1, *array.shape[1:]), lambda s, i: (s, 0, 0))

    rows_spec = pl.BlockSpec((1, per * GRID_W, cols), lambda s, i: (s, i, 0))
    return pl.pallas_call(
        body,
        grid=(samples, rows_dev // per),
        in_specs=[
            pl.BlockSpec(memory_space=pltpu.SMEM),
            rows_spec,
            RESIDENT,
            of_sample(pair),
            RESIDENT,
            RESIDENT,
        ]
        + [rows_spec] * 3,
        out_specs=pl.BlockSpec((per, 1, GRID_W, cols), lambda s, i: (i, s, 0, 0)),
        out_shape=jax.ShapeDtypeStruct((rows_dev, samples, GRID_W, cols), bf16),
        scratch_shapes=[
            pltpu.VMEM((2, cols, lanes), bf16),
            pltpu.VMEM((padded, cols), bf16),
        ],
        compiler_params=pltpu.CompilerParams(vmem_limit_bytes=32 * 2**20),
        name="attend_near",
    )(place, query, before, pair, after, table, *far)


def attend_far(query, ctx_pairs, ctx_bias, per):
    samples, tokens, cols = query.shape
    rows_dev = tokens // GRID_W
    ctx_rows = ctx_pairs[0].shape[2]
    members = [array.shape[0] for array in ctx_pairs]
    ctx_count = sum(members) * ctx_rows
    bf16, f32 = jnp.bfloat16, jnp.float32

    def body(q_ref, *refs):
        ctx_refs = refs[: len(members)]
        cb_ref, *out_refs, far_t, values = refs[len(members) :]
        sample, step = pl.program_id(0), pl.program_id(1)

        @pl.when(step == 0)
        def _():
            at = 0
            for ctx_ref, count in zip(ctx_refs, members):
                for member in range(count):
                    low = at + member * ctx_rows
                    values[low : low + ctx_rows] = ctx_ref[member, sample, :, cols:]
                size = count * ctx_rows
                block = jnp.concatenate(
                    [ctx_ref[member, sample, :, :cols] for member in range(count)], axis=0
                )
                far_t[:, at : at + size] = block.T
                at += size

        masks = head_masks(cols)
        context_bias = jnp.concatenate(
            [jnp.full((GRID_W, cols), cb_ref[h], f32) for h in range(len(masks))], axis=0
        )
        scores = [
            jnp.dot(
                spread_heads(q_ref[0, r * GRID_W : (r + 1) * GRID_W], masks),
                far_t[...],
                preferred_element_type=f32,
            )
            for r in range(per)
        ]
        for r in range(per):
            mixed, top, total = weighed(scores[r], values[...], masks)
            top = top + gather_heads(context_bias, masks)
            for out_ref, part in zip(out_refs, (mixed, top, total)):
                out_ref[0, r * GRID_W : (r + 1) * GRID_W] = part

    rows_spec = pl.BlockSpec((1, per * GRID_W, cols), lambda s, i: (s, i, 0))
    return pl.pallas_call(
        body,
        grid=(samples, rows_dev // per),
        in_specs=[
            rows_spec,
        ]
        + [RESIDENT] * len(members)
        + [pl.BlockSpec(memory_space=pltpu.SMEM)],
        out_specs=[rows_spec] * 3,
        out_shape=[jax.ShapeDtypeStruct((samples, tokens, cols), f32)] * 3,
        scratch_shapes=[
            pltpu.VMEM((cols, ctx_count), bf16),
            pltpu.VMEM((ctx_count, cols), bf16),
        ],
        compiler_params=pltpu.CompilerParams(vmem_limit_bytes=32 * 2**20),
        name="attend_far",
    )(query, *ctx_pairs, ctx_bias)


def finish(attended, w_out, latent, modulation, tiles):
    groups, _, _ = attended.shape
    samples, tokens, width = latent.shape
    block = modulation.shape[2] * tiles
    first = modulation.shape[1] - samples

    def body(att_ref, w_ref, latent_ref, tile_ref, out_ref):
        low = pl.program_id(0) * tiles
        everything = jnp.concatenate([att_ref[group] for group in range(groups)], axis=1)
        update = jnp.dot(everything, w_ref[...], preferred_element_type=jnp.float32)
        for s in range(samples):
            gate = jnp.concatenate(
                [tile_ref[low + t, first + s : first + s + 1, :] for t in range(tiles)], axis=1
            )
            part = update[s * tokens : (s + 1) * tokens]
            out_ref[s] = (latent_ref[s].astype(jnp.float32) + gate * part).astype(jnp.bfloat16)

    return pl.pallas_call(
        body,
        grid=(width // block,),
        in_specs=[
            whole(attended.shape),
            pl.BlockSpec((width, block), lambda i: (0, i)),
            pl.BlockSpec((samples, tokens, block), lambda i: (0, 0, i)),
            RESIDENT,
        ],
        out_specs=pl.BlockSpec((samples, tokens, block), lambda i: (0, 0, i)),
        out_shape=jax.ShapeDtypeStruct(latent.shape, latent.dtype),
        name="finish",
    )(attended, w_out, latent, modulation)


def shifted(size, side, stride, value):
    span = side * stride
    return [(i, i // span * span + (i + value * stride) % span) for i in range(size)]


def from_line(block, axis, side, stride):
    size = lax.axis_size(axis)
    return [block] + [
        lax.ppermute(block, axis, shifted(size, side, stride, value)) for value in range(1, side)
    ]


def computation(
    latent,
    context,
    cond,
    ctx_cond,
    w_shift,
    w_scale,
    w_gate,
    norm_gain,
    w_query,
    w_key,
    w_value,
    w_out,
    rel_bias,
    ctx_bias,
):
    samples, tokens_dev, width = latent.shape
    local_cols = w_shift.shape[1]
    sp_index = lax.axis_index("sp")
    sp_size, tp_size = lax.axis_size("sp"), lax.axis_size("tp")
    place = jnp.full((1,), sp_index, jnp.int32)
    gathered = lax.all_gather(latent, "tp", axis=1, tiled=True)
    parts = modulation_parts(place, cond, ctx_cond, (w_shift, w_scale, w_gate), sp_size)
    parts, w_out_own = lax.optimization_barrier((parts, w_out))
    w_out_all = lax.all_gather(w_out_own, "tp", axis=0, tiled=True)
    table = bias_table(rel_bias)
    summed = jnp.sum(lax.all_to_all(parts, "sp", 0, 0, tiled=True), axis=0)
    summed, table = lax.optimization_barrier((summed, table))
    modulation = resident(copy_for_each(summed, "tp"))
    w_query, w_key, w_value = resident(w_query), resident(w_key), resident(w_value)
    table = resident(table)

    gain = norm_gain[None, :]
    ctx_rows = context.shape[1]
    (ctx_pair,) = project(
        context.reshape(1, samples * ctx_rows, width),
        gain,
        modulation,
        (w_key, w_value),
        samples,
        samples * ctx_rows,
        None,
    )
    ctx_pair = ctx_pair.reshape(samples, ctx_rows, 2 * local_cols)
    ctx_pairs = from_line(ctx_pair, "sp", 4, 1)
    up = [(i, i + 1) for i in range(sp_size - 1)]
    down = [(j, i) for i, j in up]
    gathered = pltpu.with_memory_space_constraint(gathered, pltpu.HBM)
    ends = ((WIN_ROWS - REACH - 1) * GRID_W, REACH * GRID_W)
    w_triple = (w_key, w_value, w_query)
    outs = project(gathered, gain, modulation, w_triple, 0, 256, ends, 0)
    ctx_pairs, outs = lax.optimization_barrier((ctx_pairs, outs))
    ctx_line = jnp.stack(ctx_pairs)
    below = lax.ppermute(ctx_line, "sp", shifted(sp_size, 4, 4, 1))
    above = lax.ppermute(ctx_line, "sp", shifted(sp_size, 4, 4, 3))
    for s in range(1, samples):
        outs = project(gathered, gain, modulation, w_triple, 0, 256, ends, s, outs)
    pair, query, first, last = outs
    rows_all = pair.shape[1] // GRID_W * sp_size
    column = sp_index % 4
    rest = list(zip(shifted(sp_size, 4, 4, 1), shifted(sp_size, 4, 4, 3)))
    one_way = [down if i % 4 == 0 else up for i, (up, down) in enumerate(rest)]
    other_way = [up if i % 4 == 3 else down for i, (up, down) in enumerate(rest)]
    ctx_pairs = [
        ctx_line,
        below,
        above,
        lax.ppermute(jnp.where(column == 0, above[:2], below[:2]), "sp", one_way),
        lax.ppermute(jnp.where(column == 3, below[2:], above[2:]), "sp", other_way),
    ]
    before = resident(lax.ppermute(last, "sp", up))
    after = resident(lax.ppermute(first, "sp", down))
    ctx_pairs = [resident(array) for array in ctx_pairs]
    far = attend_far(query, ctx_pairs, ctx_bias, 4)
    attended = attend_near(place, query, before, pair, after, table, far, rows_all, 4)
    attended = attended.reshape(tp_size, samples * tokens_dev, local_cols)
    attended = lax.all_to_all(attended, "tp", 0, 0, tiled=True)
    return finish(attended, w_out_all, latent, modulation, 4)


def solution(mesh):
    return jax.shard_map(
        computation,
        mesh=mesh,
        in_specs=(
            P(None, ("sp", "tp"), None),
            P(None, "sp", None),
            P(),
            P(),
            P("sp", "tp"),
            P("sp", "tp"),
            P("sp", "tp"),
            P(),
            P(None, "tp"),
            P(None, "tp"),
            P(None, "tp"),
            P("tp", None),
            P("tp", None, None),
            P("tp"),
        ),
        out_specs=P(None, ("sp", "tp"), None),
        check_vma=False,
    )
```

```python
import jax
import jax.numpy as jnp
from jax import lax
from jax.experimental import pallas as pl
from jax.experimental.pallas import tpu as pltpu
from jax.sharding import PartitionSpec as P


HEAD_DIM = 64
GRID_W = 64
WIN_ROWS = 8
WIN_COLS = 16
EPSILON = 1e-06
MASKED = -1e30
REACH = WIN_ROWS // 2
BIAS_BLOCKS = 7
RESIDENT = pl.BlockSpec(memory_space=pltpu.VMEM)


def copy_for_each(shard, axis):
    length = lax.axis_size(axis)
    return lax.all_to_all(
        jnp.broadcast_to(shard[None], (length, *shard.shape)), axis, 0, 0, tiled=True
    )


def silu_rows(values):
    return jax.nn.silu(values.astype(jnp.float32)).astype(jnp.bfloat16)


def modulation_parts(place, cond, ctx_cond, weights, copies):
    samples = cond.shape[0]
    rows, cols = weights[0].shape

    def body(place_ref, cond_ref, ctx_ref, shift_ref, scale_ref, gate_ref, out_ref, wide):
        at = pl.multiple_of(place_ref[0] * rows, rows)
        ada = silu_rows(cond_ref[:, pl.ds(at, rows)])
        wide[...] = ctx_ref[...].astype(jnp.float32).reshape(1, ctx_ref.shape[0])
        ada_ctx = silu_rows(wide[:, pl.ds(at, rows)])
        both = jnp.concatenate([ada.astype(jnp.float32), ada_ctx.astype(jnp.float32)], axis=0)
        both = both.astype(jnp.bfloat16)
        result = jnp.concatenate(
            [
                jnp.dot(both, shift_ref[...], preferred_element_type=jnp.float32),
                jnp.dot(both, scale_ref[...], preferred_element_type=jnp.float32),
                jnp.dot(ada, gate_ref[...], preferred_element_type=jnp.float32),
            ],
            axis=0,
        )
        for copy in range(copies):
            out_ref[copy] = result

    return pl.pallas_call(
        body,
        in_specs=[pl.BlockSpec(memory_space=pltpu.SMEM)]
        + [pl.BlockSpec(memory_space=pltpu.VMEM)] * 5,
        out_shape=jax.ShapeDtypeStruct((copies, 3 * samples + 2, cols), jnp.float32),
        scratch_shapes=[pltpu.VMEM((1, ctx_cond.shape[0]), jnp.float32)],
        name="modulation_parts",
    )(place, cond, ctx_cond, *weights)


def resident(array):
    return pltpu.with_memory_space_constraint(array, pltpu.VMEM)


def whole(shape):
    return pl.BlockSpec(shape, lambda *_: (0,) * len(shape))


def modulation_row(tiles, row):
    return jnp.concatenate([tiles[tile, row : row + 1, :] for tile in range(tiles.shape[0])], axis=1)


def project(rows, gain, modulation, weights, row_of, block, ends, sample=None, buffers=()):
    samples, count, width = rows.shape
    every = modulation.shape[1] // 3 + 1
    chosen = range(samples) if sample is None else (sample,)
    begin = chosen[0]
    cols = weights[0].shape[1]
    first, last = ends if ends else (0, 0)
    steps = count // block

    def body(rows_ref, gain_ref, tiles_ref, *refs):
        weight_refs, out_refs = refs[: len(weights)], refs[len(weights) + len(buffers) : -2]
        factor_ref, shift_ref = refs[-2:]
        turn, step = pl.program_id(0), pl.program_id(1)

        for number in chosen:

            @pl.when((turn == number - begin) & (step == 0))
            def _(number=number):
                row = row_of + number
                factor_ref[...] = gain_ref[...] * (1.0 + modulation_row(tiles_ref, every + row))
                shift_ref[...] = modulation_row(tiles_ref, row)

        floats = rows_ref[0].astype(jnp.float32)
        inverse = lax.rsqrt(jnp.mean(floats * floats, axis=-1, keepdims=True) + EPSILON)
        hidden = (floats * inverse * factor_ref[...] + shift_ref[...]).astype(jnp.bfloat16)
        pair = [
            jnp.dot(hidden, ref[...], preferred_element_type=jnp.float32).astype(jnp.bfloat16)
            for ref in weight_refs[:2]
        ]
        if not ends:
            out_refs[0][0, :, :cols] = pair[0]
            out_refs[0][0, :, cols:] = pair[1]
            return
        out_refs[0][0, :, :cols] = pair[0]
        out_refs[0][0, :, cols:] = pair[1]
        query = jnp.dot(hidden, weight_refs[2][...], preferred_element_type=jnp.float32)
        query = query.astype(jnp.bfloat16).astype(jnp.float32) * HEAD_DIM**-0.5
        out_refs[1][0] = query.astype(jnp.bfloat16)
        for number in range(steps):
            low = number * block
            for out_ref, start, stop in (
                (out_refs[2], 0, first),
                (out_refs[3], count - last, count),
            ):
                lo, hi = max(low, start), min(low + block, stop)
                if lo < hi:

                    @pl.when(step == number)
                    def _(out_ref=out_ref, start=start, lo=lo, hi=hi, low=low):
                        for index in range(2):
                            out_ref[
                                0, lo - start : hi - start, index * cols : (index + 1) * cols
                            ] = pair[index][lo - low : hi - low]

    def blocks(size):
        return pl.BlockSpec((1, block, size), lambda s, i: (begin + s, i, 0))

    if ends:
        out_specs = [blocks(2 * cols), blocks(cols)]
        out_shape = [(samples, count, 2 * cols), (samples, count, cols)]
        for length in ends:
            out_specs += [pl.BlockSpec((1, length, 2 * cols), lambda s, i: (begin + s, 0, 0))]
            out_shape += [(samples, length, 2 * cols)]
    else:
        out_specs = [blocks(2 * cols)]
        out_shape = [(samples, count, 2 * cols)]
    return pl.pallas_call(
        body,
        grid=(len(chosen), steps),
        in_specs=[blocks(width), whole((1, width)), RESIDENT]
        + [RESIDENT] * len(weights)
        + [pl.BlockSpec(memory_space=pl.ANY)] * len(buffers),
        out_specs=out_specs,
        out_shape=[jax.ShapeDtypeStruct(shape, jnp.bfloat16) for shape in out_shape],
        scratch_shapes=[pltpu.VMEM((1, width), jnp.float32)] * 2,
        input_output_aliases={3 + len(weights) + i: i for i in range(len(buffers))},
        compiler_params=pltpu.CompilerParams(vmem_limit_bytes=24 * 2**20),
        name="project",
    )(rows, gain, modulation, *weights, *buffers)


def bias_table(rel_bias):
    heads, offsets, spread = rel_bias.shape
    slots = 2 * BIAS_BLOCKS + 2
    padded = jnp.pad(rel_bias, ((0, 0), (0, slots - offsets), (0, 128 - spread)))
    padded = padded.reshape(heads * slots, 128)

    def body(rel_ref, out_ref):
        query = lax.broadcasted_iota(jnp.int32, (GRID_W, 128), 0)
        lane = lax.broadcasted_iota(jnp.int32, (GRID_W, 128), 1)
        low = lane < GRID_W
        key = jnp.where(low, lane, lane - GRID_W)
        start = jnp.clip(query - WIN_COLS // 2, 0, GRID_W - WIN_COLS)
        inside = (key >= start) & (key < start + WIN_COLS)

        def diagonal(head, slot, move):
            row = jnp.broadcast_to(rel_ref[pl.ds(head * slots + slot, 1), :], (GRID_W, 128))
            return pltpu.roll(row, (128 - (WIN_COLS - 1) + move) % 128, 1, stride=1, stride_axis=0)

        for parity in range(2):
            for head in range(heads):
                for block in range(BIAS_BLOCKS):
                    slot = 2 * block + parity
                    both = jnp.where(
                        low, diagonal(head, slot, 0), diagonal(head, slot + 1, GRID_W)
                    )
                    out_ref[
                        parity, head * GRID_W : (head + 1) * GRID_W, block * 128 : (block + 1) * 128
                    ] = jnp.where(inside, both, MASKED)

    return pl.pallas_call(
        body,
        out_shape=jax.ShapeDtypeStruct((2, heads * GRID_W, BIAS_BLOCKS * 128), jnp.float32),
        compiler_params=pltpu.CompilerParams(vmem_limit_bytes=16 * 2**20),
        name="bias_table",
    )(padded)


def head_masks(cols):
    lane = lax.broadcasted_iota(jnp.int32, (GRID_W, cols), 1)
    return [(lane >= low) & (lane < low + HEAD_DIM) for low in range(0, cols, HEAD_DIM)]


def spread_heads(query, masks):
    return jnp.concatenate(
        [jnp.where(mask, query, jnp.zeros_like(query)) for mask in masks], axis=0
    )


def gather_heads(values, masks):
    result = jnp.where(masks[0], values[:GRID_W], 0.0)
    for h in range(1, len(masks)):
        result = jnp.where(masks[h], values[h * GRID_W : (h + 1) * GRID_W], result)
    return result


def weighed(scores, values, masks):
    top = jnp.max(scores, axis=-1, keepdims=True)
    exps = jnp.exp(scores - top)
    total = jnp.sum(exps, axis=-1, keepdims=True)
    mixed = jnp.dot(exps.astype(jnp.bfloat16), values, preferred_element_type=jnp.float32)
    return [gather_heads(array, masks) for array in (mixed, top, total)]


def attend_near(place, query, before, pair, after, table, far, rows_all, per):
    samples, tokens, cols = query.shape
    rows_dev = tokens // GRID_W
    near_keys = WIN_ROWS * GRID_W
    ahead, behind = before.shape[1], after.shape[1]
    padded = ahead + tokens + behind
    lanes = -(-padded // 128) * 128
    bf16, f32 = jnp.bfloat16, jnp.float32

    def body(place_ref, q_ref, before_ref, pair_ref, after_ref, table_ref, *refs):
        mixed_ref, top_ref, total_ref, out_ref, near_t, values = refs
        sample, step = pl.program_id(0), pl.program_id(1)

        @pl.when(step == 0)
        def _():
            values[0:ahead] = before_ref[sample, :, cols:]
            values[ahead : ahead + tokens] = pair_ref[0, :, cols:]
            values[ahead + tokens : padded] = after_ref[sample, :, cols:]
            fill = jnp.zeros((lanes - padded, cols), bf16)
            near_t[0, :, :ahead] = before_ref[sample, :, :cols].T
            near_t[0, :, ahead : ahead + tokens] = pair_ref[0, :, :cols].T
            near_t[0, :, ahead + tokens :] = jnp.concatenate(
                [after_ref[sample, :, :cols], fill], axis=0
            ).T
            near_t[1] = jnp.concatenate(
                [
                    before_ref[sample, GRID_W:, :cols],
                    pair_ref[0, :, :cols],
                    after_ref[sample, :, :cols],
                    fill,
                    jnp.zeros((GRID_W, cols), bf16),
                ],
                axis=0,
            ).T

        base = place_ref[0] * rows_dev
        masks = head_masks(cols)
        scores, starts = [], []
        for r in range(per):
            actual = base + step * per + r
            start = jnp.clip(actual - REACH, 0, rows_all - WIN_ROWS)
            local = start - base + REACH
            offset = start - actual + WIN_ROWS - 1
            spread = spread_heads(q_ref[0, r * GRID_W : (r + 1) * GRID_W], masks)
            column = pl.multiple_of((local // 2) * 128, 128)
            keys_t = near_t[local % 2, :, pl.ds(column, near_keys)]
            bias_at = pl.multiple_of((offset // 2) * 128, 128)
            scores.append(
                jnp.dot(spread, keys_t, preferred_element_type=f32)
                + table_ref[offset % 2, :, pl.ds(bias_at, near_keys)]
            )
            starts.append(pl.multiple_of(local * GRID_W, GRID_W))
        for r in range(per):
            parts = weighed(scores[r], values[pl.ds(starts[r], near_keys), :], masks)
            mixed, top, total = parts
            at = slice(r * GRID_W, (r + 1) * GRID_W)
            far_top = top_ref[0, at]
            highest = jnp.maximum(top, far_top)
            near_part = jnp.exp(top - highest)
            far_part = jnp.exp(far_top - highest)
            total = total * near_part + total_ref[0, at] * far_part
            mixed = mixed * near_part + mixed_ref[0, at] * far_part
            out_ref[r, 0] = (mixed / total).astype(bf16)

    def of_sample(array):
        return pl.BlockSpec((1, *array.shape[1:]), lambda s, i: (s, 0, 0))

    rows_spec = pl.BlockSpec((1, per * GRID_W, cols), lambda s, i: (s, i, 0))
    return pl.pallas_call(
        body,
        grid=(samples, rows_dev // per),
        in_specs=[
            pl.BlockSpec(memory_space=pltpu.SMEM),
            rows_spec,
            RESIDENT,
            of_sample(pair),
            RESIDENT,
            RESIDENT,
        ]
        + [rows_spec] * 3,
        out_specs=pl.BlockSpec((per, 1, GRID_W, cols), lambda s, i: (i, s, 0, 0)),
        out_shape=jax.ShapeDtypeStruct((rows_dev, samples, GRID_W, cols), bf16),
        scratch_shapes=[
            pltpu.VMEM((2, cols, lanes), bf16),
            pltpu.VMEM((padded, cols), bf16),
        ],
        compiler_params=pltpu.CompilerParams(vmem_limit_bytes=32 * 2**20),
        name="attend_near",
    )(place, query, before, pair, after, table, *far)


def attend_far(query, ctx_pairs, ctx_bias, per):
    samples, tokens, cols = query.shape
    rows_dev = tokens // GRID_W
    ctx_rows = ctx_pairs[0].shape[2]
    members = [array.shape[0] for array in ctx_pairs]
    ctx_count = sum(members) * ctx_rows
    bf16, f32 = jnp.bfloat16, jnp.float32

    def body(q_ref, *refs):
        ctx_refs = refs[: len(members)]
        cb_ref, *out_refs, far_t, values = refs[len(members) :]
        sample, step = pl.program_id(0), pl.program_id(1)

        @pl.when(step == 0)
        def _():
            at = 0
            for ctx_ref, count in zip(ctx_refs, members):
                for member in range(count):
                    low = at + member * ctx_rows
                    values[low : low + ctx_rows] = ctx_ref[member, sample, :, cols:]
                size = count * ctx_rows
                block = jnp.concatenate(
                    [ctx_ref[member, sample, :, :cols] for member in range(count)], axis=0
                )
                far_t[:, at : at + size] = block.T
                at += size

        masks = head_masks(cols)
        context_bias = jnp.concatenate(
            [jnp.full((GRID_W, cols), cb_ref[h], f32) for h in range(len(masks))], axis=0
        )
        scores = [
            jnp.dot(
                spread_heads(q_ref[0, r * GRID_W : (r + 1) * GRID_W], masks),
                far_t[...],
                preferred_element_type=f32,
            )
            for r in range(per)
        ]
        for r in range(per):
            mixed, top, total = weighed(scores[r], values[...], masks)
            top = top + gather_heads(context_bias, masks)
            for out_ref, part in zip(out_refs, (mixed, top, total)):
                out_ref[0, r * GRID_W : (r + 1) * GRID_W] = part

    rows_spec = pl.BlockSpec((1, per * GRID_W, cols), lambda s, i: (s, i, 0))
    return pl.pallas_call(
        body,
        grid=(samples, rows_dev // per),
        in_specs=[
            rows_spec,
        ]
        + [RESIDENT] * len(members)
        + [pl.BlockSpec(memory_space=pltpu.SMEM)],
        out_specs=[rows_spec] * 3,
        out_shape=[jax.ShapeDtypeStruct((samples, tokens, cols), f32)] * 3,
        scratch_shapes=[
            pltpu.VMEM((cols, ctx_count), bf16),
            pltpu.VMEM((ctx_count, cols), bf16),
        ],
        compiler_params=pltpu.CompilerParams(vmem_limit_bytes=32 * 2**20),
        name="attend_far",
    )(query, *ctx_pairs, ctx_bias)


def finish(attended, w_out, latent, modulation, tiles):
    groups, _, _ = attended.shape
    samples, tokens, width = latent.shape
    block = modulation.shape[2] * tiles
    first = modulation.shape[1] - samples

    def body(att_ref, w_ref, latent_ref, tile_ref, out_ref):
        low = pl.program_id(0) * tiles
        everything = jnp.concatenate([att_ref[group] for group in range(groups)], axis=1)
        update = jnp.dot(everything, w_ref[...], preferred_element_type=jnp.float32)
        for s in range(samples):
            gate = jnp.concatenate(
                [tile_ref[low + t, first + s : first + s + 1, :] for t in range(tiles)], axis=1
            )
            part = update[s * tokens : (s + 1) * tokens]
            out_ref[s] = (latent_ref[s].astype(jnp.float32) + gate * part).astype(jnp.bfloat16)

    return pl.pallas_call(
        body,
        grid=(width // block,),
        in_specs=[
            whole(attended.shape),
            pl.BlockSpec((width, block), lambda i: (0, i)),
            pl.BlockSpec((samples, tokens, block), lambda i: (0, 0, i)),
            RESIDENT,
        ],
        out_specs=pl.BlockSpec((samples, tokens, block), lambda i: (0, 0, i)),
        out_shape=jax.ShapeDtypeStruct(latent.shape, latent.dtype),
        name="finish",
    )(attended, w_out, latent, modulation)


def shifted(size, side, stride, value):
    span = side * stride
    return [(i, i // span * span + (i + value * stride) % span) for i in range(size)]


def from_line(block, axis, side, stride):
    size = lax.axis_size(axis)
    return [block] + [
        lax.ppermute(block, axis, shifted(size, side, stride, value)) for value in range(1, side)
    ]


def computation(
    latent,
    context,
    cond,
    ctx_cond,
    w_shift,
    w_scale,
    w_gate,
    norm_gain,
    w_query,
    w_key,
    w_value,
    w_out,
    rel_bias,
    ctx_bias,
):
    samples, tokens_dev, width = latent.shape
    local_cols = w_shift.shape[1]
    sp_index = lax.axis_index("sp")
    sp_size, tp_size = lax.axis_size("sp"), lax.axis_size("tp")
    place = jnp.full((1,), sp_index, jnp.int32)
    gathered = lax.all_gather(latent, "tp", axis=1, tiled=True)
    parts = modulation_parts(place, cond, ctx_cond, (w_shift, w_scale, w_gate), sp_size)
    parts, w_out_own = lax.optimization_barrier((parts, w_out))
    w_out_all = lax.all_gather(w_out_own, "tp", axis=0, tiled=True)
    table = bias_table(rel_bias)
    summed = jnp.sum(lax.all_to_all(parts, "sp", 0, 0, tiled=True), axis=0)
    summed, table = lax.optimization_barrier((summed, table))
    modulation = resident(copy_for_each(summed, "tp"))
    w_query, w_key, w_value = resident(w_query), resident(w_key), resident(w_value)
    table = resident(table)

    gain = norm_gain[None, :]
    ctx_rows = context.shape[1]
    (ctx_pair,) = project(
        context.reshape(1, samples * ctx_rows, width),
        gain,
        modulation,
        (w_key, w_value),
        samples,
        samples * ctx_rows,
        None,
    )
    ctx_pair = ctx_pair.reshape(samples, ctx_rows, 2 * local_cols)
    ctx_pairs = from_line(ctx_pair, "sp", 4, 1)
    up = [(i, i + 1) for i in range(sp_size - 1)]
    down = [(j, i) for i, j in up]
    gathered = pltpu.with_memory_space_constraint(gathered, pltpu.HBM)
    ends = ((WIN_ROWS - REACH - 1) * GRID_W, REACH * GRID_W)
    w_triple = (w_key, w_value, w_query)
    outs = project(gathered, gain, modulation, w_triple, 0, 256, ends, 0)
    ctx_pairs, outs = lax.optimization_barrier((ctx_pairs, outs))
    ctx_line = jnp.stack(ctx_pairs)
    below = lax.ppermute(ctx_line, "sp", shifted(sp_size, 4, 4, 1))
    above = lax.ppermute(ctx_line, "sp", shifted(sp_size, 4, 4, 3))
    for s in range(1, samples):
        outs = project(gathered, gain, modulation, w_triple, 0, 256, ends, s, outs)
    pair, query, first, last = outs
    rows_all = pair.shape[1] // GRID_W * sp_size
    ctx_pairs = [
        ctx_line,
        below,
        above,
        lax.ppermute(below[:2], "sp", shifted(sp_size, 4, 4, 1)),
        lax.ppermute(above[2:], "sp", shifted(sp_size, 4, 4, 3)),
    ]
    before = resident(lax.ppermute(last, "sp", up))
    after = resident(lax.ppermute(first, "sp", down))
    ctx_pairs = [resident(array) for array in ctx_pairs]
    far = attend_far(query, ctx_pairs, ctx_bias, 4)
    attended = attend_near(place, query, before, pair, after, table, far, rows_all, 4)
    attended = attended.reshape(tp_size, samples * tokens_dev, local_cols)
    attended = lax.all_to_all(attended, "tp", 0, 0, tiled=True)
    return finish(attended, w_out_all, latent, modulation, 4)


def solution(mesh):
    return jax.shard_map(
        computation,
        mesh=mesh,
        in_specs=(
            P(None, ("sp", "tp"), None),
            P(None, "sp", None),
            P(),
            P(),
            P("sp", "tp"),
            P("sp", "tp"),
            P("sp", "tp"),
            P(),
            P(None, "tp"),
            P(None, "tp"),
            P(None, "tp"),
            P("tp", None),
            P("tp", None, None),
            P("tp"),
        ),
        out_specs=P(None, ("sp", "tp"), None),
        check_vma=False,
    )
```

```python
import jax
import jax.numpy as jnp
from jax import lax
from jax.experimental import pallas as pl
from jax.experimental.pallas import tpu as pltpu
from jax.sharding import PartitionSpec as P


HEAD_DIM = 64
GRID_W = 64
WIN_ROWS = 8
WIN_COLS = 16
EPSILON = 1e-06
MASKED = -1e30
REACH = WIN_ROWS // 2
BIAS_BLOCKS = 7
RESIDENT = pl.BlockSpec(memory_space=pltpu.VMEM)


def copy_for_each(shard, axis):
    length = lax.axis_size(axis)
    return lax.all_to_all(
        jnp.broadcast_to(shard[None], (length, *shard.shape)), axis, 0, 0, tiled=True
    )


def silu_rows(values):
    return jax.nn.silu(values.astype(jnp.float32)).astype(jnp.bfloat16)


def modulation_parts(place, cond, ctx_cond, weights, copies):
    samples = cond.shape[0]
    rows, cols = weights[0].shape

    def body(place_ref, cond_ref, ctx_ref, shift_ref, scale_ref, gate_ref, out_ref, wide):
        at = pl.multiple_of(place_ref[0] * rows, rows)
        ada = silu_rows(cond_ref[:, pl.ds(at, rows)])
        wide[...] = ctx_ref[...].astype(jnp.float32).reshape(1, ctx_ref.shape[0])
        ada_ctx = silu_rows(wide[:, pl.ds(at, rows)])
        both = jnp.concatenate([ada.astype(jnp.float32), ada_ctx.astype(jnp.float32)], axis=0)
        both = both.astype(jnp.bfloat16)
        result = jnp.concatenate(
            [
                jnp.dot(both, shift_ref[...], preferred_element_type=jnp.float32),
                jnp.dot(both, scale_ref[...], preferred_element_type=jnp.float32),
                jnp.dot(ada, gate_ref[...], preferred_element_type=jnp.float32),
            ],
            axis=0,
        )
        for copy in range(copies):
            out_ref[copy] = result

    return pl.pallas_call(
        body,
        in_specs=[pl.BlockSpec(memory_space=pltpu.SMEM)]
        + [pl.BlockSpec(memory_space=pltpu.VMEM)] * 5,
        out_shape=jax.ShapeDtypeStruct((copies, 3 * samples + 2, cols), jnp.float32),
        scratch_shapes=[pltpu.VMEM((1, ctx_cond.shape[0]), jnp.float32)],
        name="modulation_parts",
    )(place, cond, ctx_cond, *weights)


def resident(array):
    return pltpu.with_memory_space_constraint(array, pltpu.VMEM)


def whole(shape):
    return pl.BlockSpec(shape, lambda *_: (0,) * len(shape))


def modulation_row(tiles, row):
    return jnp.concatenate([tiles[tile, row : row + 1, :] for tile in range(tiles.shape[0])], axis=1)


def project(rows, gain, modulation, weights, row_of, block, ends, sample=None, buffers=()):
    samples, count, width = rows.shape
    every = modulation.shape[1] // 3 + 1
    chosen = range(samples) if sample is None else (sample,)
    begin = chosen[0]
    cols = weights[0].shape[1]
    first, last = ends if ends else (0, 0)
    steps = count // block

    def body(rows_ref, gain_ref, tiles_ref, *refs):
        weight_refs, out_refs = refs[: len(weights)], refs[len(weights) + len(buffers) : -2]
        factor_ref, shift_ref = refs[-2:]
        turn, step = pl.program_id(0), pl.program_id(1)

        for number in chosen:

            @pl.when((turn == number - begin) & (step == 0))
            def _(number=number):
                row = row_of + number
                factor_ref[...] = gain_ref[...] * (1.0 + modulation_row(tiles_ref, every + row))
                shift_ref[...] = modulation_row(tiles_ref, row)

        floats = rows_ref[0].astype(jnp.float32)
        inverse = lax.rsqrt(jnp.mean(floats * floats, axis=-1, keepdims=True) + EPSILON)
        hidden = (floats * inverse * factor_ref[...] + shift_ref[...]).astype(jnp.bfloat16)
        pair = [
            jnp.dot(hidden, ref[...], preferred_element_type=jnp.float32).astype(jnp.bfloat16)
            for ref in weight_refs[:2]
        ]
        if not ends:
            out_refs[0][0, :, :cols] = pair[0]
            out_refs[0][0, :, cols:] = pair[1]
            return
        out_refs[0][0, :, :cols] = pair[0]
        out_refs[0][0, :, cols:] = pair[1]
        query = jnp.dot(hidden, weight_refs[2][...], preferred_element_type=jnp.float32)
        query = query.astype(jnp.bfloat16).astype(jnp.float32) * HEAD_DIM**-0.5
        out_refs[1][0] = query.astype(jnp.bfloat16)
        for number in range(steps):
            low = number * block
            for out_ref, start, stop in (
                (out_refs[2], 0, first),
                (out_refs[3], count - last, count),
            ):
                lo, hi = max(low, start), min(low + block, stop)
                if lo < hi:

                    @pl.when(step == number)
                    def _(out_ref=out_ref, start=start, lo=lo, hi=hi, low=low):
                        for index in range(2):
                            out_ref[
                                0, lo - start : hi - start, index * cols : (index + 1) * cols
                            ] = pair[index][lo - low : hi - low]

    def blocks(size):
        return pl.BlockSpec((1, block, size), lambda s, i: (begin + s, i, 0))

    if ends:
        out_specs = [blocks(2 * cols), blocks(cols)]
        out_shape = [(samples, count, 2 * cols), (samples, count, cols)]
        for length in ends:
            out_specs += [pl.BlockSpec((1, length, 2 * cols), lambda s, i: (begin + s, 0, 0))]
            out_shape += [(samples, length, 2 * cols)]
    else:
        out_specs = [blocks(2 * cols)]
        out_shape = [(samples, count, 2 * cols)]
    return pl.pallas_call(
        body,
        grid=(len(chosen), steps),
        in_specs=[blocks(width), whole((1, width)), RESIDENT]
        + [RESIDENT] * len(weights)
        + [pl.BlockSpec(memory_space=pl.ANY)] * len(buffers),
        out_specs=out_specs,
        out_shape=[jax.ShapeDtypeStruct(shape, jnp.bfloat16) for shape in out_shape],
        scratch_shapes=[pltpu.VMEM((1, width), jnp.float32)] * 2,
        input_output_aliases={3 + len(weights) + i: i for i in range(len(buffers))},
        compiler_params=pltpu.CompilerParams(vmem_limit_bytes=24 * 2**20),
        name="project",
    )(rows, gain, modulation, *weights, *buffers)


def bias_table(rel_bias):
    heads, offsets, spread = rel_bias.shape
    slots = 2 * BIAS_BLOCKS + 2
    padded = jnp.pad(rel_bias, ((0, 0), (0, slots - offsets), (0, 128 - spread)))
    padded = padded.reshape(heads * slots, 128)

    def body(rel_ref, out_ref):
        query = lax.broadcasted_iota(jnp.int32, (GRID_W, 128), 0)
        lane = lax.broadcasted_iota(jnp.int32, (GRID_W, 128), 1)
        low = lane < GRID_W
        key = jnp.where(low, lane, lane - GRID_W)
        start = jnp.clip(query - WIN_COLS // 2, 0, GRID_W - WIN_COLS)
        inside = (key >= start) & (key < start + WIN_COLS)

        def diagonal(head, slot, move):
            row = jnp.broadcast_to(rel_ref[pl.ds(head * slots + slot, 1), :], (GRID_W, 128))
            return pltpu.roll(row, (128 - (WIN_COLS - 1) + move) % 128, 1, stride=1, stride_axis=0)

        for parity in range(2):
            for head in range(heads):
                for block in range(BIAS_BLOCKS):
                    slot = 2 * block + parity
                    both = jnp.where(
                        low, diagonal(head, slot, 0), diagonal(head, slot + 1, GRID_W)
                    )
                    out_ref[
                        parity, head * GRID_W : (head + 1) * GRID_W, block * 128 : (block + 1) * 128
                    ] = jnp.where(inside, both, MASKED)

    return pl.pallas_call(
        body,
        out_shape=jax.ShapeDtypeStruct((2, heads * GRID_W, BIAS_BLOCKS * 128), jnp.float32),
        compiler_params=pltpu.CompilerParams(vmem_limit_bytes=16 * 2**20),
        name="bias_table",
    )(padded)


def head_masks(cols):
    lane = lax.broadcasted_iota(jnp.int32, (GRID_W, cols), 1)
    return [(lane >= low) & (lane < low + HEAD_DIM) for low in range(0, cols, HEAD_DIM)]


def spread_heads(query, masks):
    return jnp.concatenate(
        [jnp.where(mask, query, jnp.zeros_like(query)) for mask in masks], axis=0
    )


def gather_heads(values, masks):
    result = jnp.where(masks[0], values[:GRID_W], 0.0)
    for h in range(1, len(masks)):
        result = jnp.where(masks[h], values[h * GRID_W : (h + 1) * GRID_W], result)
    return result


def weighed(scores, values, masks):
    top = jnp.max(scores, axis=-1, keepdims=True)
    exps = jnp.exp(scores - top)
    total = jnp.sum(exps, axis=-1, keepdims=True)
    mixed = jnp.dot(exps.astype(jnp.bfloat16), values, preferred_element_type=jnp.float32)
    return [gather_heads(array, masks) for array in (mixed, top, total)]


def attend_near(place, query, before, pair, after, table, far, rows_all, per):
    samples, tokens, cols = query.shape
    rows_dev = tokens // GRID_W
    near_keys = WIN_ROWS * GRID_W
    ahead, behind = before.shape[1], after.shape[1]
    padded = ahead + tokens + behind
    lanes = -(-padded // 128) * 128
    bf16, f32 = jnp.bfloat16, jnp.float32

    def body(place_ref, q_ref, before_ref, pair_ref, after_ref, table_ref, *refs):
        mixed_ref, top_ref, total_ref, out_ref, near_t, values = refs
        sample, step = pl.program_id(0), pl.program_id(1)

        @pl.when(step == 0)
        def _():
            values[0:ahead] = before_ref[sample, :, cols:]
            values[ahead : ahead + tokens] = pair_ref[0, :, cols:]
            values[ahead + tokens : padded] = after_ref[sample, :, cols:]
            fill = jnp.zeros((lanes - padded, cols), bf16)
            near_t[0, :, :ahead] = before_ref[sample, :, :cols].T
            near_t[0, :, ahead : ahead + tokens] = pair_ref[0, :, :cols].T
            near_t[0, :, ahead + tokens :] = jnp.concatenate(
                [after_ref[sample, :, :cols], fill], axis=0
            ).T
            near_t[1] = jnp.concatenate(
                [
                    before_ref[sample, GRID_W:, :cols],
                    pair_ref[0, :, :cols],
                    after_ref[sample, :, :cols],
                    fill,
                    jnp.zeros((GRID_W, cols), bf16),
                ],
                axis=0,
            ).T

        base = place_ref[0] * rows_dev
        masks = head_masks(cols)
        scores, starts = [], []
        for r in range(per):
            actual = base + step * per + r
            start = jnp.clip(actual - REACH, 0, rows_all - WIN_ROWS)
            local = start - base + REACH
            offset = start - actual + WIN_ROWS - 1
            spread = spread_heads(q_ref[0, r * GRID_W : (r + 1) * GRID_W], masks)
            column = pl.multiple_of((local // 2) * 128, 128)
            keys_t = near_t[local % 2, :, pl.ds(column, near_keys)]
            bias_at = pl.multiple_of((offset // 2) * 128, 128)
            scores.append(
                jnp.dot(spread, keys_t, preferred_element_type=f32)
                + table_ref[offset % 2, :, pl.ds(bias_at, near_keys)]
            )
            starts.append(pl.multiple_of(local * GRID_W, GRID_W))
        for r in range(per):
            parts = weighed(scores[r], values[pl.ds(starts[r], near_keys), :], masks)
            mixed, top, total = parts
            at = slice(r * GRID_W, (r + 1) * GRID_W)
            far_top = top_ref[0, at]
            highest = jnp.maximum(top, far_top)
            near_part = jnp.exp(top - highest)
            far_part = jnp.exp(far_top - highest)
            total = total * near_part + total_ref[0, at] * far_part
            mixed = mixed * near_part + mixed_ref[0, at] * far_part
            out_ref[r, 0] = (mixed / total).astype(bf16)

    def of_sample(array):
        return pl.BlockSpec((1, *array.shape[1:]), lambda s, i: (s, 0, 0))

    rows_spec = pl.BlockSpec((1, per * GRID_W, cols), lambda s, i: (s, i, 0))
    return pl.pallas_call(
        body,
        grid=(samples, rows_dev // per),
        in_specs=[
            pl.BlockSpec(memory_space=pltpu.SMEM),
            rows_spec,
            RESIDENT,
            of_sample(pair),
            RESIDENT,
            RESIDENT,
        ]
        + [rows_spec] * 3,
        out_specs=pl.BlockSpec((per, 1, GRID_W, cols), lambda s, i: (i, s, 0, 0)),
        out_shape=jax.ShapeDtypeStruct((rows_dev, samples, GRID_W, cols), bf16),
        scratch_shapes=[
            pltpu.VMEM((2, cols, lanes), bf16),
            pltpu.VMEM((padded, cols), bf16),
        ],
        compiler_params=pltpu.CompilerParams(vmem_limit_bytes=32 * 2**20),
        name="attend_near",
    )(place, query, before, pair, after, table, *far)


def attend_far(query, ctx_pairs, ctx_bias, per):
    samples, tokens, cols = query.shape
    rows_dev = tokens // GRID_W
    ctx_rows = ctx_pairs[0].shape[2]
    members = [array.shape[0] for array in ctx_pairs]
    ctx_count = sum(members) * ctx_rows
    bf16, f32 = jnp.bfloat16, jnp.float32

    def body(q_ref, *refs):
        ctx_refs = refs[: len(members)]
        cb_ref, *out_refs, far_t, values = refs[len(members) :]
        sample, step = pl.program_id(0), pl.program_id(1)

        @pl.when(step == 0)
        def _():
            at = 0
            for ctx_ref, count in zip(ctx_refs, members):
                for member in range(count):
                    low = at + member * ctx_rows
                    values[low : low + ctx_rows] = ctx_ref[member, sample, :, cols:]
                size = count * ctx_rows
                block = jnp.concatenate(
                    [ctx_ref[member, sample, :, :cols] for member in range(count)], axis=0
                )
                far_t[:, at : at + size] = block.T
                at += size

        masks = head_masks(cols)
        context_bias = jnp.concatenate(
            [jnp.full((GRID_W, cols), cb_ref[h], f32) for h in range(len(masks))], axis=0
        )
        scores = [
            jnp.dot(
                spread_heads(q_ref[0, r * GRID_W : (r + 1) * GRID_W], masks),
                far_t[...],
                preferred_element_type=f32,
            )
            for r in range(per)
        ]
        for r in range(per):
            mixed, top, total = weighed(scores[r], values[...], masks)
            top = top + gather_heads(context_bias, masks)
            for out_ref, part in zip(out_refs, (mixed, top, total)):
                out_ref[0, r * GRID_W : (r + 1) * GRID_W] = part

    rows_spec = pl.BlockSpec((1, per * GRID_W, cols), lambda s, i: (s, i, 0))
    return pl.pallas_call(
        body,
        grid=(samples, rows_dev // per),
        in_specs=[
            rows_spec,
        ]
        + [RESIDENT] * len(members)
        + [pl.BlockSpec(memory_space=pltpu.SMEM)],
        out_specs=[rows_spec] * 3,
        out_shape=[jax.ShapeDtypeStruct((samples, tokens, cols), f32)] * 3,
        scratch_shapes=[
            pltpu.VMEM((cols, ctx_count), bf16),
            pltpu.VMEM((ctx_count, cols), bf16),
        ],
        compiler_params=pltpu.CompilerParams(vmem_limit_bytes=32 * 2**20),
        name="attend_far",
    )(query, *ctx_pairs, ctx_bias)


def finish(attended, w_out, latent, modulation, tiles):
    groups, _, _ = attended.shape
    samples, tokens, width = latent.shape
    block = modulation.shape[2] * tiles
    first = modulation.shape[1] - samples

    def body(att_ref, w_ref, latent_ref, tile_ref, out_ref):
        everything = jnp.concatenate([att_ref[group] for group in range(groups)], axis=1)
        update = jnp.dot(everything, w_ref[...], preferred_element_type=jnp.float32)
        for s in range(samples):
            gate = jnp.concatenate(
                [tile_ref[t, first + s : first + s + 1, :] for t in range(tiles)], axis=1
            )
            part = update[s * tokens : (s + 1) * tokens]
            out_ref[s] = (latent_ref[s].astype(jnp.float32) + gate * part).astype(jnp.bfloat16)

    return pl.pallas_call(
        body,
        grid=(width // block,),
        in_specs=[
            whole(attended.shape),
            pl.BlockSpec((width, block), lambda i: (0, i)),
            pl.BlockSpec((samples, tokens, block), lambda i: (0, 0, i)),
            pl.BlockSpec((tiles, *modulation.shape[1:]), lambda i: (i, 0, 0)),
        ],
        out_specs=pl.BlockSpec((samples, tokens, block), lambda i: (0, 0, i)),
        out_shape=jax.ShapeDtypeStruct(latent.shape, latent.dtype),
        name="finish",
    )(attended, w_out, latent, modulation)


def shifted(size, side, stride, value):
    span = side * stride
    return [(i, i // span * span + (i + value * stride) % span) for i in range(size)]


def from_line(block, axis, side, stride):
    size = lax.axis_size(axis)
    return [block] + [
        lax.ppermute(block, axis, shifted(size, side, stride, value)) for value in range(1, side)
    ]


def computation(
    latent,
    context,
    cond,
    ctx_cond,
    w_shift,
    w_scale,
    w_gate,
    norm_gain,
    w_query,
    w_key,
    w_value,
    w_out,
    rel_bias,
    ctx_bias,
):
    samples, tokens_dev, width = latent.shape
    local_cols = w_shift.shape[1]
    sp_index = lax.axis_index("sp")
    sp_size, tp_size = lax.axis_size("sp"), lax.axis_size("tp")
    place = jnp.full((1,), sp_index, jnp.int32)
    gathered = lax.all_gather(latent, "tp", axis=1, tiled=True)
    parts = modulation_parts(place, cond, ctx_cond, (w_shift, w_scale, w_gate), sp_size)
    parts, w_out_own = lax.optimization_barrier((parts, w_out))
    w_out_all = lax.all_gather(w_out_own, "tp", axis=0, tiled=True)
    table = bias_table(rel_bias)
    summed = jnp.sum(lax.all_to_all(parts, "sp", 0, 0, tiled=True), axis=0)
    summed, table = lax.optimization_barrier((summed, table))
    modulation = resident(copy_for_each(summed, "tp"))
    w_query, w_key, w_value = resident(w_query), resident(w_key), resident(w_value)
    table = resident(table)

    gain = norm_gain[None, :]
    ctx_rows = context.shape[1]
    (ctx_pair,) = project(
        pltpu.with_memory_space_constraint(
            context.reshape(1, samples * ctx_rows, width), pltpu.HBM
        ),
        gain,
        modulation,
        (w_key, w_value),
        samples,
        samples * ctx_rows,
        None,
    )
    ctx_pair = ctx_pair.reshape(samples, ctx_rows, 2 * local_cols)
    ctx_pairs = from_line(ctx_pair, "sp", 4, 1)
    up = [(i, i + 1) for i in range(sp_size - 1)]
    down = [(j, i) for i, j in up]
    gathered = pltpu.with_memory_space_constraint(gathered, pltpu.HBM)
    ends = ((WIN_ROWS - REACH - 1) * GRID_W, REACH * GRID_W)
    w_triple = (w_key, w_value, w_query)
    outs = project(gathered, gain, modulation, w_triple, 0, 256, ends, 0)
    ctx_pairs, outs = lax.optimization_barrier((ctx_pairs, outs))
    ctx_line = jnp.stack(ctx_pairs)
    below = lax.ppermute(ctx_line, "sp", shifted(sp_size, 4, 4, 1))
    above = lax.ppermute(ctx_line, "sp", shifted(sp_size, 4, 4, 3))
    for s in range(1, samples):
        outs = project(gathered, gain, modulation, w_triple, 0, 256, ends, s, outs)
    pair, query, first, last = outs
    rows_all = pair.shape[1] // GRID_W * sp_size
    ctx_pairs = [
        ctx_line,
        below,
        above,
        lax.ppermute(below[:2], "sp", shifted(sp_size, 4, 4, 1)),
        lax.ppermute(above[2:], "sp", shifted(sp_size, 4, 4, 3)),
    ]
    before = resident(lax.ppermute(last, "sp", up))
    after = resident(lax.ppermute(first, "sp", down))
    ctx_pairs = [resident(array) for array in ctx_pairs]
    far = attend_far(query, ctx_pairs, ctx_bias, 8)
    attended = attend_near(place, query, before, pair, after, table, far, rows_all, 4)
    attended = attended.reshape(tp_size, samples * tokens_dev, local_cols)
    attended = lax.all_to_all(attended, "tp", 0, 0, tiled=True)
    return finish(attended, w_out_all, latent, modulation, 4)


def solution(mesh):
    return jax.shard_map(
        computation,
        mesh=mesh,
        in_specs=(
            P(None, ("sp", "tp"), None),
            P(None, "sp", None),
            P(),
            P(),
            P("sp", "tp"),
            P("sp", "tp"),
            P("sp", "tp"),
            P(),
            P(None, "tp"),
            P(None, "tp"),
            P(None, "tp"),
            P("tp", None),
            P("tp", None, None),
            P("tp"),
        ),
        out_specs=P(None, ("sp", "tp"), None),
        check_vma=False,
    )
```

```python
import jax
import jax.numpy as jnp
from jax import lax
from jax.experimental import pallas as pl
from jax.experimental.pallas import tpu as pltpu
from jax.sharding import PartitionSpec as P


HEAD_DIM = 64
GRID_W = 64
WIN_ROWS = 8
WIN_COLS = 16
EPSILON = 1e-06
MASKED = -1e30
REACH = WIN_ROWS // 2
BIAS_BLOCKS = 7
RESIDENT = pl.BlockSpec(memory_space=pltpu.VMEM)


def copy_for_each(shard, axis):
    length = lax.axis_size(axis)
    return lax.all_to_all(
        jnp.broadcast_to(shard[None], (length, *shard.shape)), axis, 0, 0, tiled=True
    )


def silu_rows(values):
    return jax.nn.silu(values.astype(jnp.float32)).astype(jnp.bfloat16)


def modulation_parts(place, cond, ctx_cond, weights, copies):
    samples = cond.shape[0]
    rows, cols = weights[0].shape

    def body(place_ref, cond_ref, ctx_ref, shift_ref, scale_ref, gate_ref, out_ref, wide):
        at = pl.multiple_of(place_ref[0] * rows, rows)
        ada = silu_rows(cond_ref[:, pl.ds(at, rows)])
        wide[...] = ctx_ref[...].astype(jnp.float32).reshape(1, ctx_ref.shape[0])
        ada_ctx = silu_rows(wide[:, pl.ds(at, rows)])
        both = jnp.concatenate([ada.astype(jnp.float32), ada_ctx.astype(jnp.float32)], axis=0)
        both = both.astype(jnp.bfloat16)
        result = jnp.concatenate(
            [
                jnp.dot(both, shift_ref[...], preferred_element_type=jnp.float32),
                jnp.dot(both, scale_ref[...], preferred_element_type=jnp.float32),
                jnp.dot(ada, gate_ref[...], preferred_element_type=jnp.float32),
            ],
            axis=0,
        )
        for copy in range(copies):
            out_ref[copy] = result

    return pl.pallas_call(
        body,
        in_specs=[pl.BlockSpec(memory_space=pltpu.SMEM)]
        + [pl.BlockSpec(memory_space=pltpu.VMEM)] * 5,
        out_shape=jax.ShapeDtypeStruct((copies, 3 * samples + 2, cols), jnp.float32),
        scratch_shapes=[pltpu.VMEM((1, ctx_cond.shape[0]), jnp.float32)],
        name="modulation_parts",
    )(place, cond, ctx_cond, *weights)


def resident(array):
    return pltpu.with_memory_space_constraint(array, pltpu.VMEM)


def whole(shape):
    return pl.BlockSpec(shape, lambda *_: (0,) * len(shape))


def modulation_row(tiles, row):
    return jnp.concatenate([tiles[tile, row : row + 1, :] for tile in range(tiles.shape[0])], axis=1)


def project(rows, gain, modulation, weights, row_of, block, ends, sample=None, buffers=()):
    samples, count, width = rows.shape
    every = modulation.shape[1] // 3 + 1
    chosen = range(samples) if sample is None else (sample,)
    begin = chosen[0]
    cols = weights[0].shape[1]
    first, last = ends if ends else (0, 0)
    steps = count // block

    def body(rows_ref, gain_ref, tiles_ref, *refs):
        weight_refs, out_refs = refs[: len(weights)], refs[len(weights) + len(buffers) : -2]
        factor_ref, shift_ref = refs[-2:]
        turn, step = pl.program_id(0), pl.program_id(1)

        for number in chosen:

            @pl.when((turn == number - begin) & (step == 0))
            def _(number=number):
                row = row_of + number
                factor_ref[...] = gain_ref[...] * (1.0 + modulation_row(tiles_ref, every + row))
                shift_ref[...] = modulation_row(tiles_ref, row)

        floats = rows_ref[0].astype(jnp.float32)
        inverse = lax.rsqrt(jnp.mean(floats * floats, axis=-1, keepdims=True) + EPSILON)
        hidden = (floats * inverse * factor_ref[...] + shift_ref[...]).astype(jnp.bfloat16)
        pair = [
            jnp.dot(hidden, ref[...], preferred_element_type=jnp.float32).astype(jnp.bfloat16)
            for ref in weight_refs[:2]
        ]
        if not ends:
            out_refs[0][0, :, :cols] = pair[0]
            out_refs[0][0, :, cols:] = pair[1]
            return
        out_refs[0][0, :, :cols] = pair[0]
        out_refs[0][0, :, cols:] = pair[1]
        query = jnp.dot(hidden, weight_refs[2][...], preferred_element_type=jnp.float32)
        query = query.astype(jnp.bfloat16).astype(jnp.float32) * HEAD_DIM**-0.5
        out_refs[1][0] = query.astype(jnp.bfloat16)
        for number in range(steps):
            low = number * block
            for out_ref, start, stop in (
                (out_refs[2], 0, first),
                (out_refs[3], count - last, count),
            ):
                lo, hi = max(low, start), min(low + block, stop)
                if lo < hi:

                    @pl.when(step == number)
                    def _(out_ref=out_ref, start=start, lo=lo, hi=hi, low=low):
                        for index in range(2):
                            out_ref[
                                0, lo - start : hi - start, index * cols : (index + 1) * cols
                            ] = pair[index][lo - low : hi - low]

    def blocks(size):
        return pl.BlockSpec((1, block, size), lambda s, i: (begin + s, i, 0))

    if ends:
        out_specs = [blocks(2 * cols), blocks(cols)]
        out_shape = [(samples, count, 2 * cols), (samples, count, cols)]
        for length in ends:
            out_specs += [pl.BlockSpec((1, length, 2 * cols), lambda s, i: (begin + s, 0, 0))]
            out_shape += [(samples, length, 2 * cols)]
    else:
        out_specs = [blocks(2 * cols)]
        out_shape = [(samples, count, 2 * cols)]
    return pl.pallas_call(
        body,
        grid=(len(chosen), steps),
        in_specs=[blocks(width), whole((1, width)), RESIDENT]
        + [RESIDENT] * len(weights)
        + [pl.BlockSpec(memory_space=pl.ANY)] * len(buffers),
        out_specs=out_specs,
        out_shape=[jax.ShapeDtypeStruct(shape, jnp.bfloat16) for shape in out_shape],
        scratch_shapes=[pltpu.VMEM((1, width), jnp.float32)] * 2,
        input_output_aliases={3 + len(weights) + i: i for i in range(len(buffers))},
        compiler_params=pltpu.CompilerParams(vmem_limit_bytes=24 * 2**20),
        name="project",
    )(rows, gain, modulation, *weights, *buffers)


def bias_table(rel_bias):
    heads, offsets, spread = rel_bias.shape
    slots = 2 * BIAS_BLOCKS + 2
    padded = jnp.pad(rel_bias, ((0, 0), (0, slots - offsets), (0, 128 - spread)))
    padded = padded.reshape(heads * slots, 128)

    def body(rel_ref, out_ref):
        query = lax.broadcasted_iota(jnp.int32, (GRID_W, 128), 0)
        lane = lax.broadcasted_iota(jnp.int32, (GRID_W, 128), 1)
        low = lane < GRID_W
        key = jnp.where(low, lane, lane - GRID_W)
        start = jnp.clip(query - WIN_COLS // 2, 0, GRID_W - WIN_COLS)
        inside = (key >= start) & (key < start + WIN_COLS)

        def diagonal(head, slot, move):
            row = jnp.broadcast_to(rel_ref[pl.ds(head * slots + slot, 1), :], (GRID_W, 128))
            return pltpu.roll(row, (128 - (WIN_COLS - 1) + move) % 128, 1, stride=1, stride_axis=0)

        for parity in range(2):
            for head in range(heads):
                for block in range(BIAS_BLOCKS):
                    slot = 2 * block + parity
                    both = jnp.where(
                        low, diagonal(head, slot, 0), diagonal(head, slot + 1, GRID_W)
                    )
                    out_ref[
                        parity, head * GRID_W : (head + 1) * GRID_W, block * 128 : (block + 1) * 128
                    ] = jnp.where(inside, both, MASKED)

    return pl.pallas_call(
        body,
        out_shape=jax.ShapeDtypeStruct((2, heads * GRID_W, BIAS_BLOCKS * 128), jnp.float32),
        compiler_params=pltpu.CompilerParams(vmem_limit_bytes=16 * 2**20),
        name="bias_table",
    )(padded)


def head_masks(cols):
    lane = lax.broadcasted_iota(jnp.int32, (GRID_W, cols), 1)
    return [(lane >= low) & (lane < low + HEAD_DIM) for low in range(0, cols, HEAD_DIM)]


def spread_heads(query, masks):
    return jnp.concatenate(
        [jnp.where(mask, query, jnp.zeros_like(query)) for mask in masks], axis=0
    )


def gather_heads(values, masks):
    result = jnp.where(masks[0], values[:GRID_W], 0.0)
    for h in range(1, len(masks)):
        result = jnp.where(masks[h], values[h * GRID_W : (h + 1) * GRID_W], result)
    return result


def weighed(scores, values, masks):
    top = jnp.max(scores, axis=-1, keepdims=True)
    exps = jnp.exp(scores - top)
    total = jnp.sum(exps, axis=-1, keepdims=True)
    mixed = jnp.dot(exps.astype(jnp.bfloat16), values, preferred_element_type=jnp.float32)
    return [gather_heads(array, masks) for array in (mixed, top, total)]


def attend_near(place, query, before, pair, after, table, far, rows_all, per):
    samples, tokens, cols = query.shape
    rows_dev = tokens // GRID_W
    near_keys = WIN_ROWS * GRID_W
    ahead, behind = before.shape[1], after.shape[1]
    padded = ahead + tokens + behind
    lanes = -(-padded // 128) * 128
    bf16, f32 = jnp.bfloat16, jnp.float32

    def body(place_ref, q_ref, before_ref, pair_ref, after_ref, table_ref, *refs):
        mixed_ref, top_ref, total_ref, out_ref, near_t, values = refs
        sample, step = pl.program_id(0), pl.program_id(1)

        @pl.when(step == 0)
        def _():
            values[0:ahead] = before_ref[sample, :, cols:]
            values[ahead : ahead + tokens] = pair_ref[0, :, cols:]
            values[ahead + tokens : padded] = after_ref[sample, :, cols:]
            fill = jnp.zeros((lanes - padded, cols), bf16)
            near_t[0, :, :ahead] = before_ref[sample, :, :cols].T
            near_t[0, :, ahead : ahead + tokens] = pair_ref[0, :, :cols].T
            near_t[0, :, ahead + tokens :] = jnp.concatenate(
                [after_ref[sample, :, :cols], fill], axis=0
            ).T
            near_t[1] = jnp.concatenate(
                [
                    before_ref[sample, GRID_W:, :cols],
                    pair_ref[0, :, :cols],
                    after_ref[sample, :, :cols],
                    fill,
                    jnp.zeros((GRID_W, cols), bf16),
                ],
                axis=0,
            ).T

        base = place_ref[0] * rows_dev
        masks = head_masks(cols)
        scores, starts = [], []
        for r in range(per):
            actual = base + step * per + r
            start = jnp.clip(actual - REACH, 0, rows_all - WIN_ROWS)
            local = start - base + REACH
            offset = start - actual + WIN_ROWS - 1
            spread = spread_heads(q_ref[0, r * GRID_W : (r + 1) * GRID_W], masks)
            column = pl.multiple_of((local // 2) * 128, 128)
            keys_t = near_t[local % 2, :, pl.ds(column, near_keys)]
            bias_at = pl.multiple_of((offset // 2) * 128, 128)
            scores.append(
                jnp.dot(spread, keys_t, preferred_element_type=f32)
                + table_ref[offset % 2, :, pl.ds(bias_at, near_keys)]
            )
            starts.append(pl.multiple_of(local * GRID_W, GRID_W))
        for r in range(per):
            parts = weighed(scores[r], values[pl.ds(starts[r], near_keys), :], masks)
            mixed, top, total = parts
            at = slice(r * GRID_W, (r + 1) * GRID_W)
            far_top = top_ref[0, at]
            highest = jnp.maximum(top, far_top)
            near_part = jnp.exp(top - highest)
            far_part = jnp.exp(far_top - highest)
            total = total * near_part + total_ref[0, at] * far_part
            mixed = mixed * near_part + mixed_ref[0, at] * far_part
            out_ref[r, 0] = (mixed / total).astype(bf16)

    def of_sample(array):
        return pl.BlockSpec((1, *array.shape[1:]), lambda s, i: (s, 0, 0))

    rows_spec = pl.BlockSpec((1, per * GRID_W, cols), lambda s, i: (s, i, 0))
    return pl.pallas_call(
        body,
        grid=(samples, rows_dev // per),
        in_specs=[
            pl.BlockSpec(memory_space=pltpu.SMEM),
            rows_spec,
            RESIDENT,
            of_sample(pair),
            RESIDENT,
            RESIDENT,
        ]
        + [rows_spec] * 3,
        out_specs=pl.BlockSpec((per, 1, GRID_W, cols), lambda s, i: (i, s, 0, 0)),
        out_shape=jax.ShapeDtypeStruct((rows_dev, samples, GRID_W, cols), bf16),
        scratch_shapes=[
            pltpu.VMEM((2, cols, lanes), bf16),
            pltpu.VMEM((padded, cols), bf16),
        ],
        compiler_params=pltpu.CompilerParams(vmem_limit_bytes=32 * 2**20),
        name="attend_near",
    )(place, query, before, pair, after, table, *far)


def attend_far(query, ctx_pairs, ctx_bias, per):
    samples, tokens, cols = query.shape
    rows_dev = tokens // GRID_W
    ctx_rows = ctx_pairs[0].shape[2]
    members = [array.shape[0] for array in ctx_pairs]
    ctx_count = sum(members) * ctx_rows
    bf16, f32 = jnp.bfloat16, jnp.float32

    def body(q_ref, *refs):
        ctx_refs = refs[: len(members)]
        cb_ref, *out_refs, far_t, values = refs[len(members) :]
        sample, step = pl.program_id(0), pl.program_id(1)

        @pl.when(step == 0)
        def _():
            at = 0
            for ctx_ref, count in zip(ctx_refs, members):
                for member in range(count):
                    low = at + member * ctx_rows
                    values[low : low + ctx_rows] = ctx_ref[member, sample, :, cols:]
                size = count * ctx_rows
                block = jnp.concatenate(
                    [ctx_ref[member, sample, :, :cols] for member in range(count)], axis=0
                )
                far_t[:, at : at + size] = block.T
                at += size

        masks = head_masks(cols)
        context_bias = jnp.concatenate(
            [jnp.full((GRID_W, cols), cb_ref[h], f32) for h in range(len(masks))], axis=0
        )
        scores = [
            jnp.dot(
                spread_heads(q_ref[0, r * GRID_W : (r + 1) * GRID_W], masks),
                far_t[...],
                preferred_element_type=f32,
            )
            for r in range(per)
        ]
        for r in range(per):
            mixed, top, total = weighed(scores[r], values[...], masks)
            top = top + gather_heads(context_bias, masks)
            for out_ref, part in zip(out_refs, (mixed, top, total)):
                out_ref[0, r * GRID_W : (r + 1) * GRID_W] = part

    rows_spec = pl.BlockSpec((1, per * GRID_W, cols), lambda s, i: (s, i, 0))
    return pl.pallas_call(
        body,
        grid=(samples, rows_dev // per),
        in_specs=[
            rows_spec,
        ]
        + [RESIDENT] * len(members)
        + [pl.BlockSpec(memory_space=pltpu.SMEM)],
        out_specs=[rows_spec] * 3,
        out_shape=[jax.ShapeDtypeStruct((samples, tokens, cols), f32)] * 3,
        scratch_shapes=[
            pltpu.VMEM((cols, ctx_count), bf16),
            pltpu.VMEM((ctx_count, cols), bf16),
        ],
        compiler_params=pltpu.CompilerParams(vmem_limit_bytes=32 * 2**20),
        name="attend_far",
    )(query, *ctx_pairs, ctx_bias)


def finish(attended, w_out, latent, modulation, tiles):
    groups, _, _ = attended.shape
    samples, tokens, width = latent.shape
    block = modulation.shape[2] * tiles
    first = modulation.shape[1] - samples

    def body(att_ref, w_ref, latent_ref, tile_ref, out_ref):
        everything = jnp.concatenate([att_ref[group] for group in range(groups)], axis=1)
        update = jnp.dot(everything, w_ref[...], preferred_element_type=jnp.float32)
        for s in range(samples):
            gate = jnp.concatenate(
                [tile_ref[t, first + s : first + s + 1, :] for t in range(tiles)], axis=1
            )
            part = update[s * tokens : (s + 1) * tokens]
            out_ref[s] = (latent_ref[s].astype(jnp.float32) + gate * part).astype(jnp.bfloat16)

    return pl.pallas_call(
        body,
        grid=(width // block,),
        in_specs=[
            whole(attended.shape),
            pl.BlockSpec((width, block), lambda i: (0, i)),
            pl.BlockSpec((samples, tokens, block), lambda i: (0, 0, i)),
            pl.BlockSpec((tiles, *modulation.shape[1:]), lambda i: (i, 0, 0)),
        ],
        out_specs=pl.BlockSpec((samples, tokens, block), lambda i: (0, 0, i)),
        out_shape=jax.ShapeDtypeStruct(latent.shape, latent.dtype),
        name="finish",
    )(attended, w_out, latent, modulation)


def shifted(size, side, stride, value):
    span = side * stride
    return [(i, i // span * span + (i + value * stride) % span) for i in range(size)]


def from_line(block, axis, side, stride):
    size = lax.axis_size(axis)
    return [block] + [
        lax.ppermute(block, axis, shifted(size, side, stride, value)) for value in range(1, side)
    ]


def computation(
    latent,
    context,
    cond,
    ctx_cond,
    w_shift,
    w_scale,
    w_gate,
    norm_gain,
    w_query,
    w_key,
    w_value,
    w_out,
    rel_bias,
    ctx_bias,
):
    samples, tokens_dev, width = latent.shape
    local_cols = w_shift.shape[1]
    sp_index = lax.axis_index("sp")
    sp_size, tp_size = lax.axis_size("sp"), lax.axis_size("tp")
    place = jnp.full((1,), sp_index, jnp.int32)
    gathered = lax.all_gather(latent, "tp", axis=1, tiled=True)
    parts = modulation_parts(place, cond, ctx_cond, (w_shift, w_scale, w_gate), sp_size)
    parts, w_out_own = lax.optimization_barrier((parts, w_out))
    w_out_all = lax.all_gather(w_out_own, "tp", axis=0, tiled=True)
    table = bias_table(rel_bias)
    summed = jnp.sum(lax.all_to_all(parts, "sp", 0, 0, tiled=True), axis=0)
    summed, table = lax.optimization_barrier((summed, table))
    modulation = resident(copy_for_each(summed, "tp"))
    w_query, w_key, w_value = resident(w_query), resident(w_key), resident(w_value)
    table = resident(table)

    gain = norm_gain[None, :]
    ctx_rows = context.shape[1]
    (ctx_pair,) = project(
        pltpu.with_memory_space_constraint(
            context.reshape(1, samples * ctx_rows, width), pltpu.HBM
        ),
        gain,
        modulation,
        (w_key, w_value),
        samples,
        samples * ctx_rows,
        None,
    )
    ctx_pair = ctx_pair.reshape(samples, ctx_rows, 2 * local_cols)
    ctx_pairs = from_line(ctx_pair, "sp", 4, 1)
    up = [(i, i + 1) for i in range(sp_size - 1)]
    down = [(j, i) for i, j in up]
    gathered = pltpu.with_memory_space_constraint(gathered, pltpu.HBM)
    ends = ((WIN_ROWS - REACH - 1) * GRID_W, REACH * GRID_W)
    w_triple = (w_key, w_value, w_query)
    outs = project(gathered, gain, modulation, w_triple, 0, 256, ends, 0)
    ctx_line = stacked(ctx_pairs)
    below = lax.ppermute(ctx_line, "sp", shifted(sp_size, 4, 4, 1))
    above = lax.ppermute(ctx_line, "sp", shifted(sp_size, 4, 4, 3))
    for s in range(1, samples):
        outs = project(gathered, gain, modulation, w_triple, 0, 256, ends, s, outs)
    pair, query, first, last = outs
    rows_all = pair.shape[1] // GRID_W * sp_size
    ctx_pairs = [
        ctx_line,
        below,
        above,
        lax.ppermute(below[:2], "sp", shifted(sp_size, 4, 4, 1)),
        lax.ppermute(above[2:], "sp", shifted(sp_size, 4, 4, 3)),
    ]
    before = resident(lax.ppermute(last, "sp", up))
    after = resident(lax.ppermute(first, "sp", down))
    ctx_pairs = [resident(array) for array in ctx_pairs]
    far = attend_far(query, ctx_pairs, ctx_bias, 8)
    attended = attend_near(place, query, before, pair, after, table, far, rows_all, 4)
    attended = attended.reshape(tp_size, samples * tokens_dev, local_cols)
    attended = lax.all_to_all(attended, "tp", 0, 0, tiled=True)
    return finish(attended, w_out_all, latent, modulation, 4)


def stacked(blocks):
    def body(*refs):
        for number in range(len(blocks)):
            refs[-1][number] = refs[number][...]

    return pl.pallas_call(
        body,
        in_specs=[RESIDENT] * len(blocks),
        out_specs=RESIDENT,
        out_shape=jax.ShapeDtypeStruct((len(blocks), *blocks[0].shape), blocks[0].dtype),
        compiler_params=pltpu.CompilerParams(vmem_limit_bytes=8 * 2**20),
        name="stacked",
    )(*[resident(block) for block in blocks])


def solution(mesh):
    return jax.shard_map(
        computation,
        mesh=mesh,
        in_specs=(
            P(None, ("sp", "tp"), None),
            P(None, "sp", None),
            P(),
            P(),
            P("sp", "tp"),
            P("sp", "tp"),
            P("sp", "tp"),
            P(),
            P(None, "tp"),
            P(None, "tp"),
            P(None, "tp"),
            P("tp", None),
            P("tp", None, None),
            P("tp"),
        ),
        out_specs=P(None, ("sp", "tp"), None),
        check_vma=False,
    )
```
